256 devices in a mesh: kv: 64 (over z, y, core), tp: 4 (over x).
Axes of the slice: x: 4, y: 4, z: 8, core: 2. Of those that a mesh axis runs over, the one named last changes fastest.
Arguments:
- hidden_vectors: bfloat16 [512, 2048], P(None, 'kv'), may hold values from -24 to 24
- input_norm_gain: float32 [2048], P('kv'), may hold values from 0.1 to 1.9
- gate_matrix: bfloat16 [2048, 4096], P('kv', 'tp'), may hold values from -0.125 to 0.125
- value_matrix: bfloat16 [2048, 4096], P('kv', 'tp'), may hold values from -0.125 to 0.125
- write_matrix: bfloat16 [2048, 2048], P('kv', 'tp'), may hold values from -0.125 to 0.125
- read_matrix: bfloat16 [2048, 2048], P('kv', 'tp'), may hold values from -0.125 to 0.125
- step_matrix: bfloat16 [2048, 64], P('kv', 'tp'), may hold values from -0.125 to 0.125
- raw_value_rows: bfloat16 [128, 7, 4096], P('kv', None, 'tp'), may hold values from -6 to 6
- raw_write_rows: bfloat16 [128, 7, 2048], P('kv', None, 'tp'), may hold values from -6 to 6
- raw_read_rows: bfloat16 [128, 7, 2048], P('kv', None, 'tp'), may hold values from -6 to 6
- value_filter_taps: bfloat16 [4, 4096], P(None, 'tp'), may hold values from -3 to 3
- write_filter_taps: bfloat16 [4, 2048], P(None, 'tp'), may hold values from -3 to 3
- read_filter_taps: bfloat16 [4, 2048], P(None, 'tp'), may hold values from -3 to 3
- step_size_bias: float32 [64], P('tp'), may hold values from -3 to 0
- rate_logarithm: float32 [64], P('tp'), may hold values from -4 to 0.5
- direct_path_gain: float32 [64], P('tp'), may hold values from 0.1 to 1.9
- prior_step_preact: float32 [128, 4, 64], P('kv', None, 'tp'), may hold values from -6 to 6
- extra_log_decay: float32 [128, 8, 64], P('kv', None, 'tp'), may hold values from -0.7 to 0, as said below
- accepted: int32 [128], P('kv'), may hold values from 0 to 4
- prior_state: float32 [128, 64, 64, 128], P('kv', 'tp'), may hold values from -6 to 6
- group_norm_gain: float32 [4096], P('tp'), may hold values from 0.1 to 1.9
- output_matrix: bfloat16 [4096, 2048], P('tp', 'kv'), may hold values from -0.09375 to 0.09375
Outputs:
- mixer_out: bfloat16 [512, 2048], P('tp', 'kv')
- resumed_state: float32 [128, 64, 64, 128], P('kv', 'tp')
The draws below stay inside these ranges and needn't reach their ends.
Inputs may be any that keep to these rules, and one draw needn't show every extreme that they name: `extra_log_decay`: zero at most positions.
All inputs are finite; a program needn't handle non-finite values.
Results may differ from the reference program's by a relative error of at most 0.0095.
Values may be sent and summed in bfloat16 or wider, within the bound.
A program may use at most 64 MiB of HBM per device.

```python
import math
import jax
import jax.numpy as jnp
from jax import lax

D = 2048
HEADS = 64
HEAD_DIM = 64
GROUPS = 16
STATE = 128
TAPS = 4
DRAFT_TOKENS = 4
INNER = 4096
SEQS = 128
TOKENS = 512
N_TP = 4


def draw_hidden_vectors(key, part):
    normal_base = jax.random.normal(jax.random.fold_in(key, 11), (TOKENS, D), jnp.float32)
    column_scale = jnp.exp(jnp.arange(D, dtype=jnp.float32) * (math.log(4.0) / D)) * 0.5
    values = normal_base * column_scale
    return jnp.clip(values, -24.0, 24.0).astype(jnp.bfloat16)


def draw_extra_log_decay(key, part):
    chosen = jax.random.uniform(jax.random.fold_in(key, 21), (SEQS, 2 * DRAFT_TOKENS, HEADS)) < 0.15
    losses = jnp.log(jax.random.uniform(jax.random.fold_in(key, 22), (SEQS, 2 * DRAFT_TOKENS, HEADS), minval=0.5, maxval=0.8))
    return jnp.where(chosen, losses, 0.0).astype(jnp.float32)


def set_ends(drawn, key, smallest, top_value):
    shape = drawn.shape
    index_at = [jax.random.randint(jax.random.fold_in(key, axis), (), 0, shape[axis]) for axis in range(len(shape))]
    drawn = drawn.at[tuple(index_at)].set(smallest)
    longest = shape.index(max(shape))
    index_at[longest] = (index_at[longest] + 1) % shape[longest]
    return drawn.at[tuple(index_at)].set(top_value)


def shard_levels(stream_key, extent, shards, low, largest):
    def one(dim, blocks):
        heights = jax.random.uniform(jax.random.fold_in(jax.random.fold_in(stream_key, 6), dim), (blocks,), jnp.float32, low / len(shards), largest / len(shards))
        return jnp.repeat(jnp.exp(heights), extent[dim] // blocks).reshape((-1,) + (1,) * (len(extent) - dim - 1))

    gain = one(*shards[0])
    for cut in shards[1:]:
        gain = gain * one(*cut)
    return gain


def normal_values(stream_key, extent, spread, reach, pieces=(), kind=jnp.bfloat16):
    values = jax.random.normal(stream_key, extent, jnp.float32) * spread
    if len(pieces) > 0:
        values = shard_levels(stream_key, extent, pieces, -0.22, 0.18) * values
    return jnp.clip(values, min=-reach, max=reach).astype(kind)


def setup_inputs(seed: int = 0) -> dict:
    key_of = jax.random.split(jax.random.key(seed), 23)
    hidden_vectors = draw_hidden_vectors(jax.random.fold_in(key_of[22], 71), 0)
    input_norm_gain = jnp.clip(1.0 + 0.18 * jax.random.normal(key_of[1], (D,), jnp.float32), 0.1, 1.9)
    gate_matrix = normal_values(key_of[2], (D, INNER), D ** -0.5, 0.125, ((0, 64), (1, 4)))
    value_matrix = normal_values(key_of[3], (D, INNER), D ** -0.5, 0.125, ((0, 64), (1, 4)))
    write_matrix = normal_values(key_of[4], (D, GROUPS * STATE), D ** -0.5, 0.125, ((0, 64), (1, 4)))
    read_matrix = normal_values(key_of[5], (D, GROUPS * STATE), D ** -0.5, 0.125, ((0, 64), (1, 4)))
    step_matrix = normal_values(key_of[6], (D, HEADS), D ** -0.5, 0.125, ((0, 64), (1, 4)))
    raw_value_rows = normal_values(key_of[7], (SEQS, TAPS - 1 + DRAFT_TOKENS, INNER), 1.0, 6.0, ((0, 64), (2, 4)))
    raw_write_rows = normal_values(key_of[8], (SEQS, TAPS - 1 + DRAFT_TOKENS, GROUPS * STATE), 1.0, 6.0, ((0, 64), (2, 4)))
    raw_read_rows = normal_values(key_of[9], (SEQS, TAPS - 1 + DRAFT_TOKENS, GROUPS * STATE), 1.0, 6.0, ((0, 64), (2, 4)))
    value_filter_taps = normal_values(key_of[10], (TAPS, INNER), TAPS ** -0.5, 3.0, ((1, 4),))
    write_filter_taps = normal_values(key_of[11], (TAPS, GROUPS * STATE), TAPS ** -0.5, 3.0, ((1, 4),))
    read_filter_taps = normal_values(key_of[12], (TAPS, GROUPS * STATE), TAPS ** -0.5, 3.0, ((1, 4),))
    step_size_bias = jnp.clip(-3.0 + 3.0 * jax.random.uniform(key_of[13], (HEADS,), jnp.float32) ** shard_levels(key_of[13], (HEADS,), ((0, 4),), -0.2, 0.2), -3.0, 0.0)
    rate_logarithm = jnp.clip(-4.0 + 4.5 * jax.random.uniform(key_of[14], (HEADS,), jnp.float32) ** shard_levels(key_of[14], (HEADS,), ((0, 4),), -0.2, 0.2), -4.0, 0.5)
    direct_path_gain = jnp.clip(1.0 + 0.18 * jax.random.normal(key_of[15], (HEADS,), jnp.float32), 0.1, 1.9)
    prior_step_preact = normal_values(key_of[16], (SEQS, DRAFT_TOKENS, HEADS), 1.0, 6.0, ((0, 64), (2, 4)), jnp.float32)
    extra_log_decay = draw_extra_log_decay(jax.random.fold_in(key_of[22], 71), 0)
    accepted = set_ends(jax.random.randint(key_of[18], (SEQS,), 0, DRAFT_TOKENS + 1), jax.random.fold_in(key_of[18], 1), 0, DRAFT_TOKENS).astype(jnp.int32)
    prior_state = normal_values(key_of[19], (SEQS, HEADS, HEAD_DIM, STATE), 1.0, 6.0, ((0, 64), (1, 4)), jnp.float32)
    group_norm_gain = jnp.clip(1.0 + 0.18 * jax.random.normal(key_of[20], (INNER,), jnp.float32), 0.1, 1.9)
    output_matrix = normal_values(key_of[21], (INNER, D), INNER ** -0.5, 0.09375, ((0, 4), (1, 64)))
    return dict(hidden_vectors=hidden_vectors, input_norm_gain=input_norm_gain, gate_matrix=gate_matrix, value_matrix=value_matrix, write_matrix=write_matrix, read_matrix=read_matrix, step_matrix=step_matrix, raw_value_rows=raw_value_rows, raw_write_rows=raw_write_rows, raw_read_rows=raw_read_rows, value_filter_taps=value_filter_taps, write_filter_taps=write_filter_taps, read_filter_taps=read_filter_taps, step_size_bias=step_size_bias, rate_logarithm=rate_logarithm, direct_path_gain=direct_path_gain, prior_step_preact=prior_step_preact, extra_log_decay=extra_log_decay, accepted=accepted, prior_state=prior_state, group_norm_gain=group_norm_gain, output_matrix=output_matrix)


epsilon = 1e-06
highest = lax.Precision.HIGHEST

def conv_rows(row_block, taps):
    length_rows = row_block.shape[1] - (TAPS - 1)
    result = jnp.zeros((row_block.shape[0], length_rows, row_block.shape[2]), jnp.float32)
    for tap_index in range(TAPS):
        result = result + row_block[:, tap_index:tap_index + length_rows].astype(jnp.float32) * taps[tap_index].astype(jnp.float32)
    return jax.nn.silu(result)

def resume_state(start_state, values, writes, head_step_size, decay_logarithm, accepted):
    live_mask = (jnp.arange(values.shape[1])[None, :] < accepted[:, None]).astype(jnp.float32)
    kept_decay = decay_logarithm * live_mask[:, :, None]
    total_decay = lax.optimization_barrier(jnp.sum(kept_decay, axis=1))
    tail_decay = total_decay[:, None, :] - jnp.cumsum(kept_decay, axis=1)
    coefficient = live_mask[:, :, None] * jnp.exp(tail_decay) * head_step_size
    added = jnp.einsum('skh,skhp,skhn->shpn', coefficient, values, writes, precision=highest)
    return jnp.exp(total_decay)[:, :, None, None] * start_state + added

def dual_block(values, writes, reads, head_step_size, decay_logarithm, direct_path_gain, start_state):
    cumulative = jnp.cumsum(decay_logarithm, axis=1)
    carried = jnp.exp(cumulative)[..., None] * jnp.einsum('skhn,shpn->skhp', reads, start_state, precision=highest)
    order = jnp.arange(cumulative.shape[1])
    causal = order[:, None] >= order[None, :]
    difference = cumulative[:, :, None, :] - cumulative[:, None, :, :]
    decay_weight = jnp.where(causal[None, :, :, None], jnp.exp(jnp.minimum(difference, 0.0)), 0.0)
    inner_terms = jnp.einsum('sthn,suhn->stuh', reads, writes, precision=highest)
    within = jnp.einsum('stuh,suh,suhp->sthp', inner_terms * decay_weight, head_step_size, values, precision=highest)
    return carried + within + direct_path_gain[None, None, :, None] * values

def mixer_kernel_body(output_gate, fresh_values, fresh_writes, fresh_reads, step_preact, raw_value_rows, raw_write_rows, raw_read_rows, value_filter_taps, write_filter_taps, read_filter_taps, step_size_bias, rate_logarithm, direct_path_gain, prior_step_preact, extra_log_decay, accepted, prior_state, group_norm_gain):
    seq_count = raw_value_rows.shape[0]
    head_count = step_preact.shape[2]
    group_count = fresh_writes.shape[2] // STATE
    per_group = head_count // group_count
    window = accepted[:, None] + jnp.arange(TAPS - 1, dtype=jnp.int32)[None, :]

    def current(row_block, new_rows, taps):
        earlier = jnp.take_along_axis(row_block, window[:, :, None], axis=1)
        return conv_rows(jnp.concatenate([earlier, new_rows], axis=1), taps)
    conv_values = current(raw_value_rows, fresh_values, value_filter_taps).reshape(seq_count, DRAFT_TOKENS, head_count, HEAD_DIM)
    conv_writes = current(raw_write_rows, fresh_writes, write_filter_taps).reshape(seq_count, DRAFT_TOKENS, group_count, STATE)
    conv_reads = current(raw_read_rows, fresh_reads, read_filter_taps).reshape(seq_count, DRAFT_TOKENS, group_count, STATE)
    last_values = conv_rows(raw_value_rows, value_filter_taps).reshape(seq_count, DRAFT_TOKENS, head_count, HEAD_DIM)
    last_writes = conv_rows(raw_write_rows, write_filter_taps).reshape(seq_count, DRAFT_TOKENS, group_count, STATE)
    head_decay_rate = jnp.exp(rate_logarithm)
    head_step_size = jax.nn.softplus(step_preact + step_size_bias)
    decay_logarithm = -head_decay_rate * head_step_size + extra_log_decay[:, DRAFT_TOKENS:]
    prior_step = jax.nn.softplus(prior_step_preact + step_size_bias)
    prior_decay = -head_decay_rate * prior_step + extra_log_decay[:, :DRAFT_TOKENS]
    restored_state = resume_state(prior_state, last_values, jnp.repeat(last_writes, per_group, axis=2), prior_step, prior_decay, accepted)
    mixed_heads = dual_block(conv_values, jnp.repeat(conv_writes, per_group, axis=2), jnp.repeat(conv_reads, per_group, axis=2), head_step_size, decay_logarithm, direct_path_gain, restored_state)
    gated = mixed_heads.reshape(seq_count, DRAFT_TOKENS, -1) * jax.nn.silu(output_gate.astype(jnp.float32))
    group_width = INNER // GROUPS
    grouped = gated.reshape(seq_count, DRAFT_TOKENS, -1, group_width)
    scale = lax.rsqrt(lax.optimization_barrier(jnp.mean(grouped * grouped, axis=-1, keepdims=True)) + epsilon)
    normalized_hidden = (grouped * scale).reshape(seq_count, DRAFT_TOKENS, -1) * group_norm_gain
    return (normalized_hidden.astype(jnp.bfloat16).reshape(seq_count * DRAFT_TOKENS, -1), restored_state)

def reference(hidden_vectors, input_norm_gain, gate_matrix, value_matrix, write_matrix, read_matrix, step_matrix, raw_value_rows, raw_write_rows, raw_read_rows, value_filter_taps, write_filter_taps, read_filter_taps, step_size_bias, rate_logarithm, direct_path_gain, prior_step_preact, extra_log_decay, accepted, prior_state, group_norm_gain, output_matrix):
    floats_in = hidden_vectors.astype(jnp.float32)
    inverse = lax.rsqrt(lax.optimization_barrier(jnp.mean(floats_in * floats_in, axis=1)) + epsilon)[:, None]
    scaled = (floats_in * input_norm_gain).astype(jnp.bfloat16)

    def project(weight):
        return inverse * jnp.dot(scaled, weight, preferred_element_type=jnp.float32)

    def shaped(matrix):
        return matrix.reshape(SEQS, DRAFT_TOKENS, -1)
    output_gate = shaped(project(gate_matrix).astype(jnp.bfloat16))
    fresh_values = shaped(project(value_matrix).astype(jnp.bfloat16))
    fresh_writes = shaped(project(write_matrix).astype(jnp.bfloat16))
    fresh_reads = shaped(project(read_matrix).astype(jnp.bfloat16))
    step_preact = shaped(project(step_matrix))
    normalized_hidden, restored_state = mixer_kernel_body(output_gate, fresh_values, fresh_writes, fresh_reads, step_preact, raw_value_rows, raw_write_rows, raw_read_rows, value_filter_taps, write_filter_taps, read_filter_taps, step_size_bias, rate_logarithm, direct_path_gain, prior_step_preact, extra_log_decay, accepted, prior_state, group_norm_gain)
    block_width = INNER // N_TP
    mixer_out = jnp.zeros((TOKENS, D), jnp.float32)
    for block_index in range(N_TP):
        lower = block_index * block_width
        partial_value = jnp.dot(normalized_hidden[:, lower:lower + block_width], output_matrix[lower:lower + block_width], preferred_element_type=jnp.float32).astype(jnp.bfloat16)
        partial_value = lax.optimization_barrier(partial_value)
        mixer_out = mixer_out + partial_value.astype(jnp.float32)
    return (mixer_out.astype(jnp.bfloat16), restored_state)
```

```python
import jax
import jax.numpy as jnp
from jax import lax
from jax.experimental import pallas as pl
from jax.experimental.pallas import tpu as pltpu
from jax.sharding import PartitionSpec as P

MESH = pl.DeviceIdType.MESH
F32 = jnp.float32
BF16 = jnp.bfloat16
EPS = 1e-6
Z_ORDER = (4, 3, 5, 2, 6, 1, 7, 0)


def silu(x):
    return x / (1.0 + jnp.exp(-x))


def softplus(x):
    return jnp.maximum(x, 0.0) + jnp.log(1.0 + jnp.exp(-jnp.abs(x)))


def mixer_kernel(
    acc_s,
    hid, gain, wg, wv, ww, wr, ws, rawv, raww, rawr, tv, tw, tr, bias, rate, dgain, ppre, extra, prior, ngain, wo,
    out_ref, st_out,
    hid_v, gain_v, wg_v, wv_v, ww_v, wr_v, ws_v, rawv_v, raww_v, rawr_v, tv_v, tw_v, tr_v, bias_v, rate_v, dgain_v,
    ppre_v, extra_v, prior_v, ngain_v, wo_v,
    acts_t, wsend, wblk, sblk, acts_f, acts_b, psend, precv, esend, erecv, tot, fsend, frecv, nrm, wog, osend, orecv,
    base, state_b,
    lsem, osem, s1_send, s1_recv, w_send, w_recv, k_send, k_recv, p_send, p_recv, e_send, e_recv, f_send, f_recv,
    n_send, n_recv, g_send, g_recv, o_send, o_recv, ready,
):
    kv = lax.axis_index("kv")
    tp = lax.axis_index("tp")
    z = lax.div(kv, 8)
    c = lax.rem(kv, 8)

    def plane(r):
        return z * 8 + lax.rem(c + r, 8)

    def ring(r):
        return lax.rem(z + r, 8) * 8 + c

    def remote(src, dst, ssem, rsem, kv_to, tp_to):
        return pltpu.make_async_remote_copy(
            src_ref=src, dst_ref=dst, send_sem=ssem, recv_sem=rsem,
            device_id={"kv": kv_to, "tp": tp_to}, device_id_type=MESH,
        )

    pairs = [
        (hid, hid_v), (gain, gain_v), (wg, wg_v), (wv, wv_v), (ww, ww_v), (wr, wr_v), (ws, ws_v), (wo, wo_v),
        (rawv, rawv_v), (raww, raww_v), (rawr, rawr_v), (tv, tv_v), (tw, tw_v), (tr, tr_v), (bias, bias_v),
        (rate, rate_v), (dgain, dgain_v), (ppre, ppre_v), (extra, extra_v), (ngain, ngain_v), (prior, prior_v),
    ]
    loads = [pltpu.make_async_copy(s, d, lsem.at[i]) for i, (s, d) in enumerate(pairs)]
    for cp in loads:
        cp.start()

    barrier = pltpu.get_barrier_semaphore()
    for r in range(1, 8):
        pl.semaphore_signal(barrier, inc=1, device_id={"kv": plane(r), "tp": tp}, device_id_type=MESH)
    for r in range(1, 8):
        pl.semaphore_signal(barrier, inc=1, device_id={"kv": ring(r), "tp": tp}, device_id_type=MESH)
    for r in range(1, 4):
        pl.semaphore_signal(barrier, inc=1, device_id={"kv": kv, "tp": lax.rem(tp + r, 4)}, device_id_type=MESH)

    own32 = pl.ds(pl.multiple_of(c * 32, 32), 32)
    loads[0].wait()
    acts_t[own32, :] = jnp.transpose(hid_v[...].astype(F32)).astype(BF16)
    for i in range(1, 7):
        loads[i].wait()
    diag = lax.broadcasted_iota(jnp.int32, (32, 32), 0) == lax.broadcasted_iota(jnp.int32, (32, 32), 1)
    gcol = jnp.sum(jnp.where(diag, jnp.broadcast_to(gain_v[...], (32, 32)), 0.0), axis=1, keepdims=True)
    for j in range(8):
        lane = slice(j * 128, j * 128 + 128)
        wsend[j, :, 0:128] = (wg_v[:, lane].astype(F32) * gcol).astype(BF16)
        wsend[j, :, 128:256] = (wv_v[:, lane].astype(F32) * gcol).astype(BF16)
        half = slice((j % 4) * 128, (j % 4) * 128 + 128)
        source = ww_v if j < 4 else wr_v
        wsend[j, :, 256:384] = (source[:, half].astype(F32) * gcol).astype(BF16)
    wblk[own32, :] = wsend[c]
    step_w = (ws_v[...].astype(F32) * gcol).astype(BF16)
    sblk[own32, :] = jnp.concatenate([step_w.astype(F32), jnp.zeros((32, 112), F32)], axis=1).astype(BF16)

    pl.semaphore_wait(barrier, 17)
    for r in range(1, 4):
        pl.semaphore_signal(ready, inc=1, device_id={"kv": kv, "tp": lax.rem(tp + r, 4)}, device_id_type=MESH)

    acts_cp, w_cp, k_cp = [], [], []
    for r in range(1, 8):
        cp = remote(acts_t.at[own32, :], acts_t.at[own32, :], s1_send.at[r], s1_recv.at[r], plane(r), tp)
        cp.start()
        acts_cp.append(cp)
    for r in range(1, 8):
        cp = remote(wsend.at[lax.rem(c + r, 8)], wblk.at[own32, :], w_send.at[r], w_recv.at[r], plane(r), tp)
        cp.start()
        w_cp.append(cp)
        cp = remote(sblk.at[own32, :], sblk.at[own32, :], k_send.at[r], k_recv.at[r], plane(r), tp)
        cp.start()
        k_cp.append(cp)

    loads[7].wait()
    for i in range(8):
        wog[z, :, i * 128:(i + 1) * 128] = jnp.transpose(
            wo_v[i * 128:(i + 1) * 128, :].astype(F32)
        ).astype(BF16)
    g_cp = {}
    for r in range(1, 8):
        g_cp[r] = remote(wog.at[z], wog.at[z], g_send.at[r], g_recv.at[r], ring(r), tp)
    for r in (2, 6, 1, 7):
        g_cp[r].start()

    for cp in loads[8:]:
        cp.wait()
    row8 = lax.broadcasted_iota(jnp.int32, (8, 1), 0)
    tok = lax.rem(row8, 4)

    def down(x, d):
        if d == 0:
            return x
        return jnp.where(tok >= d, pltpu.roll(x, d, axis=0), 0.0)

    def up(x, d):
        return jnp.where(tok + d < 4, pltpu.roll(x, 8 - d, axis=0), 0.0)

    def last_conv(raw, taps):
        parts = []
        for s in range(2):
            rows = raw[s].astype(F32)
            t = taps[...].astype(F32)
            total = rows[0:4] * t[0:1]
            for j in range(1, 4):
                total = total + rows[j:j + 4] * t[j:j + 1]
            parts.append(total)
        return silu(jnp.concatenate(parts, axis=0))

    def base_conv(raw, taps, lo, hi):
        t = taps[...].astype(F32)
        zero = jnp.zeros((1, hi - lo), F32)
        rows_out = []
        for s in range(2):
            rows = raw[s].astype(F32)
            a = acc_s[s]
            win = rows[4:7]
            for k in range(3, -1, -1):
                win = jnp.where(a == k, rows[k:k + 3], win)
            w0, w1, w2 = win[0:1], win[1:2], win[2:3]
            rows_out += [w0 * t[0:1] + w1 * t[1:2] + w2 * t[2:3], w1 * t[0:1] + w2 * t[1:2], w2 * t[0:1], zero]
        base[:, lo:hi] = jnp.concatenate(rows_out, axis=0)

    lastv = last_conv(rawv_v, tv_v)
    lastw = last_conv(raww_v, tw_v)
    base_conv(rawv_v, tv_v, 0, 1024)
    base_conv(raww_v, tw_v, 1024, 1536)
    base_conv(rawr_v, tr_v, 1536, 2048)

    rate_e = -jnp.exp(rate_v[...])
    bias_r = bias_v[...]
    pstep = softplus(jnp.concatenate([ppre_v[0], ppre_v[1]], axis=0) + bias_r)
    pextra = jnp.concatenate([extra_v[0, 0:4], extra_v[1, 0:4]], axis=0)
    nextra = jnp.concatenate([extra_v[0, 4:8], extra_v[1, 4:8]], axis=0)
    limit = jnp.where(row8 < 4, acc_s[0], acc_s[1])
    live = jnp.where(tok < limit, 1.0, 0.0)
    kept = (rate_e * pstep + pextra) * live
    tail = up(kept, 1) + up(kept, 2) + up(kept, 3)
    coef = live * jnp.exp(tail) * pstep
    etot = jnp.exp(kept + tail)
    lane128 = lax.broadcasted_iota(jnp.int32, (8, 128), 1)
    low_half = lane128 < 64

    def spread(e, i):
        a = jnp.broadcast_to(e[:, 2 * i:2 * i + 1], (8, 128))
        b = jnp.broadcast_to(e[:, 2 * i + 1:2 * i + 2], (8, 128))
        return jnp.where(low_half, a, b)

    for g in range(4):
        vals = [lastv[:, (2 * g + i) * 128:(2 * g + i + 1) * 128] * spread(coef, 2 * g + i) for i in range(2)]
        weighted = jnp.concatenate(vals, axis=1)
        lw = lastw[:, g * 128:(g + 1) * 128]
        for s in range(2):
            own_seq = (row8 < 4) if s == 0 else (row8 >= 4)
            added = lax.dot_general(
                weighted, jnp.where(own_seq, lw, 0.0), (((0,), (0,)), ((), ())),
                precision=lax.Precision.HIGHEST, preferred_element_type=F32,
            )
            for i in range(4):
                h = g * 4 + i
                rows = slice(i * 64, i * 64 + 64)
                factor = jnp.broadcast_to(etot[s * 4:s * 4 + 1, h:h + 1], (64, 128))
                new = factor * prior_v[s, g, rows, :] + added[rows, :]
                prior_v[s, g, rows, :] = new
                state_b[s, g, rows, :] = new.astype(BF16)
    state_cp = pltpu.make_async_copy(prior_v, st_out, osem)
    state_cp.start()

    for cp in acts_cp:
        cp.wait_recv()
    for i in range(4):
        block = jnp.transpose(acts_t[:, i * 128:(i + 1) * 128].astype(F32))
        acts_f[i * 128:(i + 1) * 128, :] = block
        acts_b[i * 128:(i + 1) * 128, :] = block.astype(BF16)
    for cp in w_cp:
        cp.wait_recv()
    for cp in k_cp:
        cp.wait_recv()
    p_cp, e_cp = [], []
    for r in Z_ORDER:
        zz = lax.rem(z + r, 8)
        part = jnp.dot(
            acts_b[pl.ds(pl.multiple_of(zz * 64, 64), 64), :], wblk[...], preferred_element_type=F32
        ).astype(BF16)
        xs = acts_f[pl.ds(pl.multiple_of(zz * 64 + c * 8, 8), 8), :]
        ext = jnp.dot(xs.astype(BF16), sblk[...], preferred_element_type=F32)
        ext = jnp.where(lane128 == 16, jnp.sum(xs * xs, axis=1, keepdims=True), ext)
        if r == 0:
            precv[z] = part
            erecv[z] = ext
        else:
            psend[r] = part
            esend[r] = ext
            cp = remote(psend.at[r], precv.at[z], p_send.at[r], p_recv.at[r], ring(r), tp)
            cp.start()
            p_cp.append(cp)
            cp = remote(esend.at[r], erecv.at[z], e_send.at[r], e_recv.at[r], ring(r), tp)
            cp.start()
            e_cp.append(cp)
    for r in (4, 3, 5):
        g_cp[r].start()

    for cp in e_cp:
        cp.wait_recv()
    esum = erecv[0]
    for k in range(1, 8):
        esum = esum + erecv[k]
    inverse = lax.rsqrt(esum[:, 16:17] / 2048.0 + EPS)
    step = softplus(inverse * esum[:, 0:16] + bias_r)
    decay = rate_e * step + nextra
    cum = decay + down(decay, 1) + down(decay, 2) + down(decay, 3)
    pair_w = []
    for d in range(4):
        w = jnp.exp(jnp.minimum(cum - down(cum, d), 0.0)) * down(step, d)
        pair_w.append(jnp.where(tok >= d, w, 0.0))
    ecum = jnp.exp(cum)

    for cp in p_cp:
        cp.wait_recv()
    total = precv[0].astype(F32)
    for k in range(1, 8):
        total = total + precv[k].astype(F32)
    for j in range(8):
        rows = total[j * 8:j * 8 + 8, :]
        two = jnp.concatenate(
            [rows[:, 0:256], jnp.concatenate([rows[:, 256:384], rows[:, 256:384]], axis=1)], axis=0
        )
        fsend[j] = two.astype(BF16)
    frecv[c] = fsend[c]
    f_cp = []
    for r in range(1, 8):
        cp = remote(fsend.at[lax.rem(c + r, 8)], frecv.at[c], f_send.at[r], f_recv.at[r], plane(r), tp)
        cp.start()
        f_cp.append(cp)

    dg = jnp.broadcast_to(dgain_v[...], (8, 16))
    for cp in f_cp:
        cp.wait_recv()

    def fresh(j):
        return frecv[j].astype(F32)

    def rounded(x):
        return (x * inverse).astype(BF16).astype(F32)

    def conv(x, lo, taps, at):
        t = taps[:, at:at + 128].astype(F32)
        y = base[:, lo:lo + 128] + x * t[3:4]
        for d in range(1, 4):
            y = y + down(x, d) * t[3 - d:4 - d]
        return silu(y)

    writes, reads = [], []
    for g in range(4):
        writes.append(conv(rounded(fresh(g)[8:16, 0:128]), 1024 + g * 128, tw_v, g * 128))
        reads.append(conv(rounded(fresh(4 + g)[8:16, 0:128]), 1536 + g * 128, tr_v, g * 128))
    carried = []
    for g in range(4):
        rb = reads[g].astype(BF16)
        both = [
            lax.dot_general(rb, state_b[s, g], (((1,), (1,)), ((), ())), preferred_element_type=F32)
            for s in range(2)
        ]
        carried.append(jnp.where(row8 < 4, both[0], both[1]))
    normed = []
    for g in range(4):
        inner = [jnp.sum(reads[g] * down(writes[g], d), axis=1, keepdims=True) for d in range(4)]
        gated = []
        for i in range(2):
            j = 2 * g + i
            f = fresh(j)
            value = conv(rounded(f[0:8, 128:256]), j * 128, tv_v, j * 128)
            mixed = spread(ecum, j) * carried[g][:, i * 128:(i + 1) * 128] + spread(dg, j) * value
            for d in range(4):
                mixed = mixed + (inner[d] * spread(pair_w[d], j)) * down(value, d)
            gated.append(mixed * silu(rounded(f[0:8, 0:128])))
        mean = (jnp.sum(gated[0] * gated[0], axis=1, keepdims=True)
                + jnp.sum(gated[1] * gated[1], axis=1, keepdims=True)) / 256.0
        scale = lax.rsqrt(mean + EPS)
        for i in range(2):
            j = 2 * g + i
            normed.append(gated[i] * scale * ngain_v[:, j * 128:(j + 1) * 128])
    nrm[c] = jnp.concatenate(
        [jnp.concatenate(normed[0:4], axis=1), jnp.concatenate(normed[4:8], axis=1)], axis=0
    ).astype(BF16)

    n_cp = []
    for r in range(1, 8):
        cp = remote(nrm.at[c], nrm.at[c], n_send.at[r], n_recv.at[r], plane(r), tp)
        cp.start()
        n_cp.append(cp)
    for r in range(1, 8):
        g_cp[r].wait_recv()
    pl.semaphore_wait(ready, 3)
    for cp in n_cp:
        cp.wait_recv()

    nall = nrm[...].reshape(128, 512)
    wall = wog[...].reshape(256, 1024)
    turned = (((1,), (1,)), ((), ()))
    p0 = lax.dot_general(wall[:, 0:512], nall, turned, preferred_element_type=F32)
    p1 = lax.dot_general(wall[:, 512:1024], nall, turned, preferred_element_type=F32)
    both = (p0 + pltpu.roll(p1, 120, axis=1)).astype(BF16)
    osend[...] = both.reshape(8, 32, 128)

    owner = lax.div(z, 2)
    slot = tp * 2 + lax.rem(z, 2)
    o_cp = []
    for r in (4, 3, 5, 2, 6, 1, 7):
        cp = remote(osend.at[lax.rem(z + r, 8)], orecv.at[slot], o_send.at[r], o_recv.at[slot], ring(r), owner)
        cp.start()
        o_cp.append(cp)
    straight = remote(osend.at[z], orecv.at[slot], o_send.at[0], o_recv.at[slot], kv, owner)

    @pl.when(owner != tp)
    def _():
        straight.start()

    @pl.when(owner == tp)
    def _():
        orecv[slot] = osend[z]

    for i in range(8):
        mine = jnp.logical_and(tp == i // 2, z == tp * 2 + i % 2)

        @pl.when(jnp.logical_not(mine))
        def _():
            remote(osend.at[0], orecv.at[i], o_send.at[1], o_recv.at[i], kv, tp).wait_recv()

    sums = []
    for q in range(2):
        s4 = orecv[q].astype(F32)
        for x in range(1, 4):
            s4 = s4 + orecv[x * 2 + q].astype(F32)
        sums.append(s4)
    lane32 = lax.broadcasted_iota(jnp.int32, (32, 128), 1)
    merged = jnp.transpose(jnp.where(lax.rem(lane32, 16) < 8, sums[0], pltpu.roll(sums[1], 8, axis=1)))
    ordered = [merged[j * 16 + q * 8:j * 16 + q * 8 + 8, :] for q in range(2) for j in range(8)]
    out_ref[...] = jnp.concatenate(ordered, axis=0).astype(BF16)

    state_cp.wait()
    for cp in acts_cp + w_cp + k_cp + p_cp + e_cp + f_cp + n_cp + o_cp + [g_cp[r] for r in range(1, 8)]:
        cp.wait_send()

    @pl.when(owner != tp)
    def _():
        straight.wait_send()


def per_device(
    hidden_vectors, input_norm_gain, gate_matrix, value_matrix, write_matrix, read_matrix, step_matrix,
    raw_value_rows, raw_write_rows, raw_read_rows, value_filter_taps, write_filter_taps, read_filter_taps,
    step_size_bias, rate_logarithm, direct_path_gain, prior_step_preact, extra_log_decay, accepted, prior_state,
    group_norm_gain, output_matrix,
):
    operands = [
        hidden_vectors, input_norm_gain.reshape(1, 32), gate_matrix, value_matrix, write_matrix, read_matrix,
        step_matrix, raw_value_rows, raw_write_rows, raw_read_rows, value_filter_taps, write_filter_taps,
        read_filter_taps, step_size_bias.reshape(1, 16), rate_logarithm.reshape(1, 16),
        direct_path_gain.reshape(1, 16), prior_step_preact, extra_log_decay, prior_state.reshape(2, 4, 256, 128),
        group_norm_gain.reshape(1, 1024), output_matrix,
    ]
    buffers = [pltpu.VMEM(x.shape, x.dtype) for x in operands]
    dma = pltpu.SemaphoreType.DMA
    scratch = buffers + [
        pltpu.VMEM((256, 512), BF16),
        pltpu.VMEM((8, 32, 384), BF16),
        pltpu.VMEM((256, 384), BF16),
        pltpu.VMEM((256, 128), BF16),
        pltpu.VMEM((512, 256), F32),
        pltpu.VMEM((512, 256), BF16),
        pltpu.VMEM((8, 64, 384), BF16),
        pltpu.VMEM((8, 64, 384), BF16),
        pltpu.VMEM((8, 8, 128), F32),
        pltpu.VMEM((8, 8, 128), F32),
        pltpu.VMEM((64, 384), F32),
        pltpu.VMEM((8, 16, 256), BF16),
        pltpu.VMEM((8, 16, 256), BF16),
        pltpu.VMEM((8, 16, 512), BF16),
        pltpu.VMEM((8, 32, 1024), BF16),
        pltpu.VMEM((8, 32, 128), BF16),
        pltpu.VMEM((8, 32, 128), BF16),
        pltpu.VMEM((8, 2048), F32),
        pltpu.VMEM((2, 4, 256, 128), BF16),
        dma((len(operands),)),
        dma,
    ] + [dma((8,)) for _ in range(18)] + [pltpu.SemaphoreType.REGULAR]
    out, state = pl.pallas_call(
        mixer_kernel,
        out_shape=(
            jax.ShapeDtypeStruct((128, 32), BF16),
            jax.ShapeDtypeStruct((2, 4, 256, 128), F32),
        ),
        in_specs=[pl.BlockSpec(memory_space=pltpu.SMEM)] + [pl.BlockSpec(memory_space=pl.ANY)] * len(operands),
        out_specs=(pl.BlockSpec(memory_space=pltpu.VMEM), pl.BlockSpec(memory_space=pl.ANY)),
        scratch_shapes=scratch,
        compiler_params=pltpu.CompilerParams(
            collective_id=0, has_side_effects=True, vmem_limit_bytes=32 * 1024 * 1024
        ),
        cost_estimate=pl.CostEstimate(flops=10**9, bytes_accessed=4 * 10**6, transcendentals=10**5),
        name="mixer",
    )(accepted, *operands)
    return out, state.reshape(2, 16, 64, 128)


def solution(mesh):
    return jax.shard_map(
        per_device,
        mesh=mesh,
        in_specs=(
            P(None, "kv"),
            P("kv"),
            P("kv", "tp"),
            P("kv", "tp"),
            P("kv", "tp"),
            P("kv", "tp"),
            P("kv", "tp"),
            P("kv", None, "tp"),
            P("kv", None, "tp"),
            P("kv", None, "tp"),
            P(None, "tp"),
            P(None, "tp"),
            P(None, "tp"),
            P("tp"),
            P("tp"),
            P("tp"),
            P("kv", None, "tp"),
            P("kv", None, "tp"),
            P("kv"),
            P("kv", "tp", None, None),
            P("tp"),
            P("tp", "kv"),
        ),
        out_specs=(P("tp", "kv"), P("kv", "tp", None, None)),
        check_vma=False,
    )
```

```python
import jax
import jax.numpy as jnp
from jax import lax
from jax.experimental import pallas as pl
from jax.experimental.pallas import tpu as pltpu
from jax.sharding import PartitionSpec as P

MESH = pl.DeviceIdType.MESH
F32 = jnp.float32
BF16 = jnp.bfloat16
EPS = 1e-6
Z_ORDER = (4, 3, 5, 2, 6, 1, 7, 0)


def silu(x):
    return x / (1.0 + jnp.exp(-x))


def softplus(x):
    return jnp.maximum(x, 0.0) + jnp.log(1.0 + jnp.exp(-jnp.abs(x)))


def mixer_kernel(
    acc_s,
    hid, gain, wg, wv, ww, wr, ws, rawv, raww, rawr, tv, tw, tr, bias, rate, dgain, ppre, extra, prior, ngain, wo,
    out_ref, st_out,
    hid_v, gain_v, wg_v, wv_v, ww_v, wr_v, ws_v, rawv_v, raww_v, rawr_v, tv_v, tw_v, tr_v, bias_v, rate_v, dgain_v,
    ppre_v, extra_v, prior_v, ngain_v, wo_v,
    acts_t, wsend, wblk, kbuf, qbuf, acts_f, acts_b, psend, precv, esend, erecv, fsend, frecv, nrm, wog, osend, orecv,
    base, state_b,
    lsem, osem, s1_send, s1_recv, w_send, w_recv, k_send, k_recv, q_send, q_recv, p_send, p_recv, e_send, e_recv,
    f_send, f_recv, n_send, n_recv, g_send, g_recv, o_send, o_recv, ready,
):
    kv = lax.axis_index("kv")
    tp = lax.axis_index("tp")
    z = lax.div(kv, 8)
    c = lax.rem(kv, 8)

    def plane(r):
        return z * 8 + lax.rem(c + r, 8)

    def ring(r):
        return lax.rem(z + r, 8) * 8 + c

    def remote(src, dst, ssem, rsem, kv_to, tp_to):
        return pltpu.make_async_remote_copy(
            src_ref=src, dst_ref=dst, send_sem=ssem, recv_sem=rsem,
            device_id={"kv": kv_to, "tp": tp_to}, device_id_type=MESH,
        )

    barrier = pltpu.get_barrier_semaphore()
    for r in range(1, 8):
        pl.semaphore_signal(barrier, inc=1, device_id={"kv": plane(r), "tp": tp}, device_id_type=MESH)
    for r in range(1, 8):
        pl.semaphore_signal(barrier, inc=1, device_id={"kv": ring(r), "tp": tp}, device_id_type=MESH)
    for r in range(1, 4):
        pl.semaphore_signal(barrier, inc=1, device_id={"kv": kv, "tp": lax.rem(tp + r, 4)}, device_id_type=MESH)

    pairs = [
        (hid, hid_v), (gain, gain_v), (wg, wg_v), (wv, wv_v), (ww, ww_v), (wr, wr_v), (ws, ws_v), (wo, wo_v),
        (rawv, rawv_v), (raww, raww_v), (rawr, rawr_v), (tv, tv_v), (tw, tw_v), (tr, tr_v), (bias, bias_v),
        (rate, rate_v), (dgain, dgain_v), (ppre, ppre_v), (extra, extra_v), (ngain, ngain_v), (prior, prior_v),
    ]
    loads = [pltpu.make_async_copy(s, d, lsem.at[i]) for i, (s, d) in enumerate(pairs)]
    for cp in loads:
        cp.start()

    own32 = pl.ds(pl.multiple_of(c * 32, 32), 32)
    loads[0].wait()
    loads[1].wait()
    diag = lax.broadcasted_iota(jnp.int32, (32, 32), 0) == lax.broadcasted_iota(jnp.int32, (32, 32), 1)
    gcol = jnp.sum(jnp.where(diag, jnp.broadcast_to(gain_v[...], (32, 32)), 0.0), axis=1, keepdims=True)
    hidden = hid_v[...].astype(F32)
    acts_t[own32, :] = (hidden * gcol).astype(BF16)
    squares = jnp.sum(hidden * hidden, axis=0, keepdims=True)
    qbuf[c] = jnp.concatenate([squares[:, i * 128:(i + 1) * 128] for i in range(4)], axis=0)
    for i in range(2, 7):
        loads[i].wait()
    for j in range(8):
        lane = slice(j * 128, j * 128 + 128)
        wsend[j, :, 0:128] = wg_v[:, lane]
        wsend[j, :, 128:256] = wv_v[:, lane]
        half = slice((j % 4) * 128, (j % 4) * 128 + 128)
        wsend[j, :, 256:384] = ww_v[:, half] if j < 4 else wr_v[:, half]
    wblk[own32, :] = wsend[c]
    kbuf[c] = jnp.concatenate([ws_v[...].astype(F32), jnp.zeros((16, 96), F32)], axis=1).astype(BF16)

    pl.semaphore_wait(barrier, 17)
    for r in range(1, 4):
        pl.semaphore_signal(ready, inc=1, device_id={"kv": kv, "tp": lax.rem(tp + r, 4)}, device_id_type=MESH)

    acts_cp, w_cp, k_cp = [], [], []
    for r in range(1, 8):
        cp = remote(acts_t.at[own32, :], acts_t.at[own32, :], s1_send.at[r], s1_recv.at[r], plane(r), tp)
        cp.start()
        acts_cp.append(cp)
    for r in range(1, 8):
        cp = remote(wsend.at[lax.rem(c + r, 8)], wblk.at[own32, :], w_send.at[r], w_recv.at[r], plane(r), tp)
        cp.start()
        w_cp.append(cp)
    for r in range(1, 8):
        for buf, ssem, rsem in ((kbuf, k_send, k_recv), (qbuf, q_send, q_recv)):
            cp = remote(buf.at[c], buf.at[c], ssem.at[r], rsem.at[r], plane(r), tp)
            cp.start()
            k_cp.append(cp)

    loads[7].wait()
    wog[z] = wo_v[...]
    g_cp = {}
    for r in range(1, 8):
        g_cp[r] = remote(wog.at[z], wog.at[z], g_send.at[r], g_recv.at[r], ring(r), tp)
    for r in (2, 6, 1, 7):
        g_cp[r].start()

    for cp in loads[8:]:
        cp.wait()
    row8 = lax.broadcasted_iota(jnp.int32, (8, 1), 0)
    tok = lax.rem(row8, 4)

    def down(x, d):
        if d == 0:
            return x
        return jnp.where(tok >= d, pltpu.roll(x, d, axis=0), 0.0)

    def up(x, d):
        return jnp.where(tok + d < 4, pltpu.roll(x, 8 - d, axis=0), 0.0)

    def last_conv(raw, taps):
        t = taps[...].astype(F32)
        rows = [raw[k].astype(F32) for k in range(7)]
        parts = []
        for i in range(4):
            total = rows[i] * t[0:1]
            for j in range(1, 4):
                total = total + rows[i + j] * t[j:j + 1]
            parts.append(total)
        return silu(jnp.concatenate([p[s:s + 1] for s in range(2) for p in parts], axis=0))

    def base_conv(raw, taps, lo, hi):
        t = taps[...].astype(F32)
        rows = [raw[k].astype(F32) for k in range(7)]
        second = lax.broadcasted_iota(jnp.int32, (2, 1), 0) == 1
        a = jnp.where(second, acc_s[1], acc_s[0])
        win = []
        for i in range(3):
            w = rows[4 + i]
            for k in range(3, -1, -1):
                w = jnp.where(a == k, rows[k + i], w)
            win.append(w)
        w0, w1, w2 = win
        parts = [w0 * t[0:1] + w1 * t[1:2] + w2 * t[2:3], w1 * t[0:1] + w2 * t[1:2], w2 * t[0:1],
                 jnp.zeros((2, hi - lo), F32)]
        base[:, lo:hi] = jnp.concatenate([p[s:s + 1] for s in range(2) for p in parts], axis=0)

    lastv = last_conv(rawv_v, tv_v)
    lastw = last_conv(raww_v, tw_v)
    base_conv(rawv_v, tv_v, 0, 1024)
    base_conv(raww_v, tw_v, 1024, 1536)
    base_conv(rawr_v, tr_v, 1536, 2048)

    rate_e = -jnp.exp(rate_v[...])
    bias_r = bias_v[...]
    pstep = softplus(jnp.concatenate([ppre_v[0], ppre_v[1]], axis=0) + bias_r)
    pextra = jnp.concatenate([extra_v[0, 0:4], extra_v[1, 0:4]], axis=0)
    nextra = jnp.concatenate([extra_v[0, 4:8], extra_v[1, 4:8]], axis=0)
    limit = jnp.where(row8 < 4, acc_s[0], acc_s[1])
    live = jnp.where(tok < limit, 1.0, 0.0)
    kept = (rate_e * pstep + pextra) * live
    tail = up(kept, 1) + up(kept, 2) + up(kept, 3)
    coef = live * jnp.exp(tail) * pstep
    etot = jnp.exp(kept + tail)
    lane128 = lax.broadcasted_iota(jnp.int32, (8, 128), 1)
    low_half = lane128 < 64

    def spread(e, i):
        a = jnp.broadcast_to(e[:, 2 * i:2 * i + 1], (8, 128))
        b = jnp.broadcast_to(e[:, 2 * i + 1:2 * i + 2], (8, 128))
        return jnp.where(low_half, a, b)

    for g in range(4):
        vals = [lastv[:, (2 * g + i) * 128:(2 * g + i + 1) * 128] * spread(coef, 2 * g + i) for i in range(2)]
        weighted = jnp.concatenate(vals, axis=1)
        lw = lastw[:, g * 128:(g + 1) * 128]
        for s in range(2):
            own_seq = (row8 < 4) if s == 0 else (row8 >= 4)
            added = lax.dot_general(
                weighted, jnp.where(own_seq, lw, 0.0), (((0,), (0,)), ((), ())),
                precision=lax.Precision.HIGHEST, preferred_element_type=F32,
            )
            for i in range(4):
                h = g * 4 + i
                rows = slice(i * 64, i * 64 + 64)
                factor = jnp.broadcast_to(etot[s * 4:s * 4 + 1, h:h + 1], (64, 128))
                new = factor * prior_v[s, g, rows, :] + added[rows, :]
                prior_v[s, g, rows, :] = new
                state_b[s, g, rows, :] = new.astype(BF16)
    state_cp = pltpu.make_async_copy(prior_v, st_out, osem)
    state_cp.start()

    for cp in acts_cp:
        cp.wait_recv()
    for i in range(4):
        block = jnp.transpose(acts_t[:, i * 128:(i + 1) * 128].astype(F32))
        acts_f[i * 128:(i + 1) * 128, :] = block
        acts_b[i * 128:(i + 1) * 128, :] = block.astype(BF16)
    for cp in w_cp:
        cp.wait_recv()
    p_cp, e_cp = [], []
    for r in Z_ORDER:
        zz = lax.rem(z + r, 8)
        part = jnp.dot(
            acts_b[pl.ds(pl.multiple_of(zz * 64, 64), 64), :], wblk[...], preferred_element_type=F32
        ).astype(BF16)
        if r == 0:
            precv[z] = part
        else:
            psend[r] = part
            cp = remote(psend.at[r], precv.at[z], p_send.at[r], p_recv.at[r], ring(r), tp)
            cp.start()
            p_cp.append(cp)
    for cp in k_cp:
        cp.wait_recv()
    own_rows = jnp.concatenate(
        [acts_f[pl.ds(pl.multiple_of(k * 64 + c * 8, 8), 8), :] for k in range(8)], axis=0
    ).astype(BF16)
    step_t = jnp.concatenate([kbuf[j].astype(F32)[:, 0:32] for j in range(8)], axis=1)
    step_t = jnp.concatenate([step_t, jnp.zeros((112, 256), F32)], axis=0).astype(BF16)
    turned = (((1,), (1,)), ((), ()))
    ext = lax.dot_general(own_rows, step_t, turned, preferred_element_type=F32)
    qsum = qbuf[0]
    for j in range(1, 8):
        qsum = qsum + qbuf[j]
    qeven = pltpu.roll(qsum, 64, axis=1)
    for k in range(8):
        row = (qsum if k % 2 else qeven)[k // 2:k // 2 + 1, :]
        esend[k] = jnp.where(low_half, ext[k * 8:k * 8 + 8, :], jnp.broadcast_to(row, (8, 128)))
    erecv[z] = esend[z]
    for r in range(1, 8):
        cp = remote(esend.at[lax.rem(z + r, 8)], erecv.at[z], e_send.at[r], e_recv.at[r], ring(r), tp)
        cp.start()
        e_cp.append(cp)
    for r in (4, 3, 5):
        g_cp[r].start()

    for cp in e_cp:
        cp.wait_recv()
    esum = erecv[0]
    for k in range(1, 8):
        esum = esum + erecv[k]
    own_lane = lane128 == 64 + c * 8 + row8
    inverse = lax.rsqrt(jnp.sum(jnp.where(own_lane, esum, 0.0), axis=1, keepdims=True) / 2048.0 + EPS)
    lane64 = lax.broadcasted_iota(jnp.int32, (64, 128), 1)
    row64 = lax.broadcasted_iota(jnp.int32, (64, 128), 0)
    every = jnp.where(lane64 == 64 + row64, jnp.broadcast_to(esum[0:1, :], (64, 128)), 0.0)
    inverse64 = lax.rsqrt(jnp.sum(every, axis=1, keepdims=True) / 2048.0 + EPS)
    step = softplus(inverse * esum[:, 0:16] + bias_r)
    decay = rate_e * step + nextra
    cum = decay + down(decay, 1) + down(decay, 2) + down(decay, 3)
    pair_w = []
    for d in range(4):
        w = jnp.exp(jnp.minimum(cum - down(cum, d), 0.0)) * down(step, d)
        pair_w.append(jnp.where(tok >= d, w, 0.0))
    ecum = jnp.exp(cum)

    for cp in p_cp:
        cp.wait_recv()
    total = precv[0].astype(F32)
    for k in range(1, 8):
        total = total + precv[k].astype(F32)
    total = total * inverse64
    for j in range(8):
        rows = total[j * 8:j * 8 + 8, :]
        two = jnp.concatenate(
            [rows[:, 0:256], jnp.concatenate([rows[:, 256:384], rows[:, 256:384]], axis=1)], axis=0
        )
        fsend[j] = two.astype(BF16)
    frecv[c] = fsend[c]
    f_cp = []
    for r in range(1, 8):
        cp = remote(fsend.at[lax.rem(c + r, 8)], frecv.at[c], f_send.at[r], f_recv.at[r], plane(r), tp)
        cp.start()
        f_cp.append(cp)

    dg = jnp.broadcast_to(dgain_v[...], (8, 16))
    for cp in f_cp:
        cp.wait_recv()

    def fresh(j):
        return frecv[j].astype(F32)

    def conv(x, lo, taps, at):
        t = taps[:, at:at + 128].astype(F32)
        y = base[:, lo:lo + 128] + x * t[3:4]
        for d in range(1, 4):
            y = y + down(x, d) * t[3 - d:4 - d]
        return silu(y)

    writes, reads = [], []
    for g in range(4):
        writes.append(conv(fresh(g)[8:16, 0:128], 1024 + g * 128, tw_v, g * 128))
        reads.append(conv(fresh(4 + g)[8:16, 0:128], 1536 + g * 128, tr_v, g * 128))
    carried = []
    for g in range(4):
        rb = reads[g].astype(BF16)
        both = [
            lax.dot_general(rb, state_b[s, g], (((1,), (1,)), ((), ())), preferred_element_type=F32)
            for s in range(2)
        ]
        carried.append(jnp.where(row8 < 4, both[0], both[1]))
    normed = []
    for g in range(4):
        inner = [jnp.sum(reads[g] * down(writes[g], d), axis=1, keepdims=True) for d in range(4)]
        gated = []
        for i in range(2):
            j = 2 * g + i
            f = fresh(j)
            value = conv(f[0:8, 128:256], j * 128, tv_v, j * 128)
            mixed = spread(ecum, j) * carried[g][:, i * 128:(i + 1) * 128] + spread(dg, j) * value
            for d in range(4):
                mixed = mixed + (inner[d] * spread(pair_w[d], j)) * down(value, d)
            gated.append(mixed * silu(f[0:8, 0:128]))
        mean = (jnp.sum(gated[0] * gated[0], axis=1, keepdims=True)
                + jnp.sum(gated[1] * gated[1], axis=1, keepdims=True)) / 256.0
        scale = lax.rsqrt(mean + EPS)
        for i in range(2):
            j = 2 * g + i
            normed.append(gated[i] * scale * ngain_v[:, j * 128:(j + 1) * 128])
    nrm[c] = jnp.concatenate(
        [jnp.concatenate(normed[0:4], axis=1), jnp.concatenate(normed[4:8], axis=1)], axis=0
    ).astype(BF16)

    n_cp = []
    for r in range(1, 8):
        cp = remote(nrm.at[c], nrm.at[c], n_send.at[r], n_recv.at[r], plane(r), tp)
        cp.start()
        n_cp.append(cp)
    for r in range(1, 8):
        g_cp[r].wait_recv()
    pl.semaphore_wait(ready, 3)
    for cp in n_cp:
        cp.wait_recv()

    nall = nrm[...].astype(F32)
    wall = wog[...].reshape(256, 1024)
    p = None
    for i in range(2):
        block = nall[:, i * 8:i * 8 + 8, :].reshape(64, 512).astype(BF16)
        q = lax.dot_general(wall[:, i * 512:(i + 1) * 512], block, turned, preferred_element_type=F32)
        p = q if p is None else p + q
    for k in range(8):
        packed = jnp.concatenate([p[k * 32:k * 32 + 16, :], p[k * 32 + 16:k * 32 + 32, :]], axis=1)
        osend[k] = packed.astype(BF16)

    owner = lax.div(z, 2)
    slot = tp * 2 + lax.rem(z, 2)
    o_cp = []
    for r in (4, 3, 5, 2, 6, 1, 7):
        cp = remote(osend.at[lax.rem(z + r, 8)], orecv.at[slot], o_send.at[r], o_recv.at[slot], ring(r), owner)
        cp.start()
        o_cp.append(cp)
    straight = remote(osend.at[z], orecv.at[slot], o_send.at[0], o_recv.at[slot], kv, owner)

    @pl.when(owner != tp)
    def _():
        straight.start()

    @pl.when(owner == tp)
    def _():
        orecv[slot] = osend[z]

    for i in range(8):
        mine = jnp.logical_and(tp == i // 2, z == tp * 2 + i % 2)

        @pl.when(jnp.logical_not(mine))
        def _():
            remote(osend.at[0], orecv.at[i], o_send.at[1], o_recv.at[i], kv, tp).wait_recv()

    sums = []
    for q in range(2):
        s4 = orecv[q].astype(F32)
        for x in range(1, 4):
            s4 = s4 + orecv[x * 2 + q].astype(F32)
        sums.append(s4)
    lane16 = lax.broadcasted_iota(jnp.int32, (16, 128), 1) < 64
    top = jnp.where(lane16, sums[0], pltpu.roll(sums[1], 64, axis=1))
    bottom = jnp.where(lane16, pltpu.roll(sums[0], 64, axis=1), sums[1])
    out_ref[...] = jnp.concatenate([top, bottom], axis=0).astype(BF16)

    state_cp.wait()
    for cp in acts_cp + w_cp + k_cp + p_cp + e_cp + f_cp + n_cp + o_cp + [g_cp[r] for r in range(1, 8)]:
        cp.wait_send()

    @pl.when(owner != tp)
    def _():
        straight.wait_send()


def per_device(
    hidden_vectors, input_norm_gain, gate_matrix, value_matrix, write_matrix, read_matrix, step_matrix,
    raw_value_rows, raw_write_rows, raw_read_rows, value_filter_taps, write_filter_taps, read_filter_taps,
    step_size_bias, rate_logarithm, direct_path_gain, prior_step_preact, extra_log_decay, accepted, prior_state,
    group_norm_gain, output_matrix,
):
    operands = [
        hidden_vectors.T, input_norm_gain.reshape(1, 32), gate_matrix, value_matrix, write_matrix, read_matrix,
        step_matrix.T, raw_value_rows.transpose(1, 0, 2), raw_write_rows.transpose(1, 0, 2),
        raw_read_rows.transpose(1, 0, 2), value_filter_taps, write_filter_taps,
        read_filter_taps, step_size_bias.reshape(1, 16), rate_logarithm.reshape(1, 16),
        direct_path_gain.reshape(1, 16), prior_step_preact, extra_log_decay, prior_state.reshape(2, 4, 256, 128),
        group_norm_gain.reshape(1, 1024), output_matrix.T,
    ]
    buffers = [pltpu.VMEM(x.shape, x.dtype) for x in operands]
    dma = pltpu.SemaphoreType.DMA
    scratch = buffers + [
        pltpu.VMEM((256, 512), BF16),
        pltpu.VMEM((8, 32, 384), BF16),
        pltpu.VMEM((256, 384), BF16),
        pltpu.VMEM((8, 16, 128), BF16),
        pltpu.VMEM((8, 4, 128), F32),
        pltpu.VMEM((512, 256), F32),
        pltpu.VMEM((512, 256), BF16),
        pltpu.VMEM((8, 64, 384), BF16),
        pltpu.VMEM((8, 64, 384), BF16),
        pltpu.VMEM((8, 8, 128), F32),
        pltpu.VMEM((8, 8, 128), F32),
        pltpu.VMEM((8, 16, 256), BF16),
        pltpu.VMEM((8, 16, 256), BF16),
        pltpu.VMEM((8, 16, 512), BF16),
        pltpu.VMEM((8, 32, 1024), BF16),
        pltpu.VMEM((8, 16, 128), BF16),
        pltpu.VMEM((8, 16, 128), BF16),
        pltpu.VMEM((8, 2048), F32),
        pltpu.VMEM((2, 4, 256, 128), BF16),
        dma((len(operands),)),
        dma,
    ] + [dma((8,)) for _ in range(20)] + [pltpu.SemaphoreType.REGULAR]
    out, state = pl.pallas_call(
        mixer_kernel,
        out_shape=(
            jax.ShapeDtypeStruct((32, 128), BF16),
            jax.ShapeDtypeStruct((2, 4, 256, 128), F32),
        ),
        in_specs=[pl.BlockSpec(memory_space=pltpu.SMEM)] + [pl.BlockSpec(memory_space=pl.ANY)] * len(operands),
        out_specs=(pl.BlockSpec(memory_space=pltpu.VMEM), pl.BlockSpec(memory_space=pl.ANY)),
        scratch_shapes=scratch,
        compiler_params=pltpu.CompilerParams(
            collective_id=0, has_side_effects=True, vmem_limit_bytes=67043328
        ),
        cost_estimate=pl.CostEstimate(flops=10**9, bytes_accessed=4 * 10**6, transcendentals=10**5),
        name="mixer",
    )(accepted, *operands)
    return out.T, state.reshape(2, 16, 64, 128)


def solution(mesh):
    return jax.shard_map(
        per_device,
        mesh=mesh,
        in_specs=(
            P(None, "kv"),
            P("kv"),
            P("kv", "tp"),
            P("kv", "tp"),
            P("kv", "tp"),
            P("kv", "tp"),
            P("kv", "tp"),
            P("kv", None, "tp"),
            P("kv", None, "tp"),
            P("kv", None, "tp"),
            P(None, "tp"),
            P(None, "tp"),
            P(None, "tp"),
            P("tp"),
            P("tp"),
            P("tp"),
            P("kv", None, "tp"),
            P("kv", None, "tp"),
            P("kv"),
            P("kv", "tp", None, None),
            P("tp"),
            P("tp", "kv"),
        ),
        out_specs=(P("tp", "kv"), P("kv", "tp", None, None)),
        check_vma=False,
    )
```

```python
import jax
import jax.numpy as jnp
from jax import lax
from jax.experimental import pallas as pl
from jax.experimental.pallas import tpu as pltpu
from jax.sharding import PartitionSpec as P

MESH = pl.DeviceIdType.MESH
F32 = jnp.float32
BF16 = jnp.bfloat16
EPS = 1e-6
PRIOR = 19


def silu(x):
    return x / (1.0 + jnp.exp(-x))


def softplus(x):
    return jnp.maximum(x, 0.0) + jnp.log(1.0 + jnp.exp(-jnp.abs(x)))


def mixer_kernel(
    acc, hid, gain, wg, wv, ww, wr, ws, rawv, raww, rawr, tv, tw, tr, bias, rate, dgain, ppre, extra, prior, ngain, wo,
    out_ref, st_out,
    acc_s, hid_v, gain_v, wg_v, wv_v, ww_v, wr_v, ws_v, rawv_v, raww_v, rawr_v, tv_v, tw_v, tr_v, bias_v, rate_v, dgain_v,
    ppre_v, extra_v, ngain_v, wo_v,
    acts_t, wsend, wblk, kbuf, qbuf, acts_f, acts_b, psend, arecv, bsend, frecv, esend, erecv, nrm, wog, osend, orecv,
    base, state_b,
    lsem, s1_send, s1_recv, w_send, w_recv, k_send, k_recv, q_send, q_recv, a_send, a_recv, p_send, p_recv,
    e_send, e_recv, n_send, n_recv, g_send, g_recv, o_send, o_recv, d_send, d_recv, ready,
):
    kv = lax.axis_index("kv")
    tp = lax.axis_index("tp")
    z = lax.div(kv, 8)
    c = lax.rem(kv, 8)

    def plane(r):
        return z * 8 + lax.rem(c + r, 8)

    def ring(r):
        return lax.rem(z + r, 8) * 8 + c

    def remote(src, dst, ssem, rsem, kv_to, tp_to):
        return pltpu.make_async_remote_copy(
            src_ref=src, dst_ref=dst, send_sem=ssem, recv_sem=rsem,
            device_id={"kv": kv_to, "tp": tp_to}, device_id_type=MESH,
        )

    barrier = pltpu.get_barrier_semaphore()
    for r in range(1, 8):
        pl.semaphore_signal(barrier, inc=1, device_id={"kv": plane(r), "tp": tp}, device_id_type=MESH)
    for r in range(1, 8):
        pl.semaphore_signal(barrier, inc=1, device_id={"kv": ring(r), "tp": tp}, device_id_type=MESH)
    for r in range(1, 4):
        pl.semaphore_signal(barrier, inc=1, device_id={"kv": kv, "tp": lax.rem(tp + r, 4)}, device_id_type=MESH)

    pairs = [
        (acc, acc_s),
        (hid, hid_v), (gain, gain_v), (wg, wg_v), (wv, wv_v), (ww, ww_v), (wr, wr_v), (ws, ws_v), (wo, wo_v),
        (rawv, rawv_v), (raww, raww_v), (rawr, rawr_v), (tv, tv_v), (tw, tw_v), (tr, tr_v), (bias, bias_v),
        (rate, rate_v), (dgain, dgain_v), (ppre, ppre_v), (extra, extra_v), (ngain, ngain_v), (prior, st_out),
    ]
    loads = [pltpu.make_async_copy(s, d, lsem.at[i]) for i, (s, d) in enumerate(pairs)]
    for cp in loads:
        cp.start()

    own32 = pl.ds(pl.multiple_of(c * 32, 32), 32)
    loads[1].wait()
    loads[2].wait()
    diag = lax.broadcasted_iota(jnp.int32, (32, 32), 0) == lax.broadcasted_iota(jnp.int32, (32, 32), 1)
    gcol = jnp.sum(jnp.where(diag, jnp.broadcast_to(gain_v[...], (32, 32)), 0.0), axis=1, keepdims=True)
    hidden = hid_v[...].astype(F32)
    acts_t[own32, :] = (hidden * gcol).astype(BF16)
    squares = jnp.sum(hidden * hidden, axis=0, keepdims=True)
    qbuf[c] = jnp.concatenate([squares[:, i * 128:(i + 1) * 128] for i in range(4)], axis=0)
    for i in range(3, 8):
        loads[i].wait()
    for j in range(8):
        lane = slice(j * 128, j * 128 + 128)
        half = slice((j % 4) * 128, (j % 4) * 128 + 128)
        wsend[j, 0] = ww_v[:, half] if j < 4 else wr_v[:, half]
        wsend[j, 1] = wv_v[:, lane]
        wsend[j, 2] = wg_v[:, lane]
    for t in range(3):
        wblk[t, own32, :] = wsend[c, t]
    kbuf[c] = jnp.concatenate([ws_v[...].astype(F32), jnp.zeros((16, 96), F32)], axis=1).astype(BF16)

    pl.semaphore_wait(barrier, 17)
    for r in range(1, 4):
        pl.semaphore_signal(ready, inc=1, device_id={"kv": kv, "tp": lax.rem(tp + r, 4)}, device_id_type=MESH)

    partner = z * 8 + c + 1 - 2 * lax.rem(c, 2)

    def same_core(i):
        return pl.ds(pl.multiple_of(lax.rem(c + 8 - 2 * i, 8) * 32, 32), 32)

    acts_cp = [
        remote(acts_t.at[own32, :], acts_t.at[own32, :], s1_send.at[i], s1_recv.at[i], plane(2 * i) if i else partner, tp)
        for i in (2, 1, 3, 0)
    ]
    for cp in acts_cp:
        cp.start()
    k_cp, w_cp = [], [[], [], []]
    for r in range(1, 8):
        for buf, ssem, rsem in ((kbuf, k_send, k_recv), (qbuf, q_send, q_recv)):
            cp = remote(buf.at[c], buf.at[c], ssem.at[r], rsem.at[r], plane(r), tp)
            cp.start()
            k_cp.append(cp)
    for t in range(3):
        for r in (4, 3, 5, 2, 6, 1, 7):
            cp = remote(
                wsend.at[lax.rem(c + r, 8), t], wblk.at[t, own32, :], w_send.at[t, r], w_recv.at[t, r], plane(r), tp
            )
            cp.start()
            w_cp[t].append(cp)

    loads[8].wait()
    wog[z] = wo_v[...]
    g_cp = [[], [], [], []]

    def pass_on(hop):
        for way, step in ((0, 1), (1, 7)):
            if hop == 3 and way == 1:
                continue
            at = lax.rem(z + 8 * hop - step * hop, 8)
            cp = remote(wog.at[at], wog.at[at], g_send.at[way, hop], g_recv.at[way, hop], ring(step), tp)
            cp.start()
            g_cp[hop].append(cp)

    pass_on(0)

    for cp in loads[:1] + loads[9:]:
        cp.wait()
    row8 = lax.broadcasted_iota(jnp.int32, (8, 1), 0)
    tok = lax.rem(row8, 4)

    def down(x, d):
        if d == 0:
            return x
        return jnp.where(tok >= d, pltpu.roll(x, d, axis=0), 0.0)

    def up(x, d):
        return jnp.where(tok + d < 4, pltpu.roll(x, 8 - d, axis=0), 0.0)

    def last_conv(raw, taps):
        t = taps[...].astype(F32)
        rows = [raw[k].astype(F32) for k in range(7)]
        parts = []
        for i in range(4):
            total = rows[i] * t[0:1]
            for j in range(1, 4):
                total = total + rows[i + j] * t[j:j + 1]
            parts.append(total)
        return silu(jnp.concatenate([p[s:s + 1] for s in range(2) for p in parts], axis=0))

    def base_conv(raw, taps, lo, hi):
        t = taps[...].astype(F32)
        rows = [raw[k].astype(F32) for k in range(7)]
        second = lax.broadcasted_iota(jnp.int32, (2, 1), 0) == 1
        a = jnp.where(second, acc_s[1], acc_s[0])
        win = []
        for i in range(3):
            w = rows[4 + i]
            for k in range(3, -1, -1):
                w = jnp.where(a == k, rows[k + i], w)
            win.append(w)
        w0, w1, w2 = win
        parts = [w0 * t[0:1] + w1 * t[1:2] + w2 * t[2:3], w1 * t[0:1] + w2 * t[1:2], w2 * t[0:1],
                 jnp.zeros((2, hi - lo), F32)]
        base[:, lo:hi] = jnp.concatenate([p[s:s + 1] for s in range(2) for p in parts], axis=0)

    lastv = last_conv(rawv_v, tv_v)
    lastw = last_conv(raww_v, tw_v)
    base_conv(rawv_v, tv_v, 0, 1024)
    base_conv(raww_v, tw_v, 1024, 1536)
    base_conv(rawr_v, tr_v, 1536, 2048)

    rate_e = -jnp.exp(rate_v[...])
    bias_r = bias_v[...]
    pstep = softplus(jnp.concatenate([ppre_v[0], ppre_v[1]], axis=0) + bias_r)
    pextra = jnp.concatenate([extra_v[0, 0:4], extra_v[1, 0:4]], axis=0)
    nextra = jnp.concatenate([extra_v[0, 4:8], extra_v[1, 4:8]], axis=0)
    limit = jnp.where(row8 < 4, acc_s[0], acc_s[1])
    live = jnp.where(tok < limit, 1.0, 0.0)
    kept = (rate_e * pstep + pextra) * live
    tail = up(kept, 1) + up(kept, 2) + up(kept, 3)
    coef = live * jnp.exp(tail) * pstep
    etot = jnp.exp(kept + tail)
    lane128 = lax.broadcasted_iota(jnp.int32, (8, 128), 1)
    low_half = lane128 < 64

    def spread(e, i):
        a = jnp.broadcast_to(e[:, 2 * i:2 * i + 1], (8, 128))
        b = jnp.broadcast_to(e[:, 2 * i + 1:2 * i + 2], (8, 128))
        return jnp.where(low_half, a, b)

    for g in range(4):
        vals = [lastv[:, (2 * g + i) * 128:(2 * g + i + 1) * 128] * spread(coef, 2 * g + i) for i in range(2)]
        weighted = jnp.concatenate(vals, axis=1)
        lw = lastw[:, g * 128:(g + 1) * 128]
        for s in range(2):
            own_seq = (row8 < 4) if s == 0 else (row8 >= 4)
            added = lax.dot_general(
                weighted, jnp.where(own_seq, lw, 0.0), (((0,), (0,)), ((), ())),
                precision=lax.Precision.HIGHEST, preferred_element_type=F32,
            )
            for i in range(4):
                h = g * 4 + i
                rows = slice(i * 64, i * 64 + 64)
                factor = jnp.broadcast_to(etot[s * 4:s * 4 + 1, h:h + 1], (64, 128))
                new = factor * st_out[s, g, rows, :] + added[rows, :]
                st_out[s, g, rows, :] = new
                state_b[s, g, rows, :] = new.astype(BF16)

    d_cp = []
    for i in (1, 3, 2):
        remote(acts_t.at[own32, :], acts_t.at[own32, :], s1_send.at[i], s1_recv.at[i], partner, tp).wait_recv()
        cp = remote(acts_t.at[same_core(i), :], acts_t.at[same_core(i), :], d_send.at[i], d_recv.at[i], partner, tp)
        cp.start()
        d_cp.append(cp)
    for cp in g_cp[0]:
        cp.wait_recv()
    pass_on(1)
    remote(acts_t.at[own32, :], acts_t.at[own32, :], s1_send.at[0], s1_recv.at[0], partner, tp).wait_recv()
    for cp in d_cp:
        cp.wait_recv()
    for i in range(4):
        block = jnp.transpose(acts_t[:, i * 128:(i + 1) * 128].astype(F32))
        acts_f[i * 128:(i + 1) * 128, :] = block
        acts_b[i * 128:(i + 1) * 128, :] = block.astype(BF16)
    turned = (((1,), (1,)), ((), ()))
    even = lax.rem(z, 2) == 0
    far = lax.rem(z + 2 + 4 * lax.rem(z, 2), 8)
    a_cp, p_cp = [[], [], []], []

    def to_owners(t, src, slot, dz, skip_self):
        for r in range(1 if skip_self else 0, 8):
            cc = lax.rem(c + r, 8)
            cp = remote(
                src.at[cc], frecv.at[t, slot, c], p_send.at[t, slot, r], p_recv.at[t, slot, r],
                lax.rem(z + dz, 8) * 8 + cc, tp,
            )
            cp.start()
            p_cp.append((t, cp))

    for t in range(3):
        for cp in w_cp[t]:
            cp.wait_recv()
        part = jnp.dot(acts_b[...], wblk[t], preferred_element_type=F32)
        psend[t] = part.reshape(8, 8, 8, 128).astype(BF16)
        for kind, away, to in ((2, 4, far * 8 + c), (0, 3, ring(1)), (1, 5, ring(7))):
            cp = remote(
                psend.at[t, lax.rem(z + away, 8)], arecv.at[t, kind], a_send.at[t, kind], a_recv.at[t, kind], to, tp
            )
            cp.start()
            a_cp[t].append(cp)
        to_owners(t, psend.at[t, lax.rem(z + 1, 8)], 1, 1, False)
        to_owners(t, psend.at[t, lax.rem(z + 7, 8)], 2, 7, False)
        to_owners(t, psend.at[t, z], 0, 0, True)
        frecv[t, 0, c] = psend[t, z, c]
    for cp in k_cp:
        cp.wait_recv()
    own_rows = jnp.concatenate(
        [acts_f[pl.ds(pl.multiple_of(k * 64 + c * 8, 8), 8), :] for k in range(8)], axis=0
    ).astype(BF16)
    step_t = jnp.concatenate([kbuf[j].astype(F32)[:, 0:32] for j in range(8)], axis=1)
    step_t = jnp.concatenate([step_t, jnp.zeros((112, 256), F32)], axis=0).astype(BF16)
    ext = lax.dot_general(own_rows, step_t, turned, preferred_element_type=F32)
    qsum = qbuf[0]
    for j in range(1, 8):
        qsum = qsum + qbuf[j]
    qeven = pltpu.roll(qsum, 64, axis=1)
    for k in range(8):
        row = (qsum if k % 2 else qeven)[k // 2:k // 2 + 1, :]
        mixture = jnp.where(low_half, ext[k * 8:k * 8 + 8, :], jnp.broadcast_to(row, (8, 128)))
        high = mixture.astype(BF16).astype(F32)
        rest = (mixture - high).astype(BF16).astype(F32)
        lower = jnp.where(low_half, pltpu.roll(jnp.where(low_half, rest, 0.0), 16, axis=1), rest)
        esend[k] = jnp.where(low_half, high + lower, jnp.where(row8 < 4, high, lower)).astype(BF16)
    erecv[z] = esend[z]
    e_cp = []
    for r in (4, 3, 5, 2, 6, 1, 7):
        cp = remote(esend.at[lax.rem(z + r, 8)], erecv.at[z], e_send.at[r], e_recv.at[r], ring(r), tp)
        cp.start()
        e_cp.append(cp)
    for cp in g_cp[1]:
        cp.wait_recv()
    for t in range(3):
        for cp in a_cp[t]:
            cp.wait_recv()
        extra_block = arecv[t, 2].astype(F32)
        zero_block = jnp.zeros_like(extra_block)
        plus = psend[t, lax.rem(z + 2, 8)].astype(F32) + arecv[t, 0].astype(F32)
        minus = psend[t, lax.rem(z + 6, 8)].astype(F32) + arecv[t, 1].astype(F32)
        bsend[t, 0] = (plus + jnp.where(even, extra_block, zero_block)).astype(BF16)
        bsend[t, 1] = (minus + jnp.where(even, zero_block, extra_block)).astype(BF16)
        to_owners(t, bsend.at[t, 0], 3, 2, False)
        to_owners(t, bsend.at[t, 1], 4, 6, False)
    pass_on(2)

    for cp in e_cp:
        cp.wait_recv()
    esum = erecv[0].astype(F32)
    for k in range(1, 8):
        esum = esum + erecv[k].astype(F32)
    own_lane = lane128 == 64 + c * 8 + row8
    qrow = jnp.broadcast_to(esum[0:1, :] + esum[4:5, :], (8, 128))
    inverse = lax.rsqrt(jnp.sum(jnp.where(own_lane, qrow, 0.0), axis=1, keepdims=True) / 2048.0 + EPS)
    esum = esum + pltpu.roll(esum, 112, axis=1)
    step = softplus(inverse * esum[:, 0:16] + bias_r)
    decay = rate_e * step + nextra
    cum = decay + down(decay, 1) + down(decay, 2) + down(decay, 3)
    pair_w = []
    for d in range(4):
        w = jnp.exp(jnp.minimum(cum - down(cum, d), 0.0)) * down(step, d)
        pair_w.append(jnp.where(tok >= d, w, 0.0))
    ecum = jnp.exp(cum)

    def settle(t):
        for at, cp in p_cp:
            if at == t:
                cp.wait_recv()

    def fresh(t, j):
        x = frecv[t, 0, j].astype(F32)
        for slot in range(1, 5):
            x = x + frecv[t, slot, j].astype(F32)
        return (x * inverse).astype(BF16).astype(F32)

    dg = jnp.broadcast_to(dgain_v[...], (8, 16))
    settle(0)

    def conv(x, lo, taps, at):
        t = taps[:, at:at + 128].astype(F32)
        y = base[:, lo:lo + 128] + x * t[3:4]
        for d in range(1, 4):
            y = y + down(x, d) * t[3 - d:4 - d]
        return silu(y)

    writes = [conv(fresh(0, g), 1024 + g * 128, tw_v, g * 128) for g in range(4)]
    reads = [conv(fresh(0, 4 + g), 1536 + g * 128, tr_v, g * 128) for g in range(4)]
    carried, inner = [], []
    for g in range(4):
        rb = reads[g].astype(BF16)
        both = [
            lax.dot_general(rb, state_b[s, g], turned, preferred_element_type=F32) for s in range(2)
        ]
        carried.append(jnp.where(row8 < 4, both[0], both[1]))
        inner.append([jnp.sum(reads[g] * down(writes[g], d), axis=1, keepdims=True) for d in range(4)])
    settle(1)
    mixed = []
    for j in range(8):
        g, i = j // 2, j % 2
        value = conv(fresh(1, j), j * 128, tv_v, j * 128)
        m = spread(ecum, j) * carried[g][:, i * 128:(i + 1) * 128] + spread(dg, j) * value
        for d in range(4):
            m = m + (inner[g][d] * spread(pair_w[d], j)) * down(value, d)
        mixed.append(m)
    settle(2)
    normed = []
    for g in range(4):
        gated = [mixed[j] * silu(fresh(2, j)) for j in (2 * g, 2 * g + 1)]
        mean = jnp.sum(gated[0] * gated[0] + gated[1] * gated[1], axis=1, keepdims=True) / 256.0
        scale = lax.rsqrt(mean + EPS)
        for i in range(2):
            j = 2 * g + i
            normed.append(gated[i] * scale * ngain_v[:, j * 128:(j + 1) * 128])
    nrm[c] = jnp.concatenate(
        [jnp.concatenate(normed[0:4], axis=1), jnp.concatenate(normed[4:8], axis=1)], axis=0
    ).astype(BF16)

    n_cp = []
    for r in range(1, 8):
        cp = remote(nrm.at[c], nrm.at[c], n_send.at[r], n_recv.at[r], plane(r), tp)
        cp.start()
        n_cp.append(cp)
    for cp in g_cp[2]:
        cp.wait_recv()
    pass_on(3)
    for cp in g_cp[3]:
        cp.wait_recv()
    pl.semaphore_wait(ready, 3)
    for cp in n_cp:
        cp.wait_recv()

    nall = nrm[...].astype(F32)
    wall = wog[...].reshape(256, 1024)
    p = None
    for i in range(2):
        block = nall[:, i * 8:i * 8 + 8, :].reshape(64, 512).astype(BF16)
        q = lax.dot_general(wall[:, i * 512:(i + 1) * 512], block, turned, preferred_element_type=F32)
        p = q if p is None else p + q
    for k in range(8):
        packed = jnp.concatenate([p[k * 32:k * 32 + 16, :], p[k * 32 + 16:k * 32 + 32, :]], axis=1)
        osend[k] = packed.astype(BF16)

    owner = lax.div(z, 2)
    slot = tp * 2 + lax.rem(z, 2)
    o_cp = []
    for r in (4, 3, 5, 2, 6, 1, 7):
        cp = remote(osend.at[lax.rem(z + r, 8)], orecv.at[slot], o_send.at[r], o_recv.at[slot], ring(r), owner)
        cp.start()
        o_cp.append(cp)
    straight = remote(osend.at[z], orecv.at[slot], o_send.at[0], o_recv.at[slot], kv, owner)

    @pl.when(owner != tp)
    def _():
        straight.start()

    @pl.when(owner == tp)
    def _():
        orecv[slot] = osend[z]

    for i in range(8):
        mine = jnp.logical_and(tp == i // 2, z == tp * 2 + i % 2)

        @pl.when(jnp.logical_not(mine))
        def _():
            remote(osend.at[0], orecv.at[i], o_send.at[1], o_recv.at[i], kv, tp).wait_recv()

    sums = []
    for q in range(2):
        s4 = orecv[q].astype(F32)
        for x in range(1, 4):
            s4 = s4 + orecv[x * 2 + q].astype(F32)
        sums.append(s4)
    lane16 = lax.broadcasted_iota(jnp.int32, (16, 128), 1) < 64
    top = jnp.where(lane16, sums[0], pltpu.roll(sums[1], 64, axis=1))
    bottom = jnp.where(lane16, pltpu.roll(sums[0], 64, axis=1), sums[1])
    out_ref[...] = jnp.concatenate([top, bottom], axis=0).astype(BF16)

    for group in [acts_cp, d_cp, k_cp, e_cp, n_cp, o_cp, [cp for _, cp in p_cp]] + w_cp + a_cp + g_cp:
        for cp in group:
            cp.wait_send()

    @pl.when(owner != tp)
    def _():
        straight.wait_send()


def per_device(
    hidden_vectors, input_norm_gain, gate_matrix, value_matrix, write_matrix, read_matrix, step_matrix,
    raw_value_rows, raw_write_rows, raw_read_rows, value_filter_taps, write_filter_taps, read_filter_taps,
    step_size_bias, rate_logarithm, direct_path_gain, prior_step_preact, extra_log_decay, accepted, prior_state,
    group_norm_gain, output_matrix,
):
    operands = [
        accepted, hidden_vectors.T, input_norm_gain.reshape(1, 32), gate_matrix, value_matrix, write_matrix, read_matrix,
        step_matrix.T, raw_value_rows.transpose(1, 0, 2), raw_write_rows.transpose(1, 0, 2),
        raw_read_rows.transpose(1, 0, 2), value_filter_taps, write_filter_taps,
        read_filter_taps, step_size_bias.reshape(1, 16), rate_logarithm.reshape(1, 16),
        direct_path_gain.reshape(1, 16), prior_step_preact, extra_log_decay, prior_state.reshape(2, 4, 256, 128),
        group_norm_gain.reshape(1, 1024), output_matrix.T,
    ]
    buffers = [pltpu.SMEM((2,), jnp.int32)] + [
        pltpu.VMEM(x.shape, x.dtype) for i, x in enumerate(operands) if i not in (0, PRIOR)
    ]
    dma = pltpu.SemaphoreType.DMA
    scratch = buffers + [
        pltpu.VMEM((256, 512), BF16),
        pltpu.VMEM((8, 3, 32, 128), BF16),
        pltpu.VMEM((3, 256, 128), BF16),
        pltpu.VMEM((8, 16, 128), BF16),
        pltpu.VMEM((8, 4, 128), F32),
        pltpu.VMEM((512, 256), F32),
        pltpu.VMEM((512, 256), BF16),
        pltpu.VMEM((3, 8, 8, 8, 128), BF16),
        pltpu.VMEM((3, 3, 8, 8, 128), BF16),
        pltpu.VMEM((3, 2, 8, 8, 128), BF16),
        pltpu.VMEM((3, 5, 8, 8, 128), BF16),
        pltpu.VMEM((8, 8, 128), BF16),
        pltpu.VMEM((8, 8, 128), BF16),
        pltpu.VMEM((8, 16, 512), BF16),
        pltpu.VMEM((8, 32, 1024), BF16),
        pltpu.VMEM((8, 16, 128), BF16),
        pltpu.VMEM((8, 16, 128), BF16),
        pltpu.VMEM((8, 2048), F32),
        pltpu.VMEM((2, 4, 256, 128), BF16),
        dma((len(operands),)),
        dma((4,)), dma((4,)),
        dma((3, 8)), dma((3, 8)),
        dma((8,)), dma((8,)), dma((8,)), dma((8,)),
        dma((3, 3)), dma((3, 3)),
        dma((3, 5, 8)), dma((3, 5, 8)),
        dma((8,)), dma((8,)),
        dma((8,)), dma((8,)),
        dma((2, 4)), dma((2, 4)),
        dma((8,)), dma((8,)),
        dma((4,)), dma((4,)),
        pltpu.SemaphoreType.REGULAR,
    ]
    operands = [pltpu.with_memory_space_constraint(x, pltpu.HBM) for x in operands]
    out, state = pl.pallas_call(
        mixer_kernel,
        out_shape=(
            pltpu.VMEM((32, 128), BF16),
            pltpu.VMEM((2, 4, 256, 128), F32),
        ),
        in_specs=[pl.BlockSpec(memory_space=pl.ANY)] * len(operands),
        out_specs=(pl.BlockSpec(memory_space=pltpu.VMEM), pl.BlockSpec(memory_space=pltpu.VMEM)),
        scratch_shapes=scratch,
        compiler_params=pltpu.CompilerParams(
            collective_id=0, has_side_effects=True, vmem_limit_bytes=32 * 1024 * 1024
        ),
        cost_estimate=pl.CostEstimate(flops=10**9, bytes_accessed=4 * 10**6, transcendentals=10**5),
        name="mixer",
    )(*operands)
    return out.T, state.reshape(2, 16, 64, 128)


def solution(mesh):
    return jax.shard_map(
        per_device,
        mesh=mesh,
        in_specs=(
            P(None, "kv"),
            P("kv"),
            P("kv", "tp"),
            P("kv", "tp"),
            P("kv", "tp"),
            P("kv", "tp"),
            P("kv", "tp"),
            P("kv", None, "tp"),
            P("kv", None, "tp"),
            P("kv", None, "tp"),
            P(None, "tp"),
            P(None, "tp"),
            P(None, "tp"),
            P("tp"),
            P("tp"),
            P("tp"),
            P("kv", None, "tp"),
            P("kv", None, "tp"),
            P("kv"),
            P("kv", "tp", None, None),
            P("tp"),
            P("tp", "kv"),
        ),
        out_specs=(P("tp", "kv"), P("kv", "tp", None, None)),
        check_vma=False,
    )
```

```python
import jax
import jax.numpy as jnp
from jax import lax
from jax.experimental import pallas as pl
from jax.experimental.pallas import tpu as pltpu
from jax.sharding import PartitionSpec as P

MESH = pl.DeviceIdType.MESH
F32 = jnp.float32
BF16 = jnp.bfloat16
EPS = 1e-6
PRIOR = 19


def silu(x):
    return x / (1.0 + jnp.exp(-x))


def softplus(x):
    return jnp.maximum(x, 0.0) + jnp.log(1.0 + jnp.exp(-jnp.abs(x)))


def mixer_kernel(
    acc, hid, gain, wg, wv, ww, wr, ws, rawv, raww, rawr, tv, tw, tr, bias, rate, dgain, ppre, extra, prior, ngain, wo,
    out_ref, st_out,
    acc_s, hid_v, gain_v, wg_v, wv_v, ww_v, wr_v, ws_v, rawv_v, raww_v, rawr_v, tv_v, tw_v, tr_v, bias_v, rate_v, dgain_v,
    ppre_v, extra_v, ngain_v, wo_v,
    acts_t, wsend, wblk, kbuf, qbuf, acts_f, acts_b, psend, arecv, bsend, frecv, esend, erecv, nrm, wog, osend, orecv,
    base, state_b,
    lsem, acts_ssem, acts_rsem, d_ssem, d_rsem, w_ssem, w_rsem, k_ssem, k_rsem, q_ssem, q_rsem, g_ssem, g_rsem,
    a_ssem, a_rsem, p_ssem, p_rsem, h_ssem, h_rsem, e_ssem, e_rsem, n_ssem, n_rsem, o_ssem, o_rsem, ready,
):
    kv = lax.axis_index("kv")
    tp = lax.axis_index("tp")
    z = lax.div(kv, 8)
    c = lax.rem(kv, 8)

    def plane(r):
        return z * 8 + lax.rem(c + r, 8)

    def ring(r):
        return lax.rem(z + r, 8) * 8 + c

    def remote(src, dst, ssem, rsem, kv_to, tp_to):
        return pltpu.make_async_remote_copy(
            src_ref=src, dst_ref=dst, send_sem=ssem, recv_sem=rsem,
            device_id={"kv": kv_to, "tp": tp_to}, device_id_type=MESH,
        )

    def arrived(ref, sem):
        remote(ref, ref, acts_ssem, sem, kv, tp).wait_recv()

    def sent(ref, sem):
        remote(ref, ref, sem, d_rsem, kv, tp).wait_send()

    barrier = pltpu.get_barrier_semaphore()
    for r in range(1, 8):
        pl.semaphore_signal(barrier, inc=1, device_id={"kv": plane(r), "tp": tp}, device_id_type=MESH)
    for r in range(1, 8):
        pl.semaphore_signal(barrier, inc=1, device_id={"kv": ring(r), "tp": tp}, device_id_type=MESH)
    for r in range(1, 4):
        pl.semaphore_signal(barrier, inc=1, device_id={"kv": kv, "tp": lax.rem(tp + r, 4)}, device_id_type=MESH)

    pairs = [
        (acc, acc_s),
        (hid, hid_v), (gain, gain_v), (wg, wg_v), (wv, wv_v), (ww, ww_v), (wr, wr_v), (ws, ws_v), (wo, wo_v),
        (rawv, rawv_v), (raww, raww_v), (rawr, rawr_v), (tv, tv_v), (tw, tw_v), (tr, tr_v), (bias, bias_v),
        (rate, rate_v), (dgain, dgain_v), (ppre, ppre_v), (extra, extra_v), (ngain, ngain_v), (prior, st_out),
    ]
    loads = [pltpu.make_async_copy(s, d, lsem.at[i]) for i, (s, d) in enumerate(pairs)]
    for cp in loads:
        cp.start()

    own32 = pl.ds(pl.multiple_of(c * 32, 32), 32)
    loads[1].wait()
    loads[2].wait()
    diag = lax.broadcasted_iota(jnp.int32, (32, 32), 0) == lax.broadcasted_iota(jnp.int32, (32, 32), 1)
    gcol = jnp.sum(jnp.where(diag, jnp.broadcast_to(gain_v[...], (32, 32)), 0.0), axis=1, keepdims=True)
    hidden = hid_v[...].astype(F32)
    acts_t[own32, :] = (hidden * gcol).astype(BF16)
    squares = jnp.sum(hidden * hidden, axis=0, keepdims=True)
    qbuf[c] = jnp.concatenate([squares[:, i * 128:(i + 1) * 128] for i in range(4)], axis=0)
    for i in range(3, 8):
        loads[i].wait()
    for j in range(8):
        lane = slice(j * 128, j * 128 + 128)
        half = slice((j % 4) * 128, (j % 4) * 128 + 128)
        wsend[j, 0] = ww_v[:, half] if j < 4 else wr_v[:, half]
        wsend[j, 1] = wv_v[:, lane]
        wsend[j, 2] = wg_v[:, lane]
    for t in range(3):
        wblk[t, own32, :] = wsend[c, t]
    kbuf[c] = jnp.concatenate([ws_v[...].astype(F32), jnp.zeros((16, 96), F32)], axis=1).astype(BF16)

    pl.semaphore_wait(barrier, 17)
    for r in range(1, 4):
        pl.semaphore_signal(ready, inc=1, device_id={"kv": kv, "tp": lax.rem(tp + r, 4)}, device_id_type=MESH)

    partner = z * 8 + c + 1 - 2 * lax.rem(c, 2)

    def same_core(i):
        return pl.ds(pl.multiple_of(lax.rem(c + 8 - 2 * i, 8) * 32, 32), 32)

    for i in (2, 1, 3):
        remote(acts_t.at[own32, :], acts_t.at[own32, :], acts_ssem, acts_rsem.at[i], plane(2 * i), tp).start()
    remote(acts_t.at[own32, :], acts_t.at[own32, :], acts_ssem, d_rsem, partner, tp).start()
    for t in range(3):
        for r in (4, 3, 5, 2, 6, 1, 7):
            remote(wsend.at[lax.rem(c + r, 8), t], wblk.at[t, own32, :], w_ssem, w_rsem.at[t], plane(r), tp).start()
        if t == 0:
            for r in (4, 3, 5, 2, 6, 1, 7):
                remote(kbuf.at[c], kbuf.at[c], k_ssem, k_rsem, plane(r), tp).start()
                remote(qbuf.at[c], qbuf.at[c], q_ssem, q_rsem, plane(r), tp).start()

    loads[8].wait()
    wog[z] = wo_v[...]

    def pass_on(hop):
        for way, step in ((0, 1), (1, 7)):
            if hop == 3 and way == 1:
                continue
            at = lax.rem(z + 8 * hop - step * hop, 8)
            remote(wog.at[at], wog.at[at], g_ssem, g_rsem.at[hop], ring(step), tp).start()

    pass_on(0)

    for cp in loads[:1] + loads[9:]:
        cp.wait()
    row8 = lax.broadcasted_iota(jnp.int32, (8, 1), 0)
    tok = lax.rem(row8, 4)

    def down(x, d):
        if d == 0:
            return x
        return jnp.where(tok >= d, pltpu.roll(x, d, axis=0), 0.0)

    def up(x, d):
        return jnp.where(tok + d < 4, pltpu.roll(x, 8 - d, axis=0), 0.0)

    def last_conv(raw, taps):
        t = taps[...].astype(F32)
        rows = [raw[k].astype(F32) for k in range(7)]
        parts = []
        for i in range(4):
            total = rows[i] * t[0:1]
            for j in range(1, 4):
                total = total + rows[i + j] * t[j:j + 1]
            parts.append(total)
        return silu(jnp.concatenate([p[s:s + 1] for s in range(2) for p in parts], axis=0))

    def base_conv(raw, taps, lo, hi):
        t = taps[...].astype(F32)
        rows = [raw[k].astype(F32) for k in range(7)]
        second = lax.broadcasted_iota(jnp.int32, (2, 1), 0) == 1
        a = jnp.where(second, acc_s[1], acc_s[0])
        win = []
        for i in range(3):
            w = rows[4 + i]
            for k in range(3, -1, -1):
                w = jnp.where(a == k, rows[k + i], w)
            win.append(w)
        w0, w1, w2 = win
        parts = [w0 * t[0:1] + w1 * t[1:2] + w2 * t[2:3], w1 * t[0:1] + w2 * t[1:2], w2 * t[0:1],
                 jnp.zeros((2, hi - lo), F32)]
        base[:, lo:hi] = jnp.concatenate([p[s:s + 1] for s in range(2) for p in parts], axis=0)

    lastv = last_conv(rawv_v, tv_v)
    lastw = last_conv(raww_v, tw_v)
    base_conv(rawv_v, tv_v, 0, 1024)
    base_conv(raww_v, tw_v, 1024, 1536)
    base_conv(rawr_v, tr_v, 1536, 2048)

    rate_e = -jnp.exp(rate_v[...])
    bias_r = bias_v[...]
    pstep = softplus(jnp.concatenate([ppre_v[0], ppre_v[1]], axis=0) + bias_r)
    pextra = jnp.concatenate([extra_v[0, 0:4], extra_v[1, 0:4]], axis=0)
    nextra = jnp.concatenate([extra_v[0, 4:8], extra_v[1, 4:8]], axis=0)
    limit = jnp.where(row8 < 4, acc_s[0], acc_s[1])
    live = jnp.where(tok < limit, 1.0, 0.0)
    kept = (rate_e * pstep + pextra) * live
    tail = up(kept, 1) + up(kept, 2) + up(kept, 3)
    coef = live * jnp.exp(tail) * pstep
    etot = jnp.exp(kept + tail)
    lane128 = lax.broadcasted_iota(jnp.int32, (8, 128), 1)
    low_half = lane128 < 64

    def spread(e, i):
        a = jnp.broadcast_to(e[:, 2 * i:2 * i + 1], (8, 128))
        b = jnp.broadcast_to(e[:, 2 * i + 1:2 * i + 2], (8, 128))
        return jnp.where(low_half, a, b)

    for g in range(4):
        vals = [lastv[:, (2 * g + i) * 128:(2 * g + i + 1) * 128] * spread(coef, 2 * g + i) for i in range(2)]
        weighted = jnp.concatenate(vals, axis=1)
        lw = lastw[:, g * 128:(g + 1) * 128]
        for s in range(2):
            own_seq = (row8 < 4) if s == 0 else (row8 >= 4)
            added = lax.dot_general(
                weighted, jnp.where(own_seq, lw, 0.0), (((0,), (0,)), ((), ())),
                precision=lax.Precision.HIGHEST, preferred_element_type=F32,
            )
            for i in range(4):
                h = g * 4 + i
                rows = slice(i * 64, i * 64 + 64)
                factor = jnp.broadcast_to(etot[s * 4:s * 4 + 1, h:h + 1], (64, 128))
                new = factor * st_out[s, g, rows, :] + added[rows, :]
                st_out[s, g, rows, :] = new
                state_b[s, g, rows, :] = new.astype(BF16)

    for i in (1, 3, 2):
        arrived(acts_t.at[own32, :], acts_rsem.at[i])
        remote(acts_t.at[same_core(i), :], acts_t.at[same_core(i), :], d_ssem, d_rsem, partner, tp).start()
    arrived(wog.at[0:2], g_rsem.at[0])
    pass_on(1)
    arrived(acts_t.at[0:128, :], d_rsem)
    for i in range(4):
        block = jnp.transpose(acts_t[:, i * 128:(i + 1) * 128].astype(F32))
        acts_f[i * 128:(i + 1) * 128, :] = block
        acts_b[i * 128:(i + 1) * 128, :] = block.astype(BF16)
    turned = (((1,), (1,)), ((), ()))
    even = lax.rem(z, 2) == 0
    far = lax.rem(z + 2 + 4 * lax.rem(z, 2), 8)

    def to_owners(src, t, slot, dz, ssem, rsem):
        for r in range(0 if dz else 1, 8):
            cc = lax.rem(c + r, 8)
            remote(src.at[cc], frecv.at[t, slot, c], ssem, rsem, lax.rem(z + dz, 8) * 8 + cc, tp).start()

    for t in range(3):
        arrived(wblk.at[t, 0:224, :], w_rsem.at[t])
        part = jnp.dot(acts_b[...], wblk[t], preferred_element_type=F32)
        psend[t] = part.reshape(8, 8, 8, 128).astype(BF16)
        for kind, away, to in ((2, 4, far * 8 + c), (0, 3, ring(1)), (1, 5, ring(7))):
            remote(psend.at[t, lax.rem(z + away, 8)], arecv.at[t, kind], a_ssem, a_rsem.at[t], to, tp).start()
        to_owners(psend.at[t, lax.rem(z + 1, 8)], t, 1, 1, p_ssem, p_rsem.at[t])
        to_owners(psend.at[t, lax.rem(z + 7, 8)], t, 2, 7, p_ssem, p_rsem.at[t])
        to_owners(psend.at[t, z], t, 0, 0, h_ssem, h_rsem.at[t])
        frecv[t, 0, c] = psend[t, z, c]
    arrived(kbuf.at[0:7], k_rsem)
    arrived(qbuf.at[0:7], q_rsem)
    own_rows = jnp.concatenate(
        [acts_f[pl.ds(pl.multiple_of(k * 64 + c * 8, 8), 8), :] for k in range(8)], axis=0
    ).astype(BF16)
    step_t = jnp.concatenate([kbuf[j].astype(F32)[:, 0:32] for j in range(8)], axis=1)
    step_t = jnp.concatenate([step_t, jnp.zeros((112, 256), F32)], axis=0).astype(BF16)
    ext = lax.dot_general(own_rows, step_t, turned, preferred_element_type=F32)
    qsum = qbuf[0]
    for j in range(1, 8):
        qsum = qsum + qbuf[j]
    qeven = pltpu.roll(qsum, 64, axis=1)
    for k in range(8):
        row = (qsum if k % 2 else qeven)[k // 2:k // 2 + 1, :]
        mixture = jnp.where(low_half, ext[k * 8:k * 8 + 8, :], jnp.broadcast_to(row, (8, 128)))
        high = mixture.astype(BF16).astype(F32)
        rest = (mixture - high).astype(BF16).astype(F32)
        lower = jnp.where(low_half, pltpu.roll(jnp.where(low_half, rest, 0.0), 16, axis=1), rest)
        esend[k] = jnp.where(low_half, high + lower, jnp.where(row8 < 4, high, lower)).astype(BF16)
    erecv[z] = esend[z]
    for r in (4, 3, 5, 2, 6, 1, 7):
        remote(esend.at[lax.rem(z + r, 8)], erecv.at[z], e_ssem, e_rsem, ring(r), tp).start()
    arrived(wog.at[0:2], g_rsem.at[1])
    for t in range(3):
        arrived(arecv.at[t], a_rsem.at[t])
        extra_block = arecv[t, 2].astype(F32)
        zero_block = jnp.zeros_like(extra_block)
        plus = psend[t, lax.rem(z + 2, 8)].astype(F32) + arecv[t, 0].astype(F32)
        minus = psend[t, lax.rem(z + 6, 8)].astype(F32) + arecv[t, 1].astype(F32)
        bsend[t, 0] = (plus + jnp.where(even, extra_block, zero_block)).astype(BF16)
        bsend[t, 1] = (minus + jnp.where(even, zero_block, extra_block)).astype(BF16)
        to_owners(bsend.at[t, 0], t, 3, 2, p_ssem, p_rsem.at[t])
        to_owners(bsend.at[t, 1], t, 4, 6, p_ssem, p_rsem.at[t])
    pass_on(2)

    arrived(erecv.at[0:7], e_rsem)
    esum = erecv[0].astype(F32)
    for k in range(1, 8):
        esum = esum + erecv[k].astype(F32)
    own_lane = lane128 == 64 + c * 8 + row8
    qrow = jnp.broadcast_to(esum[0:1, :] + esum[4:5, :], (8, 128))
    inverse = lax.rsqrt(jnp.sum(jnp.where(own_lane, qrow, 0.0), axis=1, keepdims=True) / 2048.0 + EPS)
    esum = esum + pltpu.roll(esum, 112, axis=1)
    step = softplus(inverse * esum[:, 0:16] + bias_r)
    decay = rate_e * step + nextra
    cum = decay + down(decay, 1) + down(decay, 2) + down(decay, 3)
    pair_w = []
    for d in range(4):
        w = jnp.exp(jnp.minimum(cum - down(cum, d), 0.0)) * down(step, d)
        pair_w.append(jnp.where(tok >= d, w, 0.0))
    ecum = jnp.exp(cum)

    def settle(t):
        arrived(frecv.at[t, 1:5], p_rsem.at[t])
        arrived(frecv.at[t, 0, 0:7], h_rsem.at[t])

    def fresh(t, j):
        x = frecv[t, 0, j].astype(F32)
        for slot in range(1, 5):
            x = x + frecv[t, slot, j].astype(F32)
        return (x * inverse).astype(BF16).astype(F32)

    dg = jnp.broadcast_to(dgain_v[...], (8, 16))
    settle(0)

    def conv(x, lo, taps, at):
        t = taps[:, at:at + 128].astype(F32)
        y = base[:, lo:lo + 128] + x * t[3:4]
        for d in range(1, 4):
            y = y + down(x, d) * t[3 - d:4 - d]
        return silu(y)

    writes = [conv(fresh(0, g), 1024 + g * 128, tw_v, g * 128) for g in range(4)]
    reads = [conv(fresh(0, 4 + g), 1536 + g * 128, tr_v, g * 128) for g in range(4)]
    carried, inner = [], []
    for g in range(4):
        rb = reads[g].astype(BF16)
        both = [
            lax.dot_general(rb, state_b[s, g], turned, preferred_element_type=F32) for s in range(2)
        ]
        carried.append(jnp.where(row8 < 4, both[0], both[1]))
        inner.append([jnp.sum(reads[g] * down(writes[g], d), axis=1, keepdims=True) for d in range(4)])
    settle(1)
    mixed = []
    for j in range(8):
        g, i = j // 2, j % 2
        value = conv(fresh(1, j), j * 128, tv_v, j * 128)
        m = spread(ecum, j) * carried[g][:, i * 128:(i + 1) * 128] + spread(dg, j) * value
        for d in range(4):
            m = m + (inner[g][d] * spread(pair_w[d], j)) * down(value, d)
        mixed.append(m)
    settle(2)
    normed = []
    for g in range(4):
        gated = [mixed[j] * silu(fresh(2, j)) for j in (2 * g, 2 * g + 1)]
        mean = jnp.sum(gated[0] * gated[0] + gated[1] * gated[1], axis=1, keepdims=True) / 256.0
        scale = lax.rsqrt(mean + EPS)
        for i in range(2):
            j = 2 * g + i
            normed.append(gated[i] * scale * ngain_v[:, j * 128:(j + 1) * 128])
    nrm[c] = jnp.concatenate(
        [jnp.concatenate(normed[0:4], axis=1), jnp.concatenate(normed[4:8], axis=1)], axis=0
    ).astype(BF16)

    for r in (4, 3, 5, 2, 6, 1, 7):
        remote(nrm.at[c], nrm.at[c], n_ssem, n_rsem, plane(r), tp).start()
    arrived(wog.at[0:2], g_rsem.at[2])
    pass_on(3)
    arrived(wog.at[0], g_rsem.at[3])
    pl.semaphore_wait(ready, 3)
    arrived(nrm.at[0:7], n_rsem)

    nall = nrm[...].astype(F32)
    wall = wog[...].reshape(256, 1024)
    p = None
    for i in range(2):
        block = nall[:, i * 8:i * 8 + 8, :].reshape(64, 512).astype(BF16)
        q = lax.dot_general(wall[:, i * 512:(i + 1) * 512], block, turned, preferred_element_type=F32)
        p = q if p is None else p + q
    for k in range(8):
        packed = jnp.concatenate([p[k * 32:k * 32 + 16, :], p[k * 32 + 16:k * 32 + 32, :]], axis=1)
        osend[k] = packed.astype(BF16)

    owner = lax.div(z, 2)
    slot = tp * 2 + lax.rem(z, 2)
    for r in (4, 3, 5, 2, 6, 1, 7):
        remote(osend.at[lax.rem(z + r, 8)], orecv.at[slot], o_ssem, o_rsem, ring(r), owner).start()

    @pl.when(owner != tp)
    def _():
        remote(osend.at[z], orecv.at[slot], o_ssem, o_rsem, kv, owner).start()
        arrived(orecv.at[0:8], o_rsem)

    @pl.when(owner == tp)
    def _():
        orecv[slot] = osend[z]
        arrived(orecv.at[0:7], o_rsem)

    sums = []
    for q in range(2):
        s4 = orecv[q].astype(F32)
        for x in range(1, 4):
            s4 = s4 + orecv[x * 2 + q].astype(F32)
        sums.append(s4)
    lane16 = lax.broadcasted_iota(jnp.int32, (16, 128), 1) < 64
    top = jnp.where(lane16, sums[0], pltpu.roll(sums[1], 64, axis=1))
    bottom = jnp.where(lane16, pltpu.roll(sums[0], 64, axis=1), sums[1])
    out_ref[...] = jnp.concatenate([top, bottom], axis=0).astype(BF16)

    for ref, sem in (
        (acts_t.at[0:128, :], acts_ssem), (acts_t.at[0:96, :], d_ssem), (wsend.at[0:7], w_ssem),
        (kbuf.at[0:7], k_ssem), (qbuf.at[0:7], q_ssem), (wog.at[0:7], g_ssem), (arecv, a_ssem),
        (frecv.at[:, 1:5], p_ssem), (frecv.at[:, 0, 0:7], h_ssem), (erecv.at[0:7], e_ssem), (nrm.at[0:7], n_ssem),
    ):
        sent(ref, sem)

    @pl.when(owner != tp)
    def _():
        sent(osend.at[0:8], o_ssem)

    @pl.when(owner == tp)
    def _():
        sent(osend.at[0:7], o_ssem)


def per_device(
    hidden_vectors, input_norm_gain, gate_matrix, value_matrix, write_matrix, read_matrix, step_matrix,
    raw_value_rows, raw_write_rows, raw_read_rows, value_filter_taps, write_filter_taps, read_filter_taps,
    step_size_bias, rate_logarithm, direct_path_gain, prior_step_preact, extra_log_decay, accepted, prior_state,
    group_norm_gain, output_matrix,
):
    operands = [
        accepted, hidden_vectors.T, input_norm_gain.reshape(1, 32), gate_matrix, value_matrix, write_matrix, read_matrix,
        step_matrix.T, raw_value_rows.transpose(1, 0, 2), raw_write_rows.transpose(1, 0, 2),
        raw_read_rows.transpose(1, 0, 2), value_filter_taps, write_filter_taps,
        read_filter_taps, step_size_bias.reshape(1, 16), rate_logarithm.reshape(1, 16),
        direct_path_gain.reshape(1, 16), prior_step_preact, extra_log_decay, prior_state.reshape(2, 4, 256, 128),
        group_norm_gain.reshape(1, 1024), output_matrix.T,
    ]
    buffers = [pltpu.SMEM((2,), jnp.int32)] + [
        pltpu.VMEM(x.shape, x.dtype) for i, x in enumerate(operands) if i not in (0, PRIOR)
    ]
    dma = pltpu.SemaphoreType.DMA
    scratch = buffers + [
        pltpu.VMEM((256, 512), BF16),
        pltpu.VMEM((8, 3, 32, 128), BF16),
        pltpu.VMEM((3, 256, 128), BF16),
        pltpu.VMEM((8, 16, 128), BF16),
        pltpu.VMEM((8, 4, 128), F32),
        pltpu.VMEM((512, 256), F32),
        pltpu.VMEM((512, 256), BF16),
        pltpu.VMEM((3, 8, 8, 8, 128), BF16),
        pltpu.VMEM((3, 3, 8, 8, 128), BF16),
        pltpu.VMEM((3, 2, 8, 8, 128), BF16),
        pltpu.VMEM((3, 5, 8, 8, 128), BF16),
        pltpu.VMEM((8, 8, 128), BF16),
        pltpu.VMEM((8, 8, 128), BF16),
        pltpu.VMEM((8, 16, 512), BF16),
        pltpu.VMEM((8, 32, 1024), BF16),
        pltpu.VMEM((8, 16, 128), BF16),
        pltpu.VMEM((8, 16, 128), BF16),
        pltpu.VMEM((8, 2048), F32),
        pltpu.VMEM((2, 4, 256, 128), BF16),
        dma((len(operands),)),
        dma, dma((4,)), dma, dma, dma, dma((3,)), dma, dma, dma, dma, dma, dma((4,)),
        dma, dma((3,)), dma, dma((3,)), dma, dma((3,)), dma, dma, dma, dma, dma, dma,
        pltpu.SemaphoreType.REGULAR,
    ]
    operands = [pltpu.with_memory_space_constraint(x, pltpu.HBM) for x in operands]
    out, state = pl.pallas_call(
        mixer_kernel,
        out_shape=(
            pltpu.VMEM((32, 128), BF16),
            pltpu.VMEM((2, 4, 256, 128), F32),
        ),
        in_specs=[pl.BlockSpec(memory_space=pl.ANY)] * len(operands),
        out_specs=(pl.BlockSpec(memory_space=pltpu.VMEM), pl.BlockSpec(memory_space=pltpu.VMEM)),
        scratch_shapes=scratch,
        compiler_params=pltpu.CompilerParams(
            collective_id=0, has_side_effects=True, vmem_limit_bytes=32 * 1024 * 1024
        ),
        cost_estimate=pl.CostEstimate(flops=10**9, bytes_accessed=4 * 10**6, transcendentals=10**5),
        name="mixer",
    )(*operands)
    return out.T, state.reshape(2, 16, 64, 128)


def solution(mesh):
    return jax.shard_map(
        per_device,
        mesh=mesh,
        in_specs=(
            P(None, "kv"),
            P("kv"),
            P("kv", "tp"),
            P("kv", "tp"),
            P("kv", "tp"),
            P("kv", "tp"),
            P("kv", "tp"),
            P("kv", None, "tp"),
            P("kv", None, "tp"),
            P("kv", None, "tp"),
            P(None, "tp"),
            P(None, "tp"),
            P(None, "tp"),
            P("tp"),
            P("tp"),
            P("tp"),
            P("kv", None, "tp"),
            P("kv", None, "tp"),
            P("kv"),
            P("kv", "tp", None, None),
            P("tp"),
            P("tp", "kv"),
        ),
        out_specs=(P("tp", "kv"), P("kv", "tp", None, None)),
        check_vma=False,
    )
```

```python
import jax
import jax.numpy as jnp
from jax import lax
from jax.experimental import pallas as pl
from jax.experimental.pallas import tpu as pltpu
from jax.sharding import PartitionSpec as P

MESH = pl.DeviceIdType.MESH
F32 = jnp.float32
BF16 = jnp.bfloat16
EPS = 1e-6
PRIOR = 19


def silu(x):
    return x / (1.0 + jnp.exp(-x))


def softplus(x):
    return jnp.maximum(x, 0.0) + jnp.log(1.0 + jnp.exp(-jnp.abs(x)))


def mixer_kernel(
    acc, hid, gain, wg, wv, ww, wr, ws, rawv, raww, rawr, tv, tw, tr, bias, rate, dgain, ppre, extra, prior, ngain, wo,
    out_ref, st_out,
    acc_s, hid_v, gain_v, wg_v, wv_v, ww_v, wr_v, ws_v, rawv_v, raww_v, rawr_v, tv_v, tw_v, tr_v, bias_v, rate_v, dgain_v,
    ppre_v, extra_v, ngain_v, wo_v,
    acts_t, wsend, wblk, kbuf, qbuf, acts_f, acts_b, psend, arecv, bsend, frecv, esend, erecv, efar, nrm, wog, osend, orecv,
    base, state_b,
    lsem, acts_ssem, acts_rsem, d_ssem, d_rsem, w_ssem, w_rsem, k_ssem, k_rsem, q_ssem, q_rsem, g_ssem, g_rsem,
    a_ssem, a_rsem, p_ssem, p_rsem, h_ssem, h_rsem, e_ssem, e_rsem, x_ssem, x_rsem, n_ssem, n_rsem, o_ssem, o_rsem, ready,
):
    kv = lax.axis_index("kv")
    tp = lax.axis_index("tp")
    z = lax.div(kv, 8)
    c = lax.rem(kv, 8)

    def plane(r):
        return z * 8 + lax.rem(c + r, 8)

    def ring(r):
        return lax.rem(z + r, 8) * 8 + c

    def remote(src, dst, ssem, rsem, kv_to, tp_to):
        return pltpu.make_async_remote_copy(
            src_ref=src, dst_ref=dst, send_sem=ssem, recv_sem=rsem,
            device_id={"kv": kv_to, "tp": tp_to}, device_id_type=MESH,
        )

    def arrived(ref, sem):
        remote(ref, ref, acts_ssem, sem, kv, tp).wait_recv()

    def sent(ref, sem):
        remote(ref, ref, sem, d_rsem, kv, tp).wait_send()

    barrier = pltpu.get_barrier_semaphore()
    for r in range(1, 8):
        pl.semaphore_signal(barrier, inc=1, device_id={"kv": plane(r), "tp": tp}, device_id_type=MESH)
    for r in (1, 7):
        pl.semaphore_signal(barrier, inc=1, device_id={"kv": ring(r), "tp": tp}, device_id_type=MESH)
    for r in range(1, 4):
        pl.semaphore_signal(barrier, inc=1, device_id={"kv": kv, "tp": lax.rem(tp + r, 4)}, device_id_type=MESH)

    pairs = [
        (acc, acc_s),
        (hid, hid_v), (gain, gain_v), (wg, wg_v), (wv, wv_v), (ww, ww_v), (wr, wr_v), (ws, ws_v), (wo, wo_v),
        (rawv, rawv_v), (raww, raww_v), (rawr, rawr_v), (tv, tv_v), (tw, tw_v), (tr, tr_v), (bias, bias_v),
        (rate, rate_v), (dgain, dgain_v), (ppre, ppre_v), (extra, extra_v), (ngain, ngain_v), (prior, st_out),
    ]
    loads = [pltpu.make_async_copy(s, d, lsem.at[i]) for i, (s, d) in enumerate(pairs)]
    for cp in loads:
        cp.start()

    own32 = pl.ds(pl.multiple_of(c * 32, 32), 32)
    loads[1].wait()
    loads[2].wait()
    diag = lax.broadcasted_iota(jnp.int32, (32, 32), 0) == lax.broadcasted_iota(jnp.int32, (32, 32), 1)
    gcol = jnp.sum(jnp.where(diag, jnp.broadcast_to(gain_v[...], (32, 32)), 0.0), axis=1, keepdims=True)
    hidden = hid_v[...].astype(F32)
    acts_t[own32, :] = (hidden * gcol).astype(BF16)
    squares = jnp.sum(hidden * hidden, axis=0, keepdims=True)
    qbuf[c] = jnp.concatenate([squares[:, i * 128:(i + 1) * 128] for i in range(4)], axis=0)
    for i in range(3, 8):
        loads[i].wait()
    for j in range(8):
        lane = slice(j * 128, j * 128 + 128)
        half = slice((j % 4) * 128, (j % 4) * 128 + 128)
        wsend[j, 0] = ww_v[:, half] if j < 4 else wr_v[:, half]
        wsend[j, 1] = wv_v[:, lane]
        wsend[j, 2] = wg_v[:, lane]
    for t in range(3):
        wblk[t, own32, :] = wsend[c, t]
    kbuf[c] = jnp.concatenate([ws_v[...].astype(F32), jnp.zeros((16, 96), F32)], axis=1).astype(BF16)

    pl.semaphore_wait(barrier, 12)

    partner = z * 8 + c + 1 - 2 * lax.rem(c, 2)

    def same_core(i):
        return pl.ds(pl.multiple_of(lax.rem(c + 8 - 2 * i, 8) * 32, 32), 32)

    for i in (2, 1, 3):
        remote(acts_t.at[own32, :], acts_t.at[own32, :], acts_ssem, acts_rsem.at[i], plane(2 * i), tp).start()
    remote(acts_t.at[own32, :], acts_t.at[own32, :], acts_ssem, d_rsem, partner, tp).start()
    for t in range(3):
        for r in (4, 3, 5, 2, 6, 1, 7):
            remote(wsend.at[lax.rem(c + r, 8), t], wblk.at[t, own32, :], w_ssem, w_rsem.at[t], plane(r), tp).start()
        if t == 0:
            for r in (4, 3, 5, 2, 6, 1, 7):
                remote(kbuf.at[c], kbuf.at[c], k_ssem, k_rsem, plane(r), tp).start()
                remote(qbuf.at[c], qbuf.at[c], q_ssem, q_rsem, plane(r), tp).start()

    loads[8].wait()
    wog[z] = wo_v[...]

    def pass_on(hop):
        for way, step in ((0, 1), (1, 7)):
            if hop == 3 and way == 1:
                continue
            at = lax.rem(z + 8 * hop - step * hop, 8)
            remote(wog.at[at], wog.at[at], g_ssem, g_rsem.at[hop], ring(step), tp).start()

    pass_on(0)

    for cp in loads[:1] + loads[9:]:
        cp.wait()
    row8 = lax.broadcasted_iota(jnp.int32, (8, 1), 0)
    tok = lax.rem(row8, 4)

    def down(x, d):
        if d == 0:
            return x
        return jnp.where(tok >= d, pltpu.roll(x, d, axis=0), 0.0)

    def up(x, d):
        return jnp.where(tok + d < 4, pltpu.roll(x, 8 - d, axis=0), 0.0)

    def last_conv(raw, taps):
        t = taps[...].astype(F32)
        rows = [raw[k].astype(F32) for k in range(7)]
        parts = []
        for i in range(4):
            total = rows[i] * t[0:1]
            for j in range(1, 4):
                total = total + rows[i + j] * t[j:j + 1]
            parts.append(total)
        return silu(jnp.concatenate([p[s:s + 1] for s in range(2) for p in parts], axis=0))

    def base_conv(raw, taps, lo, hi):
        t = taps[...].astype(F32)
        rows = [raw[k].astype(F32) for k in range(7)]
        second = lax.broadcasted_iota(jnp.int32, (2, 1), 0) == 1
        a = jnp.where(second, acc_s[1], acc_s[0])
        win = []
        for i in range(3):
            w = rows[4 + i]
            for k in range(3, -1, -1):
                w = jnp.where(a == k, rows[k + i], w)
            win.append(w)
        w0, w1, w2 = win
        parts = [w0 * t[0:1] + w1 * t[1:2] + w2 * t[2:3], w1 * t[0:1] + w2 * t[1:2], w2 * t[0:1],
                 jnp.zeros((2, hi - lo), F32)]
        base[:, lo:hi] = jnp.concatenate([p[s:s + 1] for s in range(2) for p in parts], axis=0)

    lastv = last_conv(rawv_v, tv_v)
    lastw = last_conv(raww_v, tw_v)
    base_conv(rawv_v, tv_v, 0, 1024)
    base_conv(raww_v, tw_v, 1024, 1536)
    base_conv(rawr_v, tr_v, 1536, 2048)

    rate_e = -jnp.exp(rate_v[...])
    bias_r = bias_v[...]
    pstep = softplus(jnp.concatenate([ppre_v[0], ppre_v[1]], axis=0) + bias_r)
    pextra = jnp.concatenate([extra_v[0, 0:4], extra_v[1, 0:4]], axis=0)
    nextra = jnp.concatenate([extra_v[0, 4:8], extra_v[1, 4:8]], axis=0)
    limit = jnp.where(row8 < 4, acc_s[0], acc_s[1])
    live = jnp.where(tok < limit, 1.0, 0.0)
    kept = (rate_e * pstep + pextra) * live
    tail = up(kept, 1) + up(kept, 2) + up(kept, 3)
    coef = live * jnp.exp(tail) * pstep
    etot = jnp.exp(kept + tail)
    lane128 = lax.broadcasted_iota(jnp.int32, (8, 128), 1)
    low_half = lane128 < 64

    def spread(e, i):
        a = jnp.broadcast_to(e[:, 2 * i:2 * i + 1], (8, 128))
        b = jnp.broadcast_to(e[:, 2 * i + 1:2 * i + 2], (8, 128))
        return jnp.where(low_half, a, b)

    for g in range(4):
        vals = [lastv[:, (2 * g + i) * 128:(2 * g + i + 1) * 128] * spread(coef, 2 * g + i) for i in range(2)]
        weighted = jnp.concatenate(vals, axis=1)
        lw = lastw[:, g * 128:(g + 1) * 128]
        for s in range(2):
            own_seq = (row8 < 4) if s == 0 else (row8 >= 4)
            added = lax.dot_general(
                weighted, jnp.where(own_seq, lw, 0.0), (((0,), (0,)), ((), ())),
                precision=lax.Precision.HIGHEST, preferred_element_type=F32,
            )
            for i in range(4):
                h = g * 4 + i
                rows = slice(i * 64, i * 64 + 64)
                factor = jnp.broadcast_to(etot[s * 4:s * 4 + 1, h:h + 1], (64, 128))
                new = factor * st_out[s, g, rows, :] + added[rows, :]
                st_out[s, g, rows, :] = new
                state_b[s, g, rows, :] = new.astype(BF16)

    for i in (1, 3, 2):
        arrived(acts_t.at[own32, :], acts_rsem.at[i])
        remote(acts_t.at[same_core(i), :], acts_t.at[same_core(i), :], d_ssem, d_rsem, partner, tp).start()
    arrived(wog.at[0:2], g_rsem.at[0])
    pass_on(1)
    arrived(acts_t.at[0:128, :], d_rsem)
    for i in range(4):
        block = jnp.transpose(acts_t[:, i * 128:(i + 1) * 128].astype(F32))
        acts_f[i * 128:(i + 1) * 128, :] = block
        acts_b[i * 128:(i + 1) * 128, :] = block.astype(BF16)
    turned = (((1,), (1,)), ((), ()))
    even = lax.rem(z, 2) == 0
    far = lax.rem(z + 2 + 4 * lax.rem(z, 2), 8)

    def to_owners(src, t, slot, dz, ssem, rsem):
        for r in range(0 if dz else 1, 8):
            cc = lax.rem(c + r, 8)
            remote(src.at[cc], frecv.at[t, slot, c], ssem, rsem, lax.rem(z + dz, 8) * 8 + cc, tp).start()

    def token_block(away):
        return acts_b[pl.ds(pl.multiple_of(lax.rem(z + away, 8) * 64, 64), 64), :]

    lhs = jnp.concatenate([token_block(away) for away in (4, 3, 5)], axis=0)
    for t in range(3):
        arrived(wblk.at[t, 0:224, :], w_rsem.at[t])
        part = jnp.dot(lhs, wblk[t], preferred_element_type=F32)
        for i, (kind, away, to) in enumerate(((2, 4, far * 8 + c), (0, 3, ring(1)), (1, 5, ring(7)))):
            zz = lax.rem(z + away, 8)
            psend[t, zz] = part[i * 64:i * 64 + 64, :].reshape(8, 8, 128).astype(BF16)
            remote(psend.at[t, zz], arecv.at[t, kind], a_ssem, a_rsem.at[t], to, tp).start()
    arrived(kbuf.at[0:7], k_rsem)
    arrived(qbuf.at[0:7], q_rsem)
    own_rows = jnp.concatenate(
        [acts_f[pl.ds(pl.multiple_of(k * 64 + c * 8, 8), 8), :] for k in range(8)], axis=0
    ).astype(BF16)
    step_t = jnp.concatenate([kbuf[j].astype(F32)[:, 0:32] for j in range(8)], axis=1)
    step_t = jnp.concatenate([step_t, jnp.zeros((112, 256), F32)], axis=0).astype(BF16)
    ext = lax.dot_general(own_rows, step_t, turned, preferred_element_type=F32)
    qsum = qbuf[0]
    for j in range(1, 8):
        qsum = qsum + qbuf[j]
    qeven = pltpu.roll(qsum, 64, axis=1)
    for k in range(8):
        row = (qsum if k % 2 else qeven)[k // 2:k // 2 + 1, :]
        mixture = jnp.where(low_half, ext[k * 8:k * 8 + 8, :], jnp.broadcast_to(row, (8, 128)))
        high = mixture.astype(BF16).astype(F32)
        rest = (mixture - high).astype(BF16).astype(F32)
        lower = jnp.where(low_half, pltpu.roll(jnp.where(low_half, rest, 0.0), 16, axis=1), rest)
        esend[k] = jnp.where(low_half, high + lower, jnp.where(row8 < 4, high, lower)).astype(BF16)
    erecv[z] = esend[z]
    remote(esend.at[lax.rem(z + 4, 8)], efar, e_ssem, x_rsem, far * 8 + c, tp).start()
    lhs = jnp.concatenate([token_block(away) for away in (1, 7, 0, 2, 6)], axis=0)
    for t in range(3):
        part = jnp.dot(lhs, wblk[t], preferred_element_type=F32)
        for i, away in enumerate((1, 7, 0, 2, 6)):
            psend[t, lax.rem(z + away, 8)] = part[i * 64:i * 64 + 64, :].reshape(8, 8, 128).astype(BF16)
        to_owners(psend.at[t, lax.rem(z + 1, 8)], t, 1, 1, p_ssem, p_rsem.at[t])
        to_owners(psend.at[t, lax.rem(z + 7, 8)], t, 2, 7, p_ssem, p_rsem.at[t])
        to_owners(psend.at[t, z], t, 0, 0, h_ssem, h_rsem.at[t])
        frecv[t, 0, c] = psend[t, z, c]
    arrived(wog.at[0:2], g_rsem.at[1])
    for r in (3, 5, 2, 6, 1, 7):
        remote(esend.at[lax.rem(z + r, 8)], erecv.at[z], e_ssem, e_rsem, ring(r), tp).start()
    for t in range(3):
        arrived(arecv.at[t], a_rsem.at[t])
        extra_block = arecv[t, 2].astype(F32)
        zero_block = jnp.zeros_like(extra_block)
        plus = psend[t, lax.rem(z + 2, 8)].astype(F32) + arecv[t, 0].astype(F32)
        minus = psend[t, lax.rem(z + 6, 8)].astype(F32) + arecv[t, 1].astype(F32)
        bsend[t, 0] = (plus + jnp.where(even, extra_block, zero_block)).astype(BF16)
        bsend[t, 1] = (minus + jnp.where(even, zero_block, extra_block)).astype(BF16)
        to_owners(bsend.at[t, 0], t, 3, 2, p_ssem, p_rsem.at[t])
        to_owners(bsend.at[t, 1], t, 4, 6, p_ssem, p_rsem.at[t])
    arrived(efar, x_rsem)
    back = lax.rem(z + 6 + 4 * lax.rem(z, 2), 8)
    remote(efar, erecv.at[back], x_ssem, e_rsem, far * 8 + c, tp).start()
    pass_on(2)

    arrived(erecv.at[0:7], e_rsem)
    esum = erecv[0].astype(F32)
    for k in range(1, 8):
        esum = esum + erecv[k].astype(F32)
    own_lane = lane128 == 64 + c * 8 + row8
    qrow = jnp.broadcast_to(esum[0:1, :] + esum[4:5, :], (8, 128))
    inverse = lax.rsqrt(jnp.sum(jnp.where(own_lane, qrow, 0.0), axis=1, keepdims=True) / 2048.0 + EPS)
    esum = esum + pltpu.roll(esum, 112, axis=1)
    step = softplus(inverse * esum[:, 0:16] + bias_r)
    decay = rate_e * step + nextra
    cum = decay + down(decay, 1) + down(decay, 2) + down(decay, 3)
    pair_w = []
    for d in range(4):
        w = jnp.exp(jnp.minimum(cum - down(cum, d), 0.0)) * down(step, d)
        pair_w.append(jnp.where(tok >= d, w, 0.0))
    ecum = jnp.exp(cum)

    def settle(t):
        arrived(frecv.at[t, 1:5], p_rsem.at[t])
        arrived(frecv.at[t, 0, 0:7], h_rsem.at[t])

    def fresh(t, j):
        x = frecv[t, 0, j].astype(F32)
        for slot in range(1, 5):
            x = x + frecv[t, slot, j].astype(F32)
        return (x * inverse).astype(BF16).astype(F32)

    dg = jnp.broadcast_to(dgain_v[...], (8, 16))
    settle(0)

    def conv(x, lo, taps, at):
        t = taps[:, at:at + 128].astype(F32)
        y = base[:, lo:lo + 128] + x * t[3:4]
        for d in range(1, 4):
            y = y + down(x, d) * t[3 - d:4 - d]
        return silu(y)

    writes = [conv(fresh(0, g), 1024 + g * 128, tw_v, g * 128) for g in range(4)]
    reads = [conv(fresh(0, 4 + g), 1536 + g * 128, tr_v, g * 128) for g in range(4)]
    carried, inner = [], []
    for g in range(4):
        rb = reads[g].astype(BF16)
        both = [
            lax.dot_general(rb, state_b[s, g], turned, preferred_element_type=F32) for s in range(2)
        ]
        carried.append(jnp.where(row8 < 4, both[0], both[1]))
        inner.append([jnp.sum(reads[g] * down(writes[g], d), axis=1, keepdims=True) for d in range(4)])
    settle(1)
    mixed = []
    for j in range(8):
        g, i = j // 2, j % 2
        value = conv(fresh(1, j), j * 128, tv_v, j * 128)
        m = spread(ecum, j) * carried[g][:, i * 128:(i + 1) * 128] + spread(dg, j) * value
        for d in range(4):
            m = m + (inner[g][d] * spread(pair_w[d], j)) * down(value, d)
        mixed.append(m)
    settle(2)
    normed = []
    for g in range(4):
        gated = [mixed[j] * silu(fresh(2, j)) for j in (2 * g, 2 * g + 1)]
        mean = jnp.sum(gated[0] * gated[0] + gated[1] * gated[1], axis=1, keepdims=True) / 256.0
        scale = lax.rsqrt(mean + EPS)
        for i in range(2):
            j = 2 * g + i
            normed.append(gated[i] * scale * ngain_v[:, j * 128:(j + 1) * 128])
    nrm[c] = jnp.concatenate(
        [jnp.concatenate(normed[0:4], axis=1), jnp.concatenate(normed[4:8], axis=1)], axis=0
    ).astype(BF16)

    for r in (4, 3, 5, 2, 6, 1, 7):
        remote(nrm.at[c], nrm.at[c], n_ssem, n_rsem, plane(r), tp).start()
    arrived(wog.at[0:2], g_rsem.at[2])
    for r in range(1, 4):
        pl.semaphore_signal(ready, inc=1, device_id={"kv": kv, "tp": lax.rem(tp + r, 4)}, device_id_type=MESH)
    pass_on(3)
    arrived(wog.at[0], g_rsem.at[3])
    pl.semaphore_wait(ready, 3)
    arrived(nrm.at[0:7], n_rsem)

    nall = nrm[...].astype(F32)
    wall = wog[...].reshape(256, 1024)
    p = None
    for i in range(2):
        block = nall[:, i * 8:i * 8 + 8, :].reshape(64, 512).astype(BF16)
        q = lax.dot_general(wall[:, i * 512:(i + 1) * 512], block, turned, preferred_element_type=F32)
        p = q if p is None else p + q
    for k in range(8):
        packed = jnp.concatenate([p[k * 32:k * 32 + 16, :], p[k * 32 + 16:k * 32 + 32, :]], axis=1)
        osend[k] = packed.astype(BF16)

    owner = lax.div(z, 2)
    slot = tp * 2 + lax.rem(z, 2)
    for r in (4, 3, 5, 2, 6, 1, 7):
        remote(osend.at[lax.rem(z + r, 8)], orecv.at[slot], o_ssem, o_rsem, ring(r), owner).start()

    @pl.when(owner != tp)
    def _():
        remote(osend.at[z], orecv.at[slot], o_ssem, o_rsem, kv, owner).start()
        arrived(orecv.at[0:8], o_rsem)

    @pl.when(owner == tp)
    def _():
        orecv[slot] = osend[z]
        arrived(orecv.at[0:7], o_rsem)

    sums = []
    for q in range(2):
        s4 = orecv[q].astype(F32)
        for x in range(1, 4):
            s4 = s4 + orecv[x * 2 + q].astype(F32)
        sums.append(s4)
    lane16 = lax.broadcasted_iota(jnp.int32, (16, 128), 1) < 64
    top = jnp.where(lane16, sums[0], pltpu.roll(sums[1], 64, axis=1))
    bottom = jnp.where(lane16, pltpu.roll(sums[0], 64, axis=1), sums[1])
    out_ref[...] = jnp.concatenate([top, bottom], axis=0).astype(BF16)

    for ref, sem in (
        (acts_t.at[0:128, :], acts_ssem), (acts_t.at[0:96, :], d_ssem), (wsend.at[0:7], w_ssem),
        (kbuf.at[0:7], k_ssem), (qbuf.at[0:7], q_ssem), (wog.at[0:7], g_ssem), (arecv, a_ssem),
        (frecv.at[:, 1:5], p_ssem), (frecv.at[:, 0, 0:7], h_ssem), (erecv.at[0:7], e_ssem), (efar, x_ssem),
        (nrm.at[0:7], n_ssem),
    ):
        sent(ref, sem)

    @pl.when(owner != tp)
    def _():
        sent(osend.at[0:8], o_ssem)

    @pl.when(owner == tp)
    def _():
        sent(osend.at[0:7], o_ssem)


def hand_out(a, b, a_out, b_out, sem):
    copies = [pltpu.make_async_copy(b, b_out, sem.at[0]), pltpu.make_async_copy(a, a_out, sem.at[1])]
    for cp in copies:
        cp.start()
    for cp in copies:
        cp.wait()


def per_device(
    hidden_vectors, input_norm_gain, gate_matrix, value_matrix, write_matrix, read_matrix, step_matrix,
    raw_value_rows, raw_write_rows, raw_read_rows, value_filter_taps, write_filter_taps, read_filter_taps,
    step_size_bias, rate_logarithm, direct_path_gain, prior_step_preact, extra_log_decay, accepted, prior_state,
    group_norm_gain, output_matrix,
):
    operands = [
        accepted, hidden_vectors.T, input_norm_gain.reshape(1, 32), gate_matrix, value_matrix, write_matrix, read_matrix,
        step_matrix.T, raw_value_rows.transpose(1, 0, 2), raw_write_rows.transpose(1, 0, 2),
        raw_read_rows.transpose(1, 0, 2), value_filter_taps, write_filter_taps,
        read_filter_taps, step_size_bias.reshape(1, 16), rate_logarithm.reshape(1, 16),
        direct_path_gain.reshape(1, 16), prior_step_preact, extra_log_decay, prior_state.reshape(2, 4, 256, 128),
        group_norm_gain.reshape(1, 1024), output_matrix.T,
    ]
    buffers = [pltpu.SMEM((2,), jnp.int32)] + [
        pltpu.VMEM(x.shape, x.dtype) for i, x in enumerate(operands) if i not in (0, PRIOR)
    ]
    dma = pltpu.SemaphoreType.DMA
    scratch = buffers + [
        pltpu.VMEM((256, 512), BF16),
        pltpu.VMEM((8, 3, 32, 128), BF16),
        pltpu.VMEM((3, 256, 128), BF16),
        pltpu.VMEM((8, 16, 128), BF16),
        pltpu.VMEM((8, 4, 128), F32),
        pltpu.VMEM((512, 256), F32),
        pltpu.VMEM((512, 256), BF16),
        pltpu.VMEM((3, 8, 8, 8, 128), BF16),
        pltpu.VMEM((3, 3, 8, 8, 128), BF16),
        pltpu.VMEM((3, 2, 8, 8, 128), BF16),
        pltpu.VMEM((3, 5, 8, 8, 128), BF16),
        pltpu.VMEM((8, 8, 128), BF16),
        pltpu.VMEM((8, 8, 128), BF16),
        pltpu.VMEM((8, 128), BF16),
        pltpu.VMEM((8, 16, 512), BF16),
        pltpu.VMEM((8, 32, 1024), BF16),
        pltpu.VMEM((8, 16, 128), BF16),
        pltpu.VMEM((8, 16, 128), BF16),
        pltpu.VMEM((8, 2048), F32),
        pltpu.VMEM((2, 4, 256, 128), BF16),
        dma((len(operands),)),
        dma, dma((4,)), dma, dma, dma, dma((3,)), dma, dma, dma, dma, dma, dma((4,)),
        dma, dma((3,)), dma, dma((3,)), dma, dma((3,)), dma, dma, dma, dma, dma, dma, dma, dma,
        pltpu.SemaphoreType.REGULAR,
    ]
    operands = [pltpu.with_memory_space_constraint(x, pltpu.HBM) for x in operands]
    out, state = pl.pallas_call(
        mixer_kernel,
        out_shape=(
            pltpu.VMEM((32, 128), BF16),
            pltpu.VMEM((2, 4, 256, 128), F32),
        ),
        in_specs=[pl.BlockSpec(memory_space=pl.ANY)] * len(operands),
        out_specs=(pl.BlockSpec(memory_space=pltpu.VMEM), pl.BlockSpec(memory_space=pltpu.VMEM)),
        scratch_shapes=scratch,
        compiler_params=pltpu.CompilerParams(
            collective_id=0, has_side_effects=True, vmem_limit_bytes=32 * 1024 * 1024
        ),
        cost_estimate=pl.CostEstimate(flops=10**9, bytes_accessed=4 * 10**6, transcendentals=10**5),
        name="mixer",
    )(*operands)
    out, state = [pltpu.with_memory_space_constraint(x, pltpu.VMEM) for x in (out, state)]
    out, state = pl.pallas_call(
        hand_out,
        out_shape=(
            jax.ShapeDtypeStruct((32, 128), BF16),
            jax.ShapeDtypeStruct((2, 4, 256, 128), F32),
        ),
        in_specs=[pl.BlockSpec(memory_space=pltpu.VMEM)] * 2,
        out_specs=(pl.BlockSpec(memory_space=pl.ANY),) * 2,
        scratch_shapes=[pltpu.SemaphoreType.DMA((2,))],
        compiler_params=pltpu.CompilerParams(vmem_limit_bytes=32 * 1024 * 1024),
        name="hand_out",
    )(out, state)
    return out.T, state.reshape(2, 16, 64, 128)


def solution(mesh):
    return jax.shard_map(
        per_device,
        mesh=mesh,
        in_specs=(
            P(None, "kv"),
            P("kv"),
            P("kv", "tp"),
            P("kv", "tp"),
            P("kv", "tp"),
            P("kv", "tp"),
            P("kv", "tp"),
            P("kv", None, "tp"),
            P("kv", None, "tp"),
            P("kv", None, "tp"),
            P(None, "tp"),
            P(None, "tp"),
            P(None, "tp"),
            P("tp"),
            P("tp"),
            P("tp"),
            P("kv", None, "tp"),
            P("kv", None, "tp"),
            P("kv"),
            P("kv", "tp", None, None),
            P("tp"),
            P("tp", "kv"),
        ),
        out_specs=(P("tp", "kv"), P("kv", "tp", None, None)),
        check_vma=False,
    )
```

```python
import jax
import jax.numpy as jnp
from jax import lax
from jax.experimental import pallas as pl
from jax.experimental.pallas import tpu as pltpu
from jax.sharding import PartitionSpec as P

MESH = pl.DeviceIdType.MESH
F32 = jnp.float32
BF16 = jnp.bfloat16
EPS = 1e-6


def silu(x):
    return x / (1.0 + jnp.exp(-x))


def softplus(x):
    return jnp.maximum(x, 0.0) + jnp.log(1.0 + jnp.exp(-jnp.abs(x)))


def mixer_kernel(
    acc, hid, gain, wg, wv, ww, wr, ws, rawv, raww, rawr, tv, tw, tr, bias, rate, dgain, ppre, extra, prior, ngain, wo,
    out_ref, st_out,
    acc_s, hid_v, gain_v, wide_v, narrow_v, ws_v, wo_v, rawv_v, raw_v, tv_v, tap_v, head_v, ppre_v, extra_v, ngain_v,
    acts_t, wsend, wblk, kbuf, qbuf, acts_f, acts_b, psend, arecv, bsend, frecv, esend, erecv, efar, nrm, wog, osend, orecv,
    base, state_b,
    lsem, acts_rsem, d_rsem, w_rsem, k_rsem, q_rsem, g_rsem, a_rsem, p_rsem, h_rsem, e_rsem, x_rsem, n_rsem, o_rsem,
    ready,
):
    kv = lax.axis_index("kv")
    tp = lax.axis_index("tp")
    z = lax.div(kv, 8)
    c = lax.rem(kv, 8)

    def plane(r):
        return z * 8 + lax.rem(c + r, 8)

    def ring(r):
        return lax.rem(z + r, 8) * 8 + c

    def remote(src, dst, ssem, rsem, kv_to, tp_to):
        return pltpu.make_async_remote_copy(
            src_ref=src, dst_ref=dst, send_sem=ssem, recv_sem=rsem,
            device_id={"kv": kv_to, "tp": tp_to}, device_id_type=MESH,
        )

    acts_ssem, d_ssem, w_ssem, k_ssem, q_ssem, g_ssem, a_ssem, p_ssem, h_ssem, e_ssem, x_ssem, n_ssem, o_ssem = [
        lsem.at[i] for i in (0, 1, 2, 3, 4, 5, 6, 7, 8, 9, 10, 11, 12)
    ]

    def arrived(ref, sem):
        remote(ref, ref, acts_ssem, sem, kv, tp).wait_recv()

    def sent(ref, sem):
        remote(ref, ref, sem, e_rsem, kv, tp).wait_send()

    barrier = pltpu.get_barrier_semaphore()
    for r in range(1, 8):
        pl.semaphore_signal(barrier, inc=1, device_id={"kv": plane(r), "tp": tp}, device_id_type=MESH)
    for r in (1, 7):
        pl.semaphore_signal(barrier, inc=1, device_id={"kv": ring(r), "tp": tp}, device_id_type=MESH)
    for r in range(1, 4):
        pl.semaphore_signal(barrier, inc=1, device_id={"kv": kv, "tp": lax.rem(tp + r, 4)}, device_id_type=MESH)

    pairs = [
        ([hid], hid_v), ([gain], gain_v), ([wg, wv], wide_v), ([ww, wr], narrow_v), ([ws], ws_v), ([wo], wo_v),
        ([acc], acc_s), ([rawv], rawv_v), ([raww, rawr], raw_v), ([tv], tv_v), ([tw, tr], tap_v),
        ([bias, rate, dgain], head_v), ([ppre], ppre_v), ([extra], extra_v), ([ngain], ngain_v), ([prior], st_out),
    ]
    loads = []
    for i, (sources, target) in enumerate(pairs):
        for j, source in enumerate(sources):
            pltpu.make_async_copy(source, target.at[j] if len(sources) > 1 else target, lsem.at[i]).start()
        loads.append(pltpu.make_async_copy(target, target, lsem.at[i]))

    own32 = pl.ds(pl.multiple_of(c * 32, 32), 32)
    loads[0].wait()
    loads[1].wait()
    diag = lax.broadcasted_iota(jnp.int32, (32, 32), 0) == lax.broadcasted_iota(jnp.int32, (32, 32), 1)
    gcol = jnp.sum(jnp.where(diag, jnp.broadcast_to(gain_v[...], (32, 32)), 0.0), axis=1, keepdims=True)
    hidden = hid_v[...].astype(F32)
    hidden = pltpu.roll(hidden, lax.rem(13 - z, 8) * 64, axis=1)
    scaled = (hidden * gcol).astype(BF16)
    for h in range(2):
        acts_t[h, own32, :] = scaled[:, h * 256:(h + 1) * 256]
    squares = jnp.sum(hidden * hidden, axis=0, keepdims=True)
    qbuf[c] = jnp.concatenate([squares[:, i * 128:(i + 1) * 128] for i in range(4)], axis=0)
    for i in range(2, 5):
        loads[i].wait()
    wg_v, wv_v, ww_v, wr_v = wide_v.at[0], wide_v.at[1], narrow_v.at[0], narrow_v.at[1]
    for j in range(8):
        lane = slice(j * 128, j * 128 + 128)
        half = slice((j % 4) * 128, (j % 4) * 128 + 128)
        wsend[j, 0] = ww_v[:, half] if j < 4 else wr_v[:, half]
        wsend[j, 1] = wv_v[:, lane]
        wsend[j, 2] = wg_v[:, lane]
    for t in range(3):
        wblk[t, own32, :] = wsend[c, t]
    kbuf[c] = jnp.concatenate([ws_v[...].astype(F32), jnp.zeros((16, 96), F32)], axis=1).astype(BF16)

    pl.semaphore_wait(barrier, 12)

    partner = z * 8 + c + 1 - 2 * lax.rem(c, 2)

    def same_core(i):
        return pl.ds(pl.multiple_of(lax.rem(c + 8 - 2 * i, 8) * 32, 32), 32)

    def send_hidden(h):
        own = acts_t.at[h, own32, :]
        for i in (2, 1, 3):
            remote(own, own, acts_ssem, acts_rsem.at[h, i - 1], plane(2 * i), tp).start()
        remote(own, own, acts_ssem, d_rsem.at[h], partner, tp).start()

    def send_weights(t):
        for r in (4, 3, 5, 2, 6, 1, 7):
            remote(wsend.at[lax.rem(c + r, 8), t], wblk.at[t, own32, :], w_ssem, w_rsem.at[t], plane(r), tp).start()

    def hand_over(h):
        for i in (1, 3, 2):
            arrived(acts_t.at[h, own32, :], acts_rsem.at[h, i - 1])
            block = acts_t.at[h, same_core(i), :]
            remote(block, block, d_ssem, d_rsem.at[h], partner, tp).start()

    def turn(h):
        arrived(acts_t.at[h, 0:128, :], d_rsem.at[h])
        for i in range(2):
            block = jnp.transpose(acts_t[h, :, i * 128:(i + 1) * 128].astype(F32))
            rows = slice(h * 256 + i * 128, h * 256 + i * 128 + 128)
            acts_f[rows, :] = block
            acts_b[rows, :] = block.astype(BF16)

    send_hidden(0)
    send_weights(0)
    send_weights(1)
    send_weights(2)
    send_hidden(1)
    for r in (4, 3, 5, 2, 6, 1, 7):
        remote(kbuf.at[c], kbuf.at[c], k_ssem, k_rsem, plane(r), tp).start()
        remote(qbuf.at[c], qbuf.at[c], q_ssem, q_rsem, plane(r), tp).start()

    loads[5].wait()
    wog[z] = wo_v[...]

    def pass_on(hop):
        for way, step in ((0, 1), (1, 7)):
            at = lax.rem(z + 8 * hop - step * hop, 8)
            remote(wog.at[at], wog.at[at], g_ssem, g_rsem.at[hop], ring(step), tp).start()

    pass_on(0)

    for cp in loads[6:]:
        cp.wait()
    raww_v, rawr_v, tw_v, tr_v = raw_v.at[0], raw_v.at[1], tap_v.at[0], tap_v.at[1]
    bias_v, rate_v, dgain_v = head_v.at[0], head_v.at[1], head_v.at[2]
    row8 = lax.broadcasted_iota(jnp.int32, (8, 1), 0)
    tok = lax.rem(row8, 4)

    def down(x, d):
        if d == 0:
            return x
        return jnp.where(tok >= d, pltpu.roll(x, d, axis=0), 0.0)

    def up(x, d):
        return jnp.where(tok + d < 4, pltpu.roll(x, 8 - d, axis=0), 0.0)

    def last_conv(raw, taps):
        t = taps[...].astype(F32)
        rows = [raw[k].astype(F32) for k in range(7)]
        parts = []
        for i in range(4):
            total = rows[i] * t[0:1]
            for j in range(1, 4):
                total = total + rows[i + j] * t[j:j + 1]
            parts.append(total)
        return silu(jnp.concatenate([p[s:s + 1] for s in range(2) for p in parts], axis=0))

    def base_conv(raw, taps, lo, hi):
        t = taps[...].astype(F32)
        rows = [raw[k].astype(F32) for k in range(7)]
        second = lax.broadcasted_iota(jnp.int32, (2, 1), 0) == 1
        a = jnp.where(second, acc_s[1], acc_s[0])
        win = []
        for i in range(3):
            w = rows[4 + i]
            for k in range(3, -1, -1):
                w = jnp.where(a == k, rows[k + i], w)
            win.append(w)
        w0, w1, w2 = win
        parts = [w0 * t[0:1] + w1 * t[1:2] + w2 * t[2:3], w1 * t[0:1] + w2 * t[1:2], w2 * t[0:1],
                 jnp.zeros((2, hi - lo), F32)]
        base[:, lo:hi] = jnp.concatenate([p[s:s + 1] for s in range(2) for p in parts], axis=0)

    lastv = last_conv(rawv_v, tv_v)
    lastw = last_conv(raww_v, tw_v)
    base_conv(rawv_v, tv_v, 0, 1024)
    base_conv(raww_v, tw_v, 1024, 1536)
    base_conv(rawr_v, tr_v, 1536, 2048)

    rate_e = -jnp.exp(rate_v[...])
    bias_r = bias_v[...]
    pstep = softplus(jnp.concatenate([ppre_v[0], ppre_v[1]], axis=0) + bias_r)
    pextra = jnp.concatenate([extra_v[0, 0:4], extra_v[1, 0:4]], axis=0)
    nextra = jnp.concatenate([extra_v[0, 4:8], extra_v[1, 4:8]], axis=0)
    limit = jnp.where(row8 < 4, acc_s[0], acc_s[1])
    live = jnp.where(tok < limit, 1.0, 0.0)
    kept = (rate_e * pstep + pextra) * live
    tail = up(kept, 1) + up(kept, 2) + up(kept, 3)
    coef = live * jnp.exp(tail) * pstep
    etot = jnp.exp(kept + tail)
    lane128 = lax.broadcasted_iota(jnp.int32, (8, 128), 1)
    low_half = lane128 < 64

    def spread(e, i):
        a = jnp.broadcast_to(e[:, 2 * i:2 * i + 1], (8, 128))
        b = jnp.broadcast_to(e[:, 2 * i + 1:2 * i + 2], (8, 128))
        return jnp.where(low_half, a, b)

    for g in range(4):
        vals = [lastv[:, (2 * g + i) * 128:(2 * g + i + 1) * 128] * spread(coef, 2 * g + i) for i in range(2)]
        weighted = jnp.concatenate(vals, axis=1)
        lw = lastw[:, g * 128:(g + 1) * 128]
        for s in range(2):
            own_seq = (row8 < 4) if s == 0 else (row8 >= 4)
            added = lax.dot_general(
                weighted, jnp.where(own_seq, lw, 0.0), (((0,), (0,)), ((), ())),
                precision=lax.Precision.HIGHEST, preferred_element_type=F32,
            )
            for i in range(4):
                h = g * 4 + i
                rows = slice(i * 64, i * 64 + 64)
                factor = jnp.broadcast_to(etot[s * 4:s * 4 + 1, h:h + 1], (64, 128))
                new = factor * st_out[s, g, rows, :] + added[rows, :]
                st_out[s, g, rows, :] = new
                state_b[s, g, rows, :] = new.astype(BF16)

    hand_over(0)
    arrived(wog.at[0:2], g_rsem.at[0])
    pass_on(1)
    turn(0)
    turned = (((1,), (1,)), ((), ()))
    even = lax.rem(z, 2) == 0
    far = lax.rem(z + 2 + 4 * lax.rem(z, 2), 8)

    def to_owners(src, t, slot, dz, ssem, rsem):
        for r in range(0 if dz else 1, 8):
            cc = lax.rem(c + r, 8)
            remote(src.at[cc], frecv.at[t, slot, c], ssem, rsem, lax.rem(z + dz, 8) * 8 + cc, tp).start()

    lhs = acts_b[0:192, :]
    for t in range(3):
        arrived(wblk.at[t, 0:224, :], w_rsem.at[t])
        part = jnp.dot(lhs, wblk[t], preferred_element_type=F32)
        for i, (kind, away, to) in enumerate(((0, 3, ring(1)), (2, 4, far * 8 + c), (1, 5, ring(7)))):
            zz = lax.rem(z + away, 8)
            psend[t, zz] = part[i * 64:i * 64 + 64, :].reshape(8, 8, 128).astype(BF16)
            remote(psend.at[t, zz], arecv.at[t, kind], a_ssem, a_rsem.at[t], to, tp).start()
    hand_over(1)
    turn(1)
    arrived(kbuf.at[0:7], k_rsem)
    arrived(qbuf.at[0:7], q_rsem)
    own_rows = jnp.concatenate(
        [acts_f[pl.ds(pl.multiple_of(k * 64 + c * 8, 8), 8), :] for k in range(8)], axis=0
    ).astype(BF16)
    step_t = jnp.concatenate([kbuf[j].astype(F32)[:, 0:32] for j in range(8)], axis=1)
    step_t = jnp.concatenate([step_t, jnp.zeros((112, 256), F32)], axis=0).astype(BF16)
    ext = lax.dot_general(own_rows, step_t, turned, preferred_element_type=F32)
    qsum = qbuf[0]
    for j in range(1, 8):
        qsum = qsum + qbuf[j]
    qeven = pltpu.roll(qsum, 64, axis=1)
    for k in range(8):
        row = (qsum if k % 2 else qeven)[k // 2:k // 2 + 1, :]
        mixture = jnp.where(low_half, ext[k * 8:k * 8 + 8, :], jnp.broadcast_to(row, (8, 128)))
        high = mixture.astype(BF16).astype(F32)
        rest = (mixture - high).astype(BF16).astype(F32)
        lower = jnp.where(low_half, pltpu.roll(jnp.where(low_half, rest, 0.0), 16, axis=1), rest)
        esend[lax.rem(z + 3 + k, 8)] = jnp.where(low_half, high + lower, jnp.where(row8 < 4, high, lower)).astype(BF16)
    erecv[z] = esend[z]
    remote(esend.at[lax.rem(z + 4, 8)], efar, e_ssem, x_rsem, far * 8 + c, tp).start()
    lhs = acts_b[192:512, :]
    for t in range(3):
        part = jnp.dot(lhs, wblk[t], preferred_element_type=F32)
        for i, away in enumerate((6, 7, 0, 1, 2)):
            psend[t, lax.rem(z + away, 8)] = part[i * 64:i * 64 + 64, :].reshape(8, 8, 128).astype(BF16)
        to_owners(psend.at[t, lax.rem(z + 1, 8)], t, 1, 1, p_ssem, p_rsem.at[t])
        to_owners(psend.at[t, lax.rem(z + 7, 8)], t, 2, 7, p_ssem, p_rsem.at[t])
        to_owners(psend.at[t, z], t, 0, 0, h_ssem, h_rsem.at[t])
        frecv[t, 0, c] = psend[t, z, c]
    arrived(wog.at[0:2], g_rsem.at[1])
    for r in (3, 5, 2, 6, 1, 7):
        remote(esend.at[lax.rem(z + r, 8)], erecv.at[z], e_ssem, e_rsem, ring(r), tp).start()
    for t in range(3):
        arrived(arecv.at[t], a_rsem.at[t])
        extra_block = arecv[t, 2].astype(F32)
        zero_block = jnp.zeros_like(extra_block)
        plus = psend[t, lax.rem(z + 2, 8)].astype(F32) + arecv[t, 0].astype(F32)
        minus = psend[t, lax.rem(z + 6, 8)].astype(F32) + arecv[t, 1].astype(F32)
        bsend[t, 0] = (plus + jnp.where(even, extra_block, zero_block)).astype(BF16)
        bsend[t, 1] = (minus + jnp.where(even, zero_block, extra_block)).astype(BF16)
        to_owners(bsend.at[t, 0], t, 3, 2, p_ssem, p_rsem.at[t])
        to_owners(bsend.at[t, 1], t, 4, 6, p_ssem, p_rsem.at[t])
    arrived(efar, x_rsem)
    back = lax.rem(z + 6 + 4 * lax.rem(z, 2), 8)
    remote(efar, erecv.at[back], x_ssem, e_rsem, far * 8 + c, tp).start()
    pass_on(2)

    arrived(erecv.at[0:7], e_rsem)
    remote(wog.at[back], wog.at[back], g_ssem, g_rsem.at[3], far * 8 + c, tp).start()
    esum = erecv[0].astype(F32)
    for k in range(1, 8):
        esum = esum + erecv[k].astype(F32)
    own_lane = lane128 == 64 + c * 8 + row8
    qrow = jnp.broadcast_to(esum[0:1, :] + esum[4:5, :], (8, 128))
    inverse = lax.rsqrt(jnp.sum(jnp.where(own_lane, qrow, 0.0), axis=1, keepdims=True) / 2048.0 + EPS)
    esum = esum + pltpu.roll(esum, 112, axis=1)
    step = softplus(inverse * esum[:, 0:16] + bias_r)
    decay = rate_e * step + nextra
    cum = decay + down(decay, 1) + down(decay, 2) + down(decay, 3)
    pair_w = []
    for d in range(4):
        w = jnp.exp(jnp.minimum(cum - down(cum, d), 0.0)) * down(step, d)
        pair_w.append(jnp.where(tok >= d, w, 0.0))
    ecum = jnp.exp(cum)

    def settle(t):
        arrived(frecv.at[t, 1:5], p_rsem.at[t])
        arrived(frecv.at[t, 0, 0:7], h_rsem.at[t])

    def fresh(t, j):
        x = frecv[t, 0, j].astype(F32)
        for slot in range(1, 5):
            x = x + frecv[t, slot, j].astype(F32)
        return (x * inverse).astype(BF16).astype(F32)

    dg = jnp.broadcast_to(dgain_v[...], (8, 16))
    settle(0)

    def conv(x, lo, taps, at):
        t = taps[:, at:at + 128].astype(F32)
        y = base[:, lo:lo + 128] + x * t[3:4]
        for d in range(1, 4):
            y = y + down(x, d) * t[3 - d:4 - d]
        return silu(y)

    writes = [conv(fresh(0, g), 1024 + g * 128, tw_v, g * 128) for g in range(4)]
    reads = [conv(fresh(0, 4 + g), 1536 + g * 128, tr_v, g * 128) for g in range(4)]
    carried, inner = [], []
    for g in range(4):
        rb = reads[g].astype(BF16)
        both = [
            lax.dot_general(rb, state_b[s, g], turned, preferred_element_type=F32) for s in range(2)
        ]
        carried.append(jnp.where(row8 < 4, both[0], both[1]))
        inner.append([jnp.sum(reads[g] * down(writes[g], d), axis=1, keepdims=True) for d in range(4)])
    settle(1)
    mixed = []
    for j in range(8):
        g, i = j // 2, j % 2
        value = conv(fresh(1, j), j * 128, tv_v, j * 128)
        m = spread(ecum, j) * carried[g][:, i * 128:(i + 1) * 128] + spread(dg, j) * value
        for d in range(4):
            m = m + (inner[g][d] * spread(pair_w[d], j)) * down(value, d)
        mixed.append(m)
    settle(2)
    normed = []
    for g in range(4):
        gated = [mixed[j] * silu(fresh(2, j)) for j in (2 * g, 2 * g + 1)]
        mean = jnp.sum(gated[0] * gated[0] + gated[1] * gated[1], axis=1, keepdims=True) / 256.0
        scale = lax.rsqrt(mean + EPS)
        for i in range(2):
            j = 2 * g + i
            normed.append(gated[i] * scale * ngain_v[:, j * 128:(j + 1) * 128])
    nrm[c] = jnp.concatenate(
        [jnp.concatenate(normed[0:4], axis=1), jnp.concatenate(normed[4:8], axis=1)], axis=0
    ).astype(BF16)

    for r in (4, 3, 5, 2, 6, 1, 7):
        remote(nrm.at[c], nrm.at[c], n_ssem, n_rsem, plane(r), tp).start()
    arrived(wog.at[0:2], g_rsem.at[2])
    for r in range(1, 4):
        pl.semaphore_signal(ready, inc=1, device_id={"kv": kv, "tp": lax.rem(tp + r, 4)}, device_id_type=MESH)
    arrived(wog.at[0], g_rsem.at[3])
    pl.semaphore_wait(ready, 3)
    arrived(nrm.at[0:7], n_rsem)

    nall = nrm[...].astype(F32)
    wall = wog[...].reshape(256, 1024)
    p = None
    for i in range(2):
        block = nall[:, i * 8:i * 8 + 8, :].reshape(64, 512).astype(BF16)
        q = lax.dot_general(wall[:, i * 512:(i + 1) * 512], block, turned, preferred_element_type=F32)
        p = q if p is None else p + q
    for k in range(8):
        packed = jnp.concatenate([p[k * 32:k * 32 + 16, :], p[k * 32 + 16:k * 32 + 32, :]], axis=1)
        osend[k] = packed.astype(BF16)

    owner = lax.div(z, 2)
    slot = tp * 2 + lax.rem(z, 2)
    for r in (4, 3, 5, 2, 6, 1, 7):
        remote(osend.at[lax.rem(z + r, 8)], orecv.at[slot], o_ssem, o_rsem, ring(r), owner).start()

    @pl.when(owner != tp)
    def _():
        remote(osend.at[z], orecv.at[slot], o_ssem, o_rsem, kv, owner).start()
        arrived(orecv.at[0:8], o_rsem)

    @pl.when(owner == tp)
    def _():
        orecv[slot] = osend[z]
        arrived(orecv.at[0:7], o_rsem)

    sums = []
    for q in range(2):
        s4 = orecv[q].astype(F32)
        for x in range(1, 4):
            s4 = s4 + orecv[x * 2 + q].astype(F32)
        sums.append(s4)
    lane16 = lax.broadcasted_iota(jnp.int32, (16, 128), 1) < 64
    top = jnp.where(lane16, sums[0], pltpu.roll(sums[1], 64, axis=1))
    bottom = jnp.where(lane16, pltpu.roll(sums[0], 64, axis=1), sums[1])
    out_ref[...] = jnp.concatenate([top, bottom], axis=0).astype(BF16)

    for ref, sem in (
        (acts_t.at[:, 0:128, :], acts_ssem), (acts_t.at[:, 0:96, :], d_ssem), (wsend.at[0:7], w_ssem),
        (kbuf.at[0:7], k_ssem), (qbuf.at[0:7], q_ssem), (wog.at[0:7], g_ssem), (arecv, a_ssem),
        (frecv.at[:, 1:5], p_ssem), (frecv.at[:, 0, 0:7], h_ssem), (erecv.at[0:7], e_ssem), (efar, x_ssem),
        (nrm.at[0:7], n_ssem),
    ):
        sent(ref, sem)

    @pl.when(owner != tp)
    def _():
        sent(osend.at[0:8], o_ssem)

    @pl.when(owner == tp)
    def _():
        sent(osend.at[0:7], o_ssem)


def hand_out(a, b, a_out, b_out, sem):
    copies = [pltpu.make_async_copy(b.at[s, pl.ds(g, 2)], b_out.at[s, pl.ds(g, 2)], sem.at[2 * s + g // 2])
              for s in range(2) for g in (0, 2)]
    copies.append(pltpu.make_async_copy(a, a_out, sem.at[4]))
    for cp in copies:
        cp.start()
    for cp in copies:
        cp.wait()


def per_device(
    hidden_vectors, input_norm_gain, gate_matrix, value_matrix, write_matrix, read_matrix, step_matrix,
    raw_value_rows, raw_write_rows, raw_read_rows, value_filter_taps, write_filter_taps, read_filter_taps,
    step_size_bias, rate_logarithm, direct_path_gain, prior_step_preact, extra_log_decay, accepted, prior_state,
    group_norm_gain, output_matrix,
):
    operands = [
        accepted, hidden_vectors.T, input_norm_gain.reshape(1, 32), gate_matrix, value_matrix, write_matrix, read_matrix,
        step_matrix.T, raw_value_rows.transpose(1, 0, 2), raw_write_rows.transpose(1, 0, 2),
        raw_read_rows.transpose(1, 0, 2), value_filter_taps, write_filter_taps,
        read_filter_taps, step_size_bias.reshape(1, 16), rate_logarithm.reshape(1, 16),
        direct_path_gain.reshape(1, 16), prior_step_preact, extra_log_decay, prior_state.reshape(2, 4, 256, 128),
        group_norm_gain.reshape(1, 1024), output_matrix.T,
    ]
    buffers = [
        pltpu.SMEM((2,), jnp.int32),
        pltpu.VMEM((32, 512), BF16),
        pltpu.VMEM((1, 32), F32),
        pltpu.VMEM((2, 32, 1024), BF16),
        pltpu.VMEM((2, 32, 512), BF16),
        pltpu.VMEM((16, 32), BF16),
        pltpu.VMEM((32, 1024), BF16),
        pltpu.VMEM((7, 2, 1024), BF16),
        pltpu.VMEM((2, 7, 2, 512), BF16),
        pltpu.VMEM((4, 1024), BF16),
        pltpu.VMEM((2, 4, 512), BF16),
        pltpu.VMEM((3, 1, 16), F32),
        pltpu.VMEM((2, 4, 16), F32),
        pltpu.VMEM((2, 8, 16), F32),
        pltpu.VMEM((1, 1024), F32),
    ]
    dma = pltpu.SemaphoreType.DMA
    scratch = buffers + [
        pltpu.VMEM((2, 256, 256), BF16),
        pltpu.VMEM((8, 3, 32, 128), BF16),
        pltpu.VMEM((3, 256, 128), BF16),
        pltpu.VMEM((8, 16, 128), BF16),
        pltpu.VMEM((8, 4, 128), F32),
        pltpu.VMEM((512, 256), F32),
        pltpu.VMEM((512, 256), BF16),
        pltpu.VMEM((3, 8, 8, 8, 128), BF16),
        pltpu.VMEM((3, 3, 8, 8, 128), BF16),
        pltpu.VMEM((3, 2, 8, 8, 128), BF16),
        pltpu.VMEM((3, 5, 8, 8, 128), BF16),
        pltpu.VMEM((8, 8, 128), BF16),
        pltpu.VMEM((8, 8, 128), BF16),
        pltpu.VMEM((8, 128), BF16),
        pltpu.VMEM((8, 16, 512), BF16),
        pltpu.VMEM((8, 32, 1024), BF16),
        pltpu.VMEM((8, 16, 128), BF16),
        pltpu.VMEM((8, 16, 128), BF16),
        pltpu.VMEM((8, 2048), F32),
        pltpu.VMEM((2, 4, 256, 128), BF16),
        dma((16,)),
        dma((2, 3)), dma((2,)), dma((3,)), dma, dma, dma((4,)), dma((3,)), dma((3,)), dma((3,)), dma, dma, dma, dma,
        pltpu.SemaphoreType.REGULAR,
    ]
    operands = [pltpu.with_memory_space_constraint(x, pltpu.HBM) for x in operands]
    out, state = pl.pallas_call(
        mixer_kernel,
        out_shape=(
            pltpu.VMEM((32, 128), BF16),
            pltpu.VMEM((2, 4, 256, 128), F32),
        ),
        in_specs=[pl.BlockSpec(memory_space=pl.ANY)] * len(operands),
        out_specs=(pl.BlockSpec(memory_space=pltpu.VMEM), pl.BlockSpec(memory_space=pltpu.VMEM)),
        scratch_shapes=scratch,
        compiler_params=pltpu.CompilerParams(
            collective_id=0, has_side_effects=True, vmem_limit_bytes=32 * 1024 * 1024
        ),
        cost_estimate=pl.CostEstimate(flops=10**9, bytes_accessed=4 * 10**6, transcendentals=10**5),
        name="mixer",
    )(*operands)
    out, state = [pltpu.with_memory_space_constraint(x, pltpu.VMEM) for x in (out, state)]
    out, state = pl.pallas_call(
        hand_out,
        out_shape=(
            jax.ShapeDtypeStruct((32, 128), BF16),
            jax.ShapeDtypeStruct((2, 4, 256, 128), F32),
        ),
        in_specs=[pl.BlockSpec(memory_space=pltpu.VMEM)] * 2,
        out_specs=(pl.BlockSpec(memory_space=pl.ANY),) * 2,
        scratch_shapes=[pltpu.SemaphoreType.DMA((5,))],
        compiler_params=pltpu.CompilerParams(vmem_limit_bytes=32 * 1024 * 1024),
        name="hand_out",
    )(out, state)
    return out.T, state.reshape(2, 16, 64, 128)


def solution(mesh):
    return jax.shard_map(
        per_device,
        mesh=mesh,
        in_specs=(
            P(None, "kv"),
            P("kv"),
            P("kv", "tp"),
            P("kv", "tp"),
            P("kv", "tp"),
            P("kv", "tp"),
            P("kv", "tp"),
            P("kv", None, "tp"),
            P("kv", None, "tp"),
            P("kv", None, "tp"),
            P(None, "tp"),
            P(None, "tp"),
            P(None, "tp"),
            P("tp"),
            P("tp"),
            P("tp"),
            P("kv", None, "tp"),
            P("kv", None, "tp"),
            P("kv"),
            P("kv", "tp", None, None),
            P("tp"),
            P("tp", "kv"),
        ),
        out_specs=(P("tp", "kv"), P("kv", "tp", None, None)),
        check_vma=False,
    )
```

```python
import jax
import jax.numpy as jnp
from jax import lax
from jax.experimental import pallas as pl
from jax.experimental.pallas import tpu as pltpu
from jax.sharding import PartitionSpec as P

MESH = pl.DeviceIdType.MESH
F32 = jnp.float32
BF16 = jnp.bfloat16
EPS = 1e-6


def silu(x):
    return x / (1.0 + jnp.exp(-x))


def softplus(x):
    return jnp.maximum(x, 0.0) + jnp.log1p(jnp.exp(-jnp.abs(x)))


def mixer_kernel(
    acc, hid, gain, wg, wv, ww, wr, ws, rawv, raww, rawr, tv, tw, tr, bias, rate, dgain, ppre, extra, prior, ngain, wo,
    out_ref, st_out,
    acc_s, hid_v, gain_v, wide_v, narrow_v, ws_v, wo_v, rawv_v, raw_v, tv_v, tap_v, head_v, ppre_v, extra_v, ngain_v,
    acts_t, wsend, wblk, kbuf, qbuf, acts_f, acts_b, psend, arecv, bsend, frecv, esend, erecv, efar, nrm, wog, osend, orecv,
    base, state_b,
    lsem, acts_rsem, d_rsem, w_rsem, k_rsem, q_rsem, g_rsem, a_rsem, p_rsem, h_rsem, b_rsem, e_rsem, x_rsem, n_rsem, o_rsem,
    ready,
):
    kv = lax.axis_index("kv")
    tp = lax.axis_index("tp")
    z = lax.div(kv, 8)
    c = lax.rem(kv, 8)

    def plane(r):
        return z * 8 + lax.rem(c + r, 8)

    def ring(r):
        return lax.rem(z + r, 8) * 8 + c

    def remote(src, dst, ssem, rsem, kv_to, tp_to):
        return pltpu.make_async_remote_copy(
            src_ref=src, dst_ref=dst, send_sem=ssem, recv_sem=rsem,
            device_id={"kv": kv_to, "tp": tp_to}, device_id_type=MESH,
        )

    acts_ssem, d_ssem, w_ssem, k_ssem, q_ssem, g_ssem, a_ssem, p_ssem, h_ssem, e_ssem, x_ssem, n_ssem, o_ssem, b_ssem = [
        lsem.at[i] for i in range(14)
    ]

    def arrived(ref, sem):
        remote(ref, ref, acts_ssem, sem, kv, tp).wait_recv()

    def sent(ref, sem):
        remote(ref, ref, sem, e_rsem, kv, tp).wait_send()

    barrier = pltpu.get_barrier_semaphore()
    for r in range(1, 8):
        pl.semaphore_signal(barrier, inc=1, device_id={"kv": plane(r), "tp": tp}, device_id_type=MESH)
    for r in (1, 7):
        pl.semaphore_signal(barrier, inc=1, device_id={"kv": ring(r), "tp": tp}, device_id_type=MESH)
    for r in range(1, 4):
        pl.semaphore_signal(barrier, inc=1, device_id={"kv": kv, "tp": lax.rem(tp + r, 4)}, device_id_type=MESH)

    pairs = [
        ([hid], hid_v), ([gain], gain_v), ([wg, wv], wide_v), ([ww, wr], narrow_v), ([ws], ws_v), ([wo], wo_v),
        ([acc], acc_s), ([rawv], rawv_v), ([raww, rawr], raw_v), ([tv], tv_v), ([tw, tr], tap_v),
        ([bias, rate, dgain], head_v), ([ppre], ppre_v), ([extra], extra_v), ([ngain], ngain_v), ([prior], st_out),
    ]
    loads = []
    for i, (sources, target) in enumerate(pairs):
        for j, source in enumerate(sources):
            pltpu.make_async_copy(source, target.at[j] if len(sources) > 1 else target, lsem.at[i]).start()
        loads.append(pltpu.make_async_copy(target, target, lsem.at[i]))

    own32 = pl.ds(pl.multiple_of(c * 32, 32), 32)
    loads[0].wait()
    loads[1].wait()
    diag = lax.broadcasted_iota(jnp.int32, (32, 32), 0) == lax.broadcasted_iota(jnp.int32, (32, 32), 1)
    gcol = jnp.sum(jnp.where(diag, jnp.broadcast_to(gain_v[...], (32, 32)), 0.0), axis=1, keepdims=True)
    hidden = hid_v[...].astype(F32)
    hidden = pltpu.roll(hidden, lax.rem(13 - z, 8) * 64, axis=1)
    scaled = (hidden * gcol).astype(BF16)
    for h in range(2):
        acts_t[h, own32, :] = scaled[:, h * 256:(h + 1) * 256]
    squares = jnp.sum(hidden * hidden, axis=0, keepdims=True)
    qbuf[c] = jnp.concatenate([squares[:, i * 128:(i + 1) * 128] for i in range(4)], axis=0)
    for i in range(2, 5):
        loads[i].wait()
    wg_v, wv_v, ww_v, wr_v = wide_v.at[0], wide_v.at[1], narrow_v.at[0], narrow_v.at[1]
    for j in range(8):
        near = slice((j % 4) * 128, (j % 4) * 128 + 128)
        wsend[j, 0] = (ww_v if j < 4 else wr_v)[:, near]
        for h in range(2):
            lane = slice((j % 4 + 4 * h) * 128, (j % 4 + 4 * h) * 128 + 128)
            wsend[j, 1 + h] = (wv_v if j < 4 else wg_v)[:, lane]
    for t in range(3):
        wblk[t, own32, :] = wsend[c, t]
    kbuf[c] = jnp.concatenate([ws_v[...].astype(F32), jnp.zeros((16, 96), F32)], axis=1).astype(BF16)

    loads[5].wait()
    wog[z] = wo_v[...]

    def pass_on(hop):
        for way, step in ((0, 1), (1, 7)):
            at = lax.rem(z + 8 * hop - step * hop, 8)
            remote(wog.at[at], wog.at[at], g_ssem, g_rsem.at[hop], ring(step), tp).start()


    pl.semaphore_wait(barrier, 12)

    partner = z * 8 + c + 1 - 2 * lax.rem(c, 2)

    def same_core(i):
        return pl.ds(pl.multiple_of(lax.rem(c + 8 - 2 * i, 8) * 32, 32), 32)

    def send_hidden(h):
        own = acts_t.at[h, own32, :]
        for i in (2, 1, 3):
            remote(own, own, acts_ssem, acts_rsem.at[h, i - 1], plane(2 * i), tp).start()
        remote(own, own, acts_ssem, d_rsem.at[h], partner, tp).start()

    def send_weights(t):
        for r in (4, 3, 5, 2, 6, 1, 7):
            remote(wsend.at[lax.rem(c + r, 8), t], wblk.at[t, own32, :], w_ssem, w_rsem.at[t], plane(r), tp).start()

    def hand_over(h):
        for i in (1, 3, 2):
            arrived(acts_t.at[h, own32, :], acts_rsem.at[h, i - 1])
            block = acts_t.at[h, same_core(i), :]
            remote(block, block, d_ssem, d_rsem.at[h], partner, tp).start()

    def turn(h):
        arrived(acts_t.at[h, 0:128, :], d_rsem.at[h])
        for i in range(2):
            block = jnp.transpose(acts_t[h, :, i * 128:(i + 1) * 128].astype(F32))
            rows = slice(h * 256 + i * 128, h * 256 + i * 128 + 128)
            acts_f[rows, :] = block
            acts_b[rows, :] = block.astype(BF16)

    send_hidden(0)
    send_weights(0)
    pass_on(0)
    send_weights(1)
    send_weights(2)
    send_hidden(1)
    for r in (4, 3, 5, 2, 6, 1, 7):
        remote(kbuf.at[c], kbuf.at[c], k_ssem, k_rsem, plane(r), tp).start()
        remote(qbuf.at[c], qbuf.at[c], q_ssem, q_rsem, plane(r), tp).start()

    for cp in loads[6:]:
        cp.wait()
    raww_v, rawr_v, tw_v, tr_v = raw_v.at[0], raw_v.at[1], tap_v.at[0], tap_v.at[1]
    bias_v, rate_v, dgain_v = head_v.at[0], head_v.at[1], head_v.at[2]
    row8 = lax.broadcasted_iota(jnp.int32, (8, 1), 0)
    tok = lax.rem(row8, 4)

    def down(x, d):
        if d == 0:
            return x
        return jnp.where(tok >= d, pltpu.roll(x, d, axis=0), 0.0)

    def up(x, d):
        return jnp.where(tok + d < 4, pltpu.roll(x, 8 - d, axis=0), 0.0)

    def last_conv(raw, taps):
        t = taps[...].astype(F32)
        rows = [raw[k].astype(F32) for k in range(7)]
        parts = []
        for i in range(4):
            total = rows[i] * t[0:1]
            for j in range(1, 4):
                total = total + rows[i + j] * t[j:j + 1]
            parts.append(total)
        return silu(jnp.concatenate([p[s:s + 1] for s in range(2) for p in parts], axis=0))

    def base_conv(raw, taps, lo, hi):
        t = taps[...].astype(F32)
        rows = [raw[k].astype(F32) for k in range(7)]
        second = lax.broadcasted_iota(jnp.int32, (2, 1), 0) == 1
        a = jnp.where(second, acc_s[1], acc_s[0])
        win = []
        for i in range(3):
            w = rows[4 + i]
            for k in range(3, -1, -1):
                w = jnp.where(a == k, rows[k + i], w)
            win.append(w)
        w0, w1, w2 = win
        parts = [w0 * t[0:1] + w1 * t[1:2] + w2 * t[2:3], w1 * t[0:1] + w2 * t[1:2], w2 * t[0:1],
                 jnp.zeros((2, hi - lo), F32)]
        base[:, lo:hi] = jnp.concatenate([p[s:s + 1] for s in range(2) for p in parts], axis=0)

    lastv = last_conv(rawv_v, tv_v)
    lastw = last_conv(raww_v, tw_v)
    base_conv(rawv_v, tv_v, 0, 1024)
    base_conv(raww_v, tw_v, 1024, 1536)
    base_conv(rawr_v, tr_v, 1536, 2048)

    rate_e = -jnp.exp(rate_v[...])
    bias_r = bias_v[...]
    pstep = softplus(jnp.concatenate([ppre_v[0], ppre_v[1]], axis=0) + bias_r)
    pextra = jnp.concatenate([extra_v[0, 0:4], extra_v[1, 0:4]], axis=0)
    nextra = jnp.concatenate([extra_v[0, 4:8], extra_v[1, 4:8]], axis=0)
    limit = jnp.where(row8 < 4, acc_s[0], acc_s[1])
    live = jnp.where(tok < limit, 1.0, 0.0)
    kept = (rate_e * pstep + pextra) * live
    tail = up(kept, 1) + up(kept, 2) + up(kept, 3)
    coef = live * jnp.exp(tail) * pstep
    etot = jnp.exp(kept + tail)
    lane128 = lax.broadcasted_iota(jnp.int32, (8, 128), 1)
    low_half = lane128 < 64

    def spread(e, i):
        a = jnp.broadcast_to(e[:, 2 * i:2 * i + 1], (8, 128))
        b = jnp.broadcast_to(e[:, 2 * i + 1:2 * i + 2], (8, 128))
        return jnp.where(low_half, a, b)

    for g in range(4):
        vals = [lastv[:, (2 * g + i) * 128:(2 * g + i + 1) * 128] * spread(coef, 2 * g + i) for i in range(2)]
        weighted = jnp.concatenate(vals, axis=1)
        lw = lastw[:, g * 128:(g + 1) * 128]
        for s in range(2):
            own_seq = (row8 < 4) if s == 0 else (row8 >= 4)
            added = lax.dot_general(
                weighted, jnp.where(own_seq, lw, 0.0), (((0,), (0,)), ((), ())),
                precision=lax.Precision.HIGHEST, preferred_element_type=F32,
            )
            for i in range(4):
                h = g * 4 + i
                rows = slice(i * 64, i * 64 + 64)
                factor = jnp.broadcast_to(etot[s * 4:s * 4 + 1, h:h + 1], (64, 128))
                new = factor * st_out[s, g, rows, :] + added[rows, :]
                st_out[s, g, rows, :] = new
                state_b[s, g, rows, :] = new.astype(BF16)

    hand_over(0)
    arrived(wog.at[0:2], g_rsem.at[0])
    pass_on(1)
    turn(0)
    turned = (((1,), (1,)), ((), ()))
    even = lax.rem(z, 2) == 0
    far = lax.rem(z + 2 + 4 * lax.rem(z, 2), 8)

    def to_owners(src, t, slot, dz, ssem, rsem):
        for r in range(0 if dz else 1, 8):
            cc = lax.rem(c + r, 8)
            remote(src.at[cc], frecv.at[t, slot, c], ssem, rsem, lax.rem(z + dz, 8) * 8 + cc, tp).start()

    lhs = acts_b[0:192, :]
    for t in range(3):
        arrived(wblk.at[t, 0:224, :], w_rsem.at[t])
        part = jnp.dot(lhs, wblk[t], preferred_element_type=F32)
        for i, (kind, away, to) in enumerate(((0, 3, ring(1)), (2, 4, far * 8 + c), (1, 5, ring(7)))):
            zz = lax.rem(z + away, 8)
            psend[t, zz] = part[i * 64:i * 64 + 64, :].reshape(8, 8, 128).astype(BF16)
            remote(psend.at[t, zz], arecv.at[t, kind], a_ssem, a_rsem.at[t], to, tp).start()
    hand_over(1)
    turn(1)
    arrived(kbuf.at[0:7], k_rsem)
    arrived(qbuf.at[0:7], q_rsem)
    own_rows = jnp.concatenate(
        [acts_f[pl.ds(pl.multiple_of(k * 64 + c * 8, 8), 8), :] for k in range(8)], axis=0
    ).astype(BF16)
    step_t = jnp.concatenate([kbuf[j].astype(F32)[:, 0:32] for j in range(8)], axis=1)
    step_t = jnp.concatenate([step_t, jnp.zeros((112, 256), F32)], axis=0).astype(BF16)
    ext = lax.dot_general(own_rows, step_t, turned, preferred_element_type=F32)
    qsum = qbuf[0]
    for j in range(1, 8):
        qsum = qsum + qbuf[j]
    qeven = pltpu.roll(qsum, 64, axis=1)
    for k in range(8):
        row = (qsum if k % 2 else qeven)[k // 2:k // 2 + 1, :]
        mixture = jnp.where(low_half, ext[k * 8:k * 8 + 8, :], jnp.broadcast_to(row, (8, 128)))
        high = mixture.astype(BF16).astype(F32)
        rest = (mixture - high).astype(BF16).astype(F32)
        lower = jnp.where(low_half, pltpu.roll(jnp.where(low_half, rest, 0.0), 16, axis=1), rest)
        esend[lax.rem(z + 3 + k, 8)] = jnp.where(low_half, high + lower, jnp.where(row8 < 4, high, lower)).astype(BF16)
    erecv[z] = esend[z]
    remote(esend.at[lax.rem(z + 4, 8)], efar, e_ssem, x_rsem, far * 8 + c, tp).start()
    lhs = acts_b[192:512, :]
    for t in range(3):
        part = jnp.dot(lhs, wblk[t], preferred_element_type=F32)
        for i, away in enumerate((6, 7, 0, 1, 2)):
            psend[t, lax.rem(z + away, 8)] = part[i * 64:i * 64 + 64, :].reshape(8, 8, 128).astype(BF16)
    frecv[:, 0, c] = psend[:, z, c]
    for slot, dz, rsem in ((1, 1, b_rsem), (2, 7, b_rsem), (0, 0, h_rsem)):
        for r in range(0 if dz else 1, 8):
            cc = lax.rem(c + r, 8)
            zz = lax.rem(z + dz, 8)
            remote(
                psend.at[:, zz, cc], frecv.at[:, slot, c], b_ssem if dz else h_ssem, rsem, zz * 8 + cc, tp
            ).start()
    arrived(wog.at[0:2], g_rsem.at[1])
    for r in (3, 5, 2, 6, 1, 7):
        remote(esend.at[lax.rem(z + r, 8)], erecv.at[z], e_ssem, e_rsem, ring(r), tp).start()
    for t in range(3):
        arrived(arecv.at[t], a_rsem.at[t])
        extra_block = arecv[t, 2].astype(F32)
        zero_block = jnp.zeros_like(extra_block)
        plus = psend[t, lax.rem(z + 2, 8)].astype(F32) + arecv[t, 0].astype(F32)
        minus = psend[t, lax.rem(z + 6, 8)].astype(F32) + arecv[t, 1].astype(F32)
        bsend[t, 0] = (plus + jnp.where(even, extra_block, zero_block)).astype(BF16)
        bsend[t, 1] = (minus + jnp.where(even, zero_block, extra_block)).astype(BF16)
        to_owners(bsend.at[t, 0], t, 3, 2, p_ssem, p_rsem.at[t])
        to_owners(bsend.at[t, 1], t, 4, 6, p_ssem, p_rsem.at[t])
    arrived(efar, x_rsem)
    back = lax.rem(z + 6 + 4 * lax.rem(z, 2), 8)
    remote(efar, erecv.at[back], x_ssem, e_rsem, far * 8 + c, tp).start()
    pass_on(2)

    arrived(erecv.at[0:7], e_rsem)
    remote(wog.at[back], wog.at[back], g_ssem, g_rsem.at[3], far * 8 + c, tp).start()
    esum = erecv[0].astype(F32)
    for k in range(1, 8):
        esum = esum + erecv[k].astype(F32)
    own_lane = lane128 == 64 + c * 8 + row8
    qrow = jnp.broadcast_to(esum[0:1, :] + esum[4:5, :], (8, 128))
    inverse = lax.rsqrt(jnp.sum(jnp.where(own_lane, qrow, 0.0), axis=1, keepdims=True) / 2048.0 + EPS)
    esum = esum + pltpu.roll(esum, 112, axis=1)
    step = softplus(inverse * esum[:, 0:16] + bias_r)
    decay = rate_e * step + nextra
    cum = decay + down(decay, 1) + down(decay, 2) + down(decay, 3)
    pair_w = []
    for d in range(4):
        w = jnp.exp(jnp.minimum(cum - down(cum, d), 0.0)) * down(step, d)
        pair_w.append(jnp.where(tok >= d, w, 0.0))
    ecum = jnp.exp(cum)

    def settle(t):
        if t == 0:
            arrived(frecv.at[:, 1:3], b_rsem)
            arrived(frecv.at[:, 0, 0:7], h_rsem)
        arrived(frecv.at[t, 3:5], p_rsem.at[t])

    def fresh(t, j):
        x = frecv[t, 0, j].astype(F32)
        for slot in range(1, 5):
            x = x + frecv[t, slot, j].astype(F32)
        return (x * inverse).astype(BF16).astype(F32)

    dg = jnp.broadcast_to(dgain_v[...], (8, 16))
    settle(0)

    def conv(x, lo, taps, at):
        t = taps[:, at:at + 128].astype(F32)
        y = base[:, lo:lo + 128] + x * t[3:4]
        for d in range(1, 4):
            y = y + down(x, d) * t[3 - d:4 - d]
        return silu(y)

    writes = [conv(fresh(0, g), 1024 + g * 128, tw_v, g * 128) for g in range(4)]
    reads = [conv(fresh(0, 4 + g), 1536 + g * 128, tr_v, g * 128) for g in range(4)]
    carried, inner = [], []
    for g in range(4):
        rb = reads[g].astype(BF16)
        both = [
            lax.dot_general(rb, state_b[s, g], turned, preferred_element_type=F32) for s in range(2)
        ]
        carried.append(jnp.where(row8 < 4, both[0], both[1]))
        inner.append([jnp.sum(reads[g] * down(writes[g], d), axis=1, keepdims=True) for d in range(4)])
    for half in range(2):
        settle(1 + half)
        gated = []
        for i in range(4):
            j = 4 * half + i
            g = j // 2
            value = conv(fresh(1 + half, i), j * 128, tv_v, j * 128)
            m = spread(ecum, j) * carried[g][:, (j % 2) * 128:(j % 2) * 128 + 128] + spread(dg, j) * value
            for d in range(4):
                m = m + (inner[g][d] * spread(pair_w[d], j)) * down(value, d)
            gated.append(m * silu(fresh(1 + half, 4 + i)))
        normed = []
        for a, b in ((0, 1), (2, 3)):
            mean = jnp.sum(gated[a] * gated[a] + gated[b] * gated[b], axis=1, keepdims=True) / 256.0
            scale = lax.rsqrt(mean + EPS)
            for i in (a, b):
                j = 4 * half + i
                normed.append(gated[i] * scale * ngain_v[:, j * 128:(j + 1) * 128])
        nrm[half, c] = jnp.concatenate(normed, axis=1).astype(BF16)
        for r in (4, 3, 5, 2, 6, 1, 7):
            remote(nrm.at[half, c], nrm.at[half, c], n_ssem, n_rsem.at[half], plane(r), tp).start()
    arrived(wog.at[0:2], g_rsem.at[2])
    for r in range(1, 4):
        pl.semaphore_signal(ready, inc=1, device_id={"kv": kv, "tp": lax.rem(tp + r, 4)}, device_id_type=MESH)
    arrived(wog.at[0], g_rsem.at[3])
    pl.semaphore_wait(ready, 3)
    wall = wog[...].reshape(256, 1024)
    p = None
    for i in range(2):
        arrived(nrm.at[i, 0:7], n_rsem.at[i])
        block = nrm[i].astype(F32).reshape(64, 512).astype(BF16)
        q = lax.dot_general(wall[:, i * 512:(i + 1) * 512], block, turned, preferred_element_type=F32)
        p = q if p is None else p + q
    for k in range(8):
        packed = jnp.concatenate([p[k * 32:k * 32 + 16, :], p[k * 32 + 16:k * 32 + 32, :]], axis=1)
        osend[k] = packed.astype(BF16)

    owner = lax.div(z, 2)
    slot = tp * 2 + lax.rem(z, 2)
    for r in (4, 3, 5, 2, 6, 1, 7):
        remote(osend.at[lax.rem(z + r, 8)], orecv.at[slot], o_ssem, o_rsem, ring(r), owner).start()

    @pl.when(owner != tp)
    def _():
        remote(osend.at[z], orecv.at[slot], o_ssem, o_rsem, kv, owner).start()
        arrived(orecv.at[0:8], o_rsem)

    @pl.when(owner == tp)
    def _():
        orecv[slot] = osend[z]
        arrived(orecv.at[0:7], o_rsem)

    sums = []
    for q in range(2):
        s4 = orecv[q].astype(F32)
        for x in range(1, 4):
            s4 = s4 + orecv[x * 2 + q].astype(F32)
        sums.append(s4)
    lane16 = lax.broadcasted_iota(jnp.int32, (16, 128), 1) < 64
    top = jnp.where(lane16, sums[0], pltpu.roll(sums[1], 64, axis=1))
    bottom = jnp.where(lane16, pltpu.roll(sums[0], 64, axis=1), sums[1])
    out_ref[...] = jnp.concatenate([top, bottom], axis=0).astype(BF16)

    for ref, sem in (
        (acts_t.at[:, 0:128, :], acts_ssem), (acts_t.at[:, 0:96, :], d_ssem), (wsend.at[0:7], w_ssem),
        (kbuf.at[0:7], k_ssem), (qbuf.at[0:7], q_ssem), (wog.at[0:7], g_ssem), (arecv, a_ssem),
        (frecv.at[:, 3:5], p_ssem), (frecv.at[:, 0, 0:7], h_ssem), (frecv.at[:, 1:3], b_ssem), (erecv.at[0:7], e_ssem), (efar, x_ssem),
        (nrm.at[:, 0:7], n_ssem),
    ):
        sent(ref, sem)

    @pl.when(owner != tp)
    def _():
        sent(osend.at[0:8], o_ssem)

    @pl.when(owner == tp)
    def _():
        sent(osend.at[0:7], o_ssem)


def hand_out(a, b, a_out, b_out, sem):
    copies = [pltpu.make_async_copy(b.at[s, pl.ds(g, 2)], b_out.at[s, pl.ds(g, 2)], sem.at[2 * s + g // 2])
              for s in range(2) for g in (0, 2)]
    copies.append(pltpu.make_async_copy(a, a_out, sem.at[4]))
    for cp in copies:
        cp.start()
    for cp in copies:
        cp.wait()


def per_device(
    hidden_vectors, input_norm_gain, gate_matrix, value_matrix, write_matrix, read_matrix, step_matrix,
    raw_value_rows, raw_write_rows, raw_read_rows, value_filter_taps, write_filter_taps, read_filter_taps,
    step_size_bias, rate_logarithm, direct_path_gain, prior_step_preact, extra_log_decay, accepted, prior_state,
    group_norm_gain, output_matrix,
):
    operands = [
        accepted, hidden_vectors.T, input_norm_gain.reshape(1, 32), gate_matrix, value_matrix, write_matrix, read_matrix,
        step_matrix.T, raw_value_rows.transpose(1, 0, 2), raw_write_rows.transpose(1, 0, 2),
        raw_read_rows.transpose(1, 0, 2), value_filter_taps, write_filter_taps,
        read_filter_taps, step_size_bias.reshape(1, 16), rate_logarithm.reshape(1, 16),
        direct_path_gain.reshape(1, 16), prior_step_preact, extra_log_decay, prior_state.reshape(2, 4, 256, 128),
        group_norm_gain.reshape(1, 1024), output_matrix.T,
    ]
    buffers = [
        pltpu.SMEM((2,), jnp.int32),
        pltpu.VMEM((32, 512), BF16),
        pltpu.VMEM((1, 32), F32),
        pltpu.VMEM((2, 32, 1024), BF16),
        pltpu.VMEM((2, 32, 512), BF16),
        pltpu.VMEM((16, 32), BF16),
        pltpu.VMEM((32, 1024), BF16),
        pltpu.VMEM((7, 2, 1024), BF16),
        pltpu.VMEM((2, 7, 2, 512), BF16),
        pltpu.VMEM((4, 1024), BF16),
        pltpu.VMEM((2, 4, 512), BF16),
        pltpu.VMEM((3, 1, 16), F32),
        pltpu.VMEM((2, 4, 16), F32),
        pltpu.VMEM((2, 8, 16), F32),
        pltpu.VMEM((1, 1024), F32),
    ]
    dma = pltpu.SemaphoreType.DMA
    scratch = buffers + [
        pltpu.VMEM((2, 256, 256), BF16),
        pltpu.VMEM((8, 3, 32, 128), BF16),
        pltpu.VMEM((3, 256, 128), BF16),
        pltpu.VMEM((8, 16, 128), BF16),
        pltpu.VMEM((8, 4, 128), F32),
        pltpu.VMEM((512, 256), F32),
        pltpu.VMEM((512, 256), BF16),
        pltpu.VMEM((3, 8, 8, 8, 128), BF16),
        pltpu.VMEM((3, 3, 8, 8, 128), BF16),
        pltpu.VMEM((3, 2, 8, 8, 128), BF16),
        pltpu.VMEM((3, 5, 8, 8, 128), BF16),
        pltpu.VMEM((8, 8, 128), BF16),
        pltpu.VMEM((8, 8, 128), BF16),
        pltpu.VMEM((8, 128), BF16),
        pltpu.VMEM((2, 8, 8, 512), BF16),
        pltpu.VMEM((8, 32, 1024), BF16),
        pltpu.VMEM((8, 16, 128), BF16),
        pltpu.VMEM((8, 16, 128), BF16),
        pltpu.VMEM((8, 2048), F32),
        pltpu.VMEM((2, 4, 256, 128), BF16),
        dma((16,)),
        dma((2, 3)), dma((2,)), dma((3,)), dma, dma, dma((4,)), dma((3,)), dma((3,)), dma, dma, dma, dma, dma((2,)), dma,
        pltpu.SemaphoreType.REGULAR,
    ]
    operands = [pltpu.with_memory_space_constraint(x, pltpu.HBM) for x in operands]
    out, state = pl.pallas_call(
        mixer_kernel,
        out_shape=(
            pltpu.VMEM((32, 128), BF16),
            pltpu.VMEM((2, 4, 256, 128), F32),
        ),
        in_specs=[pl.BlockSpec(memory_space=pl.ANY)] * len(operands),
        out_specs=(pl.BlockSpec(memory_space=pltpu.VMEM), pl.BlockSpec(memory_space=pltpu.VMEM)),
        scratch_shapes=scratch,
        compiler_params=pltpu.CompilerParams(
            collective_id=0, has_side_effects=True, vmem_limit_bytes=32 * 1024 * 1024
        ),
        cost_estimate=pl.CostEstimate(flops=10**9, bytes_accessed=4 * 10**6, transcendentals=10**5),
        name="mixer",
    )(*operands)
    out, state = [pltpu.with_memory_space_constraint(x, pltpu.VMEM) for x in (out, state)]
    out, state = pl.pallas_call(
        hand_out,
        out_shape=(
            jax.ShapeDtypeStruct((32, 128), BF16),
            jax.ShapeDtypeStruct((2, 4, 256, 128), F32),
        ),
        in_specs=[pl.BlockSpec(memory_space=pltpu.VMEM)] * 2,
        out_specs=(pl.BlockSpec(memory_space=pl.ANY),) * 2,
        scratch_shapes=[pltpu.SemaphoreType.DMA((5,))],
        compiler_params=pltpu.CompilerParams(vmem_limit_bytes=32 * 1024 * 1024),
        name="hand_out",
    )(out, state)
    return out.T, state.reshape(2, 16, 64, 128)


def solution(mesh):
    return jax.shard_map(
        per_device,
        mesh=mesh,
        in_specs=(
            P(None, "kv"),
            P("kv"),
            P("kv", "tp"),
            P("kv", "tp"),
            P("kv", "tp"),
            P("kv", "tp"),
            P("kv", "tp"),
            P("kv", None, "tp"),
            P("kv", None, "tp"),
            P("kv", None, "tp"),
            P(None, "tp"),
            P(None, "tp"),
            P(None, "tp"),
            P("tp"),
            P("tp"),
            P("tp"),
            P("kv", None, "tp"),
            P("kv", None, "tp"),
            P("kv"),
            P("kv", "tp", None, None),
            P("tp"),
            P("tp", "kv"),
        ),
        out_specs=(P("tp", "kv"), P("kv", "tp", None, None)),
        check_vma=False,
    )
```

```python
import jax
import jax.numpy as jnp
from jax import lax
from jax.experimental import pallas as pl
from jax.experimental.pallas import tpu as pltpu
from jax.sharding import PartitionSpec as P

MESH = pl.DeviceIdType.MESH
F32 = jnp.float32
BF16 = jnp.bfloat16
EPS = 1e-6


def silu(x):
    return x / (1.0 + jnp.exp(-x))


def softplus(x):
    return jnp.maximum(x, 0.0) + jnp.log1p(jnp.exp(-jnp.abs(x)))


def mixer_kernel(
    acc, hid, gain, wg, wv, ww, wr, ws, rawv, raww, rawr, tv, tw, tr, bias, rate, dgain, ppre, extra, prior, ngain, wo,
    orecv, st_out,
    acc_s, hid_v, gain_v, wide_v, narrow_v, ws_v, wo_v, rawv_v, raw_v, tv_v, tap_v, head_v, ppre_v, extra_v, ngain_v,
    acts_t, wsend, wblk, kbuf, qbuf, acts_f, acts_b, psend, arecv, bsend, frecv, esend, erecv, efar, nrm, wog, osend,
    base, state_b,
    lsem, acts_rsem, d_rsem, w_rsem, k_rsem, q_rsem, g_rsem, a_rsem, p_rsem, h_rsem, b_rsem, e_rsem, x_rsem, n_rsem, o_rsem,
    ready,
):
    kv = lax.axis_index("kv")
    tp = lax.axis_index("tp")
    z = lax.div(kv, 8)
    c = lax.rem(kv, 8)

    def plane(r):
        return z * 8 + lax.rem(c + r, 8)

    def ring(r):
        return lax.rem(z + r, 8) * 8 + c

    def remote(src, dst, ssem, rsem, kv_to, tp_to):
        return pltpu.make_async_remote_copy(
            src_ref=src, dst_ref=dst, send_sem=ssem, recv_sem=rsem,
            device_id={"kv": kv_to, "tp": tp_to}, device_id_type=MESH,
        )

    acts_ssem, d_ssem, w_ssem, k_ssem, q_ssem, g_ssem, a_ssem, p_ssem, h_ssem, e_ssem, x_ssem, n_ssem, o_ssem, b_ssem = [
        lsem.at[i] for i in range(14)
    ]

    def arrived(ref, sem):
        remote(ref, ref, acts_ssem, sem, kv, tp).wait_recv()

    def sent(ref, sem):
        remote(ref, ref, sem, e_rsem, kv, tp).wait_send()

    barrier = pltpu.get_barrier_semaphore()
    for r in range(1, 8):
        pl.semaphore_signal(barrier, inc=1, device_id={"kv": plane(r), "tp": tp}, device_id_type=MESH)
    for r in (1, 7):
        pl.semaphore_signal(barrier, inc=1, device_id={"kv": ring(r), "tp": tp}, device_id_type=MESH)
    for r in range(1, 4):
        pl.semaphore_signal(barrier, inc=1, device_id={"kv": kv, "tp": lax.rem(tp + r, 4)}, device_id_type=MESH)

    pairs = [
        ([hid], hid_v), ([gain], gain_v), ([wg, wv], wide_v), ([ww, wr], narrow_v), ([ws], ws_v), ([wo], wo_v),
        ([acc], acc_s), ([rawv], rawv_v), ([raww, rawr], raw_v), ([tv], tv_v), ([tw, tr], tap_v),
        ([bias, rate, dgain], head_v), ([ppre], ppre_v), ([extra], extra_v), ([ngain], ngain_v), ([prior], st_out),
    ]
    loads = []
    for i, (sources, target) in enumerate(pairs):
        for j, source in enumerate(sources):
            pltpu.make_async_copy(source, target.at[j] if len(sources) > 1 else target, lsem.at[i]).start()
        loads.append(pltpu.make_async_copy(target, target, lsem.at[i]))

    own32 = pl.ds(pl.multiple_of(c * 32, 32), 32)
    loads[0].wait()
    loads[1].wait()
    diag = lax.broadcasted_iota(jnp.int32, (32, 32), 0) == lax.broadcasted_iota(jnp.int32, (32, 32), 1)
    gcol = jnp.sum(jnp.where(diag, jnp.broadcast_to(gain_v[...], (32, 32)), 0.0), axis=1, keepdims=True)
    hidden = hid_v[...].astype(F32)
    hidden = pltpu.roll(hidden, lax.rem(13 - z, 8) * 64, axis=1)
    scaled = (hidden * gcol).astype(BF16)
    for h in range(2):
        acts_t[h, own32, :] = scaled[:, h * 256:(h + 1) * 256]
    squares = jnp.sum(hidden * hidden, axis=0, keepdims=True)
    qbuf[c] = jnp.concatenate([squares[:, i * 128:(i + 1) * 128] for i in range(4)], axis=0)
    for i in range(2, 5):
        loads[i].wait()
    wg_v, wv_v, ww_v, wr_v = wide_v.at[0], wide_v.at[1], narrow_v.at[0], narrow_v.at[1]
    for j in range(8):
        near = slice((j % 4) * 128, (j % 4) * 128 + 128)
        wsend[j, 0] = (ww_v if j < 4 else wr_v)[:, near]
        for h in range(2):
            lane = slice((j % 4 + 4 * h) * 128, (j % 4 + 4 * h) * 128 + 128)
            wsend[j, 1 + h] = (wv_v if j < 4 else wg_v)[:, lane]
    for t in range(3):
        wblk[t, own32, :] = wsend[c, t]
    kbuf[c] = jnp.concatenate([ws_v[...].astype(F32), jnp.zeros((16, 96), F32)], axis=1).astype(BF16)

    loads[5].wait()
    wog[z] = wo_v[...]

    def pass_on(hop):
        for way, step in ((0, 1), (1, 7)):
            at = lax.rem(z + 8 * hop - step * hop, 8)
            remote(wog.at[at], wog.at[at], g_ssem, g_rsem.at[hop], ring(step), tp).start()


    pl.semaphore_wait(barrier, 12)

    partner = z * 8 + c + 1 - 2 * lax.rem(c, 2)

    def same_core(i):
        return pl.ds(pl.multiple_of(lax.rem(c + 8 - 2 * i, 8) * 32, 32), 32)

    def send_hidden(h):
        own = acts_t.at[h, own32, :]
        for i in (2, 1, 3):
            remote(own, own, acts_ssem, acts_rsem.at[h, i - 1], plane(2 * i), tp).start()
        remote(own, own, acts_ssem, d_rsem.at[h], partner, tp).start()

    def send_weights(t):
        for r in (4, 3, 5, 2, 6, 1, 7):
            remote(wsend.at[lax.rem(c + r, 8), t], wblk.at[t, own32, :], w_ssem, w_rsem.at[t], plane(r), tp).start()

    def hand_over(h):
        for i in (1, 3, 2):
            arrived(acts_t.at[h, own32, :], acts_rsem.at[h, i - 1])
            block = acts_t.at[h, same_core(i), :]
            remote(block, block, d_ssem, d_rsem.at[h], partner, tp).start()

    def turn(h):
        arrived(acts_t.at[h, 0:128, :], d_rsem.at[h])
        for i in range(2):
            block = jnp.transpose(acts_t[h, :, i * 128:(i + 1) * 128].astype(F32))
            rows = slice(h * 256 + i * 128, h * 256 + i * 128 + 128)
            acts_f[rows, :] = block
            acts_b[rows, :] = block.astype(BF16)

    send_hidden(0)
    send_weights(0)
    pass_on(0)
    send_weights(1)
    send_weights(2)
    send_hidden(1)
    for r in (4, 3, 5, 2, 6, 1, 7):
        remote(kbuf.at[c], kbuf.at[c], k_ssem, k_rsem, plane(r), tp).start()
        remote(qbuf.at[c], qbuf.at[c], q_ssem, q_rsem, plane(r), tp).start()

    for cp in loads[6:]:
        cp.wait()
    raww_v, rawr_v, tw_v, tr_v = raw_v.at[0], raw_v.at[1], tap_v.at[0], tap_v.at[1]
    bias_v, rate_v, dgain_v = head_v.at[0], head_v.at[1], head_v.at[2]
    row8 = lax.broadcasted_iota(jnp.int32, (8, 1), 0)
    tok = lax.rem(row8, 4)

    def down(x, d):
        if d == 0:
            return x
        return jnp.where(tok >= d, pltpu.roll(x, d, axis=0), 0.0)

    def up(x, d):
        return jnp.where(tok + d < 4, pltpu.roll(x, 8 - d, axis=0), 0.0)

    def last_conv(raw, taps):
        t = taps[...].astype(F32)
        rows = [raw[k].astype(F32) for k in range(7)]
        parts = []
        for i in range(4):
            total = rows[i] * t[0:1]
            for j in range(1, 4):
                total = total + rows[i + j] * t[j:j + 1]
            parts.append(total)
        return silu(jnp.concatenate([p[s:s + 1] for s in range(2) for p in parts], axis=0))

    def base_conv(raw, taps, lo, hi):
        t = taps[...].astype(F32)
        rows = [raw[k].astype(F32) for k in range(7)]
        second = lax.broadcasted_iota(jnp.int32, (2, 1), 0) == 1
        a = jnp.where(second, acc_s[1], acc_s[0])
        win = []
        for i in range(3):
            w = rows[4 + i]
            for k in range(3, -1, -1):
                w = jnp.where(a == k, rows[k + i], w)
            win.append(w)
        w0, w1, w2 = win
        parts = [w0 * t[0:1] + w1 * t[1:2] + w2 * t[2:3], w1 * t[0:1] + w2 * t[1:2], w2 * t[0:1],
                 jnp.zeros((2, hi - lo), F32)]
        base[:, lo:hi] = jnp.concatenate([p[s:s + 1] for s in range(2) for p in parts], axis=0)

    lastv = last_conv(rawv_v, tv_v)
    lastw = last_conv(raww_v, tw_v)
    base_conv(rawv_v, tv_v, 0, 1024)
    base_conv(raww_v, tw_v, 1024, 1536)
    base_conv(rawr_v, tr_v, 1536, 2048)

    rate_e = -jnp.exp(rate_v[...])
    bias_r = bias_v[...]
    pstep = softplus(jnp.concatenate([ppre_v[0], ppre_v[1]], axis=0) + bias_r)
    pextra = jnp.concatenate([extra_v[0, 0:4], extra_v[1, 0:4]], axis=0)
    nextra = jnp.concatenate([extra_v[0, 4:8], extra_v[1, 4:8]], axis=0)
    limit = jnp.where(row8 < 4, acc_s[0], acc_s[1])
    live = jnp.where(tok < limit, 1.0, 0.0)
    kept = (rate_e * pstep + pextra) * live
    tail = up(kept, 1) + up(kept, 2) + up(kept, 3)
    coef = live * jnp.exp(tail) * pstep
    etot = jnp.exp(kept + tail)
    lane128 = lax.broadcasted_iota(jnp.int32, (8, 128), 1)
    low_half = lane128 < 64

    def spread(e, i):
        a = jnp.broadcast_to(e[:, 2 * i:2 * i + 1], (8, 128))
        b = jnp.broadcast_to(e[:, 2 * i + 1:2 * i + 2], (8, 128))
        return jnp.where(low_half, a, b)

    for g in range(4):
        vals = [lastv[:, (2 * g + i) * 128:(2 * g + i + 1) * 128] * spread(coef, 2 * g + i) for i in range(2)]
        weighted = jnp.concatenate(vals, axis=1)
        lw = lastw[:, g * 128:(g + 1) * 128]
        for s in range(2):
            own_seq = (row8 < 4) if s == 0 else (row8 >= 4)
            added = lax.dot_general(
                weighted, jnp.where(own_seq, lw, 0.0), (((0,), (0,)), ((), ())),
                precision=lax.Precision.HIGHEST, preferred_element_type=F32,
            )
            for i in range(4):
                h = g * 4 + i
                rows = slice(i * 64, i * 64 + 64)
                factor = jnp.broadcast_to(etot[s * 4:s * 4 + 1, h:h + 1], (64, 128))
                new = factor * st_out[s, g, rows, :] + added[rows, :]
                st_out[s, g, rows, :] = new
                state_b[s, g, rows, :] = new.astype(BF16)

    hand_over(0)
    arrived(wog.at[0:2], g_rsem.at[0])
    pass_on(1)
    turn(0)
    turned = (((1,), (1,)), ((), ()))
    even = lax.rem(z, 2) == 0
    far = lax.rem(z + 2 + 4 * lax.rem(z, 2), 8)

    def to_owners(src, t, slot, dz, ssem, rsem):
        for r in range(0 if dz else 1, 8):
            cc = lax.rem(c + r, 8)
            remote(src.at[cc], frecv.at[t, slot, c], ssem, rsem, lax.rem(z + dz, 8) * 8 + cc, tp).start()

    lhs = acts_b[0:192, :]
    for t in range(3):
        arrived(wblk.at[t, 0:224, :], w_rsem.at[t])
        part = jnp.dot(lhs, wblk[t], preferred_element_type=F32)
        for i, (kind, away, to) in ((1, (2, 4, far * 8 + c)), (0, (0, 3, ring(1))), (2, (1, 5, ring(7)))):
            zz = lax.rem(z + away, 8)
            psend[t, zz] = part[i * 64:i * 64 + 64, :].reshape(8, 8, 128).astype(BF16)
            remote(psend.at[t, zz], arecv.at[t, kind], a_ssem, a_rsem.at[t], to, tp).start()
    hand_over(1)
    turn(1)
    arrived(kbuf.at[0:7], k_rsem)
    arrived(qbuf.at[0:7], q_rsem)
    own_rows = jnp.concatenate(
        [acts_f[pl.ds(pl.multiple_of(k * 64 + c * 8, 8), 8), :] for k in range(8)], axis=0
    ).astype(BF16)
    step_t = jnp.concatenate([kbuf[j].astype(F32)[:, 0:32] for j in range(8)], axis=1)
    step_t = jnp.concatenate([step_t, jnp.zeros((112, 256), F32)], axis=0).astype(BF16)
    ext = lax.dot_general(own_rows, step_t, turned, preferred_element_type=F32)
    qsum = qbuf[0]
    for j in range(1, 8):
        qsum = qsum + qbuf[j]
    qeven = pltpu.roll(qsum, 64, axis=1)
    for k in range(8):
        row = (qsum if k % 2 else qeven)[k // 2:k // 2 + 1, :]
        mixture = jnp.where(low_half, ext[k * 8:k * 8 + 8, :], jnp.broadcast_to(row, (8, 128)))
        high = mixture.astype(BF16).astype(F32)
        rest = (mixture - high).astype(BF16).astype(F32)
        lower = jnp.where(low_half, pltpu.roll(jnp.where(low_half, rest, 0.0), 16, axis=1), rest)
        esend[lax.rem(z + 3 + k, 8)] = jnp.where(low_half, high + lower, jnp.where(row8 < 4, high, lower)).astype(BF16)
    erecv[z] = esend[z]
    remote(esend.at[lax.rem(z + 4, 8)], efar, e_ssem, x_rsem, far * 8 + c, tp).start()
    lhs = acts_b[192:512, :]
    for t in range(3):
        part = jnp.dot(lhs, wblk[t], preferred_element_type=F32)
        for i, away in enumerate((6, 7, 0, 1, 2)):
            psend[t, lax.rem(z + away, 8)] = part[i * 64:i * 64 + 64, :].reshape(8, 8, 128).astype(BF16)
    frecv[:, 0, c] = psend[:, z, c]
    for slot, dz, rsem in ((1, 1, b_rsem), (2, 7, b_rsem), (0, 0, h_rsem)):
        for r in range(0 if dz else 1, 8):
            cc = lax.rem(c + r, 8)
            zz = lax.rem(z + dz, 8)
            remote(
                psend.at[:, zz, cc], frecv.at[:, slot, c], b_ssem if dz else h_ssem, rsem, zz * 8 + cc, tp
            ).start()
    arrived(wog.at[0:2], g_rsem.at[1])
    for r in (3, 5, 2, 6, 1, 7):
        remote(esend.at[lax.rem(z + r, 8)], erecv.at[z], e_ssem, e_rsem, ring(r), tp).start()
    for t in range(3):
        arrived(arecv.at[t], a_rsem.at[t])
        extra_block = arecv[t, 2].astype(F32)
        zero_block = jnp.zeros_like(extra_block)
        plus = psend[t, lax.rem(z + 2, 8)].astype(F32) + arecv[t, 0].astype(F32)
        minus = psend[t, lax.rem(z + 6, 8)].astype(F32) + arecv[t, 1].astype(F32)
        bsend[t, 0] = (plus + jnp.where(even, extra_block, zero_block)).astype(BF16)
        bsend[t, 1] = (minus + jnp.where(even, zero_block, extra_block)).astype(BF16)
        to_owners(bsend.at[t, 0], t, 3, 2, p_ssem, p_rsem.at[t])
        to_owners(bsend.at[t, 1], t, 4, 6, p_ssem, p_rsem.at[t])
    arrived(efar, x_rsem)
    back = lax.rem(z + 6 + 4 * lax.rem(z, 2), 8)
    remote(efar, erecv.at[back], x_ssem, e_rsem, far * 8 + c, tp).start()
    pass_on(2)

    arrived(erecv.at[0:7], e_rsem)
    remote(wog.at[back], wog.at[back], g_ssem, g_rsem.at[3], far * 8 + c, tp).start()
    esum = erecv[0].astype(F32)
    for k in range(1, 8):
        esum = esum + erecv[k].astype(F32)
    own_lane = lane128 == 64 + c * 8 + row8
    qrow = jnp.broadcast_to(esum[0:1, :] + esum[4:5, :], (8, 128))
    inverse = lax.rsqrt(jnp.sum(jnp.where(own_lane, qrow, 0.0), axis=1, keepdims=True) / 2048.0 + EPS)
    esum = esum + pltpu.roll(esum, 112, axis=1)
    step = softplus(inverse * esum[:, 0:16] + bias_r)
    decay = rate_e * step + nextra
    cum = decay + down(decay, 1) + down(decay, 2) + down(decay, 3)
    pair_w = []
    for d in range(4):
        w = jnp.exp(jnp.minimum(cum - down(cum, d), 0.0)) * down(step, d)
        pair_w.append(jnp.where(tok >= d, w, 0.0))
    ecum = jnp.exp(cum)

    def settle(t):
        if t == 0:
            arrived(frecv.at[:, 1:3], b_rsem)
            arrived(frecv.at[:, 0, 0:7], h_rsem)
        arrived(frecv.at[t, 3:5], p_rsem.at[t])

    def fresh(t, j):
        x = frecv[t, 0, j].astype(F32)
        for slot in range(1, 5):
            x = x + frecv[t, slot, j].astype(F32)
        return (x * inverse).astype(BF16).astype(F32)

    dg = jnp.broadcast_to(dgain_v[...], (8, 16))
    settle(0)

    def conv(x, lo, taps, at):
        t = taps[:, at:at + 128].astype(F32)
        y = base[:, lo:lo + 128] + x * t[3:4]
        for d in range(1, 4):
            y = y + down(x, d) * t[3 - d:4 - d]
        return silu(y)

    writes = [conv(fresh(0, g), 1024 + g * 128, tw_v, g * 128) for g in range(4)]
    reads = [conv(fresh(0, 4 + g), 1536 + g * 128, tr_v, g * 128) for g in range(4)]
    carried, inner = [], []
    for g in range(4):
        rb = reads[g].astype(BF16)
        both = [
            lax.dot_general(rb, state_b[s, g], turned, preferred_element_type=F32) for s in range(2)
        ]
        carried.append(jnp.where(row8 < 4, both[0], both[1]))
        inner.append([jnp.sum(reads[g] * down(writes[g], d), axis=1, keepdims=True) for d in range(4)])
    for half in range(2):
        settle(1 + half)
        gated = []
        for i in range(4):
            j = 4 * half + i
            g = j // 2
            value = conv(fresh(1 + half, i), j * 128, tv_v, j * 128)
            m = spread(ecum, j) * carried[g][:, (j % 2) * 128:(j % 2) * 128 + 128] + spread(dg, j) * value
            for d in range(4):
                m = m + (inner[g][d] * spread(pair_w[d], j)) * down(value, d)
            gated.append(m * silu(fresh(1 + half, 4 + i)))
        normed = []
        for a, b in ((0, 1), (2, 3)):
            mean = jnp.sum(gated[a] * gated[a] + gated[b] * gated[b], axis=1, keepdims=True) / 256.0
            scale = lax.rsqrt(mean + EPS)
            for i in (a, b):
                j = 4 * half + i
                normed.append(gated[i] * scale * ngain_v[:, j * 128:(j + 1) * 128])
        nrm[half, c] = jnp.concatenate(normed, axis=1).astype(BF16)
        for r in (4, 3, 5, 2, 6, 1, 7):
            remote(nrm.at[half, c], nrm.at[half, c], n_ssem, n_rsem.at[half], plane(r), tp).start()
    arrived(wog.at[0:2], g_rsem.at[2])
    for r in range(1, 4):
        pl.semaphore_signal(ready, inc=1, device_id={"kv": kv, "tp": lax.rem(tp + r, 4)}, device_id_type=MESH)
    arrived(wog.at[0], g_rsem.at[3])
    pl.semaphore_wait(ready, 3)
    wall = wog[...].reshape(256, 1024)
    p = None
    for i in range(2):
        arrived(nrm.at[i, 0:7], n_rsem.at[i])
        block = nrm[i].astype(F32).reshape(64, 512).astype(BF16)
        q = lax.dot_general(wall[:, i * 512:(i + 1) * 512], block, turned, preferred_element_type=F32)
        p = q if p is None else p + q
    for k in range(8):
        packed = jnp.concatenate([p[k * 32:k * 32 + 16, :], p[k * 32 + 16:k * 32 + 32, :]], axis=1)
        osend[k] = packed.astype(BF16)

    owner = lax.div(z, 2)
    slot = tp * 2 + lax.rem(z, 2)
    for r in (4, 3, 5, 2, 6, 1, 7):
        remote(osend.at[lax.rem(z + r, 8)], orecv.at[slot], o_ssem, o_rsem, ring(r), owner).start()

    @pl.when(owner != tp)
    def _():
        remote(osend.at[z], orecv.at[slot], o_ssem, o_rsem, kv, owner).start()
        arrived(orecv.at[0:8], o_rsem)

    @pl.when(owner == tp)
    def _():
        orecv[slot] = osend[z]
        arrived(orecv.at[0:7], o_rsem)

    for ref, sem in (
        (acts_t.at[:, 0:128, :], acts_ssem), (acts_t.at[:, 0:96, :], d_ssem), (wsend.at[0:7], w_ssem),
        (kbuf.at[0:7], k_ssem), (qbuf.at[0:7], q_ssem), (wog.at[0:7], g_ssem), (arecv, a_ssem),
        (frecv.at[:, 3:5], p_ssem), (frecv.at[:, 0, 0:7], h_ssem), (frecv.at[:, 1:3], b_ssem), (erecv.at[0:7], e_ssem), (efar, x_ssem),
        (nrm.at[:, 0:7], n_ssem),
    ):
        sent(ref, sem)

    @pl.when(owner != tp)
    def _():
        sent(osend.at[0:8], o_ssem)

    @pl.when(owner == tp)
    def _():
        sent(osend.at[0:7], o_ssem)


def hand_out(orecv, b, a_out, b_out, out_v, sem):
    copies = [pltpu.make_async_copy(b.at[s, pl.ds(g, 2)], b_out.at[s, pl.ds(g, 2)], sem.at[2 * s + g // 2])
              for s in range(2) for g in (0, 2)]
    for cp in copies:
        cp.start()
    sums = []
    for q in range(2):
        s4 = orecv[q].astype(F32)
        for x in range(1, 4):
            s4 = s4 + orecv[x * 2 + q].astype(F32)
        sums.append(s4)
    lane16 = lax.broadcasted_iota(jnp.int32, (16, 128), 1) < 64
    top = jnp.where(lane16, sums[0], pltpu.roll(sums[1], 64, axis=1))
    bottom = jnp.where(lane16, pltpu.roll(sums[0], 64, axis=1), sums[1])
    out_v[...] = jnp.concatenate([top, bottom], axis=0).astype(BF16)
    copies.append(pltpu.make_async_copy(out_v, a_out, sem.at[4]))
    copies[-1].start()
    for cp in copies:
        cp.wait()


def per_device(
    hidden_vectors, input_norm_gain, gate_matrix, value_matrix, write_matrix, read_matrix, step_matrix,
    raw_value_rows, raw_write_rows, raw_read_rows, value_filter_taps, write_filter_taps, read_filter_taps,
    step_size_bias, rate_logarithm, direct_path_gain, prior_step_preact, extra_log_decay, accepted, prior_state,
    group_norm_gain, output_matrix,
):
    operands = [
        accepted, hidden_vectors.T, input_norm_gain.reshape(1, 32), gate_matrix, value_matrix, write_matrix, read_matrix,
        step_matrix.T, raw_value_rows.transpose(1, 0, 2), raw_write_rows.transpose(1, 0, 2),
        raw_read_rows.transpose(1, 0, 2), value_filter_taps, write_filter_taps,
        read_filter_taps, step_size_bias.reshape(1, 16), rate_logarithm.reshape(1, 16),
        direct_path_gain.reshape(1, 16), prior_step_preact, extra_log_decay, prior_state.reshape(2, 4, 256, 128),
        group_norm_gain.reshape(1, 1024), output_matrix.T,
    ]
    buffers = [
        pltpu.SMEM((2,), jnp.int32),
        pltpu.VMEM((32, 512), BF16),
        pltpu.VMEM((1, 32), F32),
        pltpu.VMEM((2, 32, 1024), BF16),
        pltpu.VMEM((2, 32, 512), BF16),
        pltpu.VMEM((16, 32), BF16),
        pltpu.VMEM((32, 1024), BF16),
        pltpu.VMEM((7, 2, 1024), BF16),
        pltpu.VMEM((2, 7, 2, 512), BF16),
        pltpu.VMEM((4, 1024), BF16),
        pltpu.VMEM((2, 4, 512), BF16),
        pltpu.VMEM((3, 1, 16), F32),
        pltpu.VMEM((2, 4, 16), F32),
        pltpu.VMEM((2, 8, 16), F32),
        pltpu.VMEM((1, 1024), F32),
    ]
    dma = pltpu.SemaphoreType.DMA
    scratch = buffers + [
        pltpu.VMEM((2, 256, 256), BF16),
        pltpu.VMEM((8, 3, 32, 128), BF16),
        pltpu.VMEM((3, 256, 128), BF16),
        pltpu.VMEM((8, 16, 128), BF16),
        pltpu.VMEM((8, 4, 128), F32),
        pltpu.VMEM((512, 256), F32),
        pltpu.VMEM((512, 256), BF16),
        pltpu.VMEM((3, 8, 8, 8, 128), BF16),
        pltpu.VMEM((3, 3, 8, 8, 128), BF16),
        pltpu.VMEM((3, 2, 8, 8, 128), BF16),
        pltpu.VMEM((3, 5, 8, 8, 128), BF16),
        pltpu.VMEM((8, 8, 128), BF16),
        pltpu.VMEM((8, 8, 128), BF16),
        pltpu.VMEM((8, 128), BF16),
        pltpu.VMEM((2, 8, 8, 512), BF16),
        pltpu.VMEM((8, 32, 1024), BF16),
        pltpu.VMEM((8, 16, 128), BF16),
        pltpu.VMEM((8, 2048), F32),
        pltpu.VMEM((2, 4, 256, 128), BF16),
        dma((16,)),
        dma((2, 3)), dma((2,)), dma((3,)), dma, dma, dma((4,)), dma((3,)), dma((3,)), dma, dma, dma, dma, dma((2,)), dma,
        pltpu.SemaphoreType.REGULAR,
    ]
    operands = [pltpu.with_memory_space_constraint(x, pltpu.HBM) for x in operands]
    out, state = pl.pallas_call(
        mixer_kernel,
        out_shape=(
            pltpu.VMEM((8, 16, 128), BF16),
            pltpu.VMEM((2, 4, 256, 128), F32),
        ),
        in_specs=[pl.BlockSpec(memory_space=pl.ANY)] * len(operands),
        out_specs=(pl.BlockSpec(memory_space=pltpu.VMEM), pl.BlockSpec(memory_space=pltpu.VMEM)),
        scratch_shapes=scratch,
        compiler_params=pltpu.CompilerParams(
            collective_id=0, has_side_effects=True, vmem_limit_bytes=32 * 1024 * 1024
        ),
        cost_estimate=pl.CostEstimate(flops=10**9, bytes_accessed=4 * 10**6, transcendentals=10**5),
        name="mixer",
    )(*operands)
    out, state = [pltpu.with_memory_space_constraint(x, pltpu.VMEM) for x in (out, state)]
    out, state = pl.pallas_call(
        hand_out,
        out_shape=(
            jax.ShapeDtypeStruct((32, 128), BF16),
            jax.ShapeDtypeStruct((2, 4, 256, 128), F32),
        ),
        in_specs=[pl.BlockSpec(memory_space=pltpu.VMEM)] * 2,
        out_specs=(pl.BlockSpec(memory_space=pl.ANY),) * 2,
        scratch_shapes=[pltpu.VMEM((32, 128), BF16), pltpu.SemaphoreType.DMA((5,))],
        compiler_params=pltpu.CompilerParams(vmem_limit_bytes=32 * 1024 * 1024),
        name="hand_out",
    )(out, state)
    return out.T, state.reshape(2, 16, 64, 128)


def solution(mesh):
    return jax.shard_map(
        per_device,
        mesh=mesh,
        in_specs=(
            P(None, "kv"),
            P("kv"),
            P("kv", "tp"),
            P("kv", "tp"),
            P("kv", "tp"),
            P("kv", "tp"),
            P("kv", "tp"),
            P("kv", None, "tp"),
            P("kv", None, "tp"),
            P("kv", None, "tp"),
            P(None, "tp"),
            P(None, "tp"),
            P(None, "tp"),
            P("tp"),
            P("tp"),
            P("tp"),
            P("kv", None, "tp"),
            P("kv", None, "tp"),
            P("kv"),
            P("kv", "tp", None, None),
            P("tp"),
            P("tp", "kv"),
        ),
        out_specs=(P("tp", "kv"), P("kv", "tp", None, None)),
        check_vma=False,
    )
```
